128 devices in a mesh: sp: 64 (over z, y, x), tp: 2 (over core).
Axes of the slice: x: 4, y: 4, z: 4, core: 2. Of those that a mesh axis runs over, the one named last changes fastest.
Arguments:
- gate_pre: bfloat16 [16384, 2048], P('sp', 'tp'), may hold values from -6 to 6
- conv_in: bfloat16 [16384, 2048], P('sp', 'tp'), may hold values from -6 to 6
- conv_taps: bfloat16 [4, 2048], P(None, 'tp'), may hold values from -3 to 3
- recur_map: bfloat16 [8, 256, 256], P('tp'), may hold values from -0.375 to 0.375
- input_map: bfloat16 [8, 256, 256], P('tp'), may hold values from -0.375 to 0.375
- rate_logit: float32 [2048], P('tp'), may hold values from 4.5 to 15
- decay_shift: float32 [16384, 8], P('sp', 'tp'), may hold values from -1.5 to 0
- out_weight: bfloat16 [2048, 2048], replicated, may hold values from -0.25 to 0.25
- residual: bfloat16 [16384, 2048], P(('sp', 'tp')), may hold values from -6 to 6
- gain_mix: float32 [2048], replicated, may hold values from 0.1 to 1.9
- routes: int32 [16384, 4], P(('sp', 'tp')), may hold values from 0 to 127, all different within a row; in each aligned block of 128 rows (0 to 127, 128 to 255, ...) at most 8 rows name the same one
- route_weight: float32 [16384, 4], P(('sp', 'tp')), may hold values from 0.2 to 1
- shared_gate: bfloat16 [2048, 512], replicated, may hold values from -0.125 to 0.125
- shared_up: bfloat16 [2048, 512], replicated, may hold values from -0.125 to 0.125
- shared_down: bfloat16 [512, 2048], replicated, may hold values from -0.375 to 0.375
- expert_gate: bfloat16 [128, 2048, 512], P(('sp', 'tp')), may hold values from -0.125 to 0.125
- expert_up: bfloat16 [128, 2048, 512], P(('sp', 'tp')), may hold values from -0.125 to 0.125
- expert_down: bfloat16 [128, 512, 2048], P(('sp', 'tp')), may hold values from -0.375 to 0.375
- gain_out: float32 [2048], replicated, may hold values from 0.1 to 1.9
Outputs:
- layer_out: bfloat16 [16384, 2048], P(('sp', 'tp'))
The draws below stay inside these ranges and needn't reach their ends.
Inputs may be any that keep to these rules, and one draw needn't show every extreme that they name: `routes`: each row names 4 different experts. In the rows of one device (aligned blocks of 128 rows) no expert is named more than 8 times, and in some blocks one expert is named exactly 8 times.
All inputs are finite; a program needn't handle non-finite values.
Results may differ from the reference program's by a relative error of at most 0.014.
Values may be sent and summed in bfloat16 or wider, within the bound.
No kernel may reach another device: no remote copies, remote signals or barrier semaphores. Data moves between devices by JAX's collectives and lax.ppermute only.
A program may use at most 128 MiB of HBM per device.

```python
import math
import jax
import jax.numpy as jnp
import numpy as np
from jax import lax

D = 2048
HEADS = 8
BW = 256
DR = 2048
CONV = 4
FE = 512
FS = 512
TOPK = 4
TOKENS_PER_SHARD = 256
TOKENS = 16384
ROWS = 128
EXPERTS = 128
CAP = 8


def draw_rate_logit(key, part):
    flag_key, slow_key, fast_key = jax.random.split(jax.random.fold_in(key, 11), 3)
    fast_share = 0.5
    is_fast = jax.random.uniform(flag_key, (HEADS,), jnp.float32) < fast_share
    slow_rate = jnp.exp(jax.random.uniform(slow_key, (HEADS, BW), jnp.float32, math.log(0.3), math.log(1.2))) / TOKENS
    fast_rate = jnp.exp(jax.random.uniform(fast_key, (HEADS, BW), jnp.float32, math.log(0.02), math.log(0.067)))
    chosen_rate = jnp.where(is_fast[:, None], fast_rate, slow_rate)
    return (-jnp.log(jnp.expm1(chosen_rate / 8.0))).reshape(HEADS * BW).astype(jnp.float32)


def draw_decay_shift(key, part):
    base_key, place_key, size_key = jax.random.split(jax.random.fold_in(key, 23), 3)
    block_count = TOKENS // TOKENS_PER_SHARD
    lowest_value, highest = (0.1, 1.0)
    base = jnp.exp(jax.random.uniform(base_key, (block_count, HEADS), jnp.float32, math.log(lowest_value), math.log(highest))) / TOKENS
    equilibrium_memory = -jnp.repeat(base, TOKENS_PER_SHARD, axis=0)
    location_sequence = jax.random.randint(place_key, (2, HEADS), 0, TOKENS)
    objective_scores = jnp.log(jax.random.uniform(size_key, (2, HEADS), jnp.float32, 0.5, 0.8))
    ordinal_locator = jnp.arange(TOKENS)[:, None]
    arrival_clusters = jnp.where(ordinal_locator == location_sequence[0][None, :], objective_scores[0][None, :], 0.0) + jnp.where(ordinal_locator == location_sequence[1][None, :], objective_scores[1][None, :], 0.0)
    return (equilibrium_memory + arrival_clusters).astype(jnp.float32)


def block_scale(key, extent, cuts, least, top_value):
    def one(position, shards_of):
        steps = jax.random.uniform(jax.random.fold_in(jax.random.fold_in(key, 6), position), (shards_of,), jnp.float32, least / len(cuts), top_value / len(cuts))
        return jnp.repeat(jnp.exp(steps), extent[position] // shards_of).reshape((-1,) + (1,) * (len(extent) - position - 1))

    factor_of = one(*cuts[0])
    for cut in cuts[1:]:
        factor_of = factor_of * one(*cut)
    return factor_of


def assign_block(key, own, number, rows, number_of, top, most, slope):
    ranking = jax.random.permutation(key, number_of)
    packed, common = shares(number_of, rows * top, most, slope, True), shares(number_of, rows * top, most, slope, False)
    places = jnp.arange(number_of)

    def named(tallies, offset_by):
        used = int((tallies > 0).sum())
        fixed = max(1, used // 4)
        passed = fixed + (places - fixed + offset_by * (used - fixed)) % max(1, number_of - fixed)
        return jnp.zeros((number_of,), jnp.int32).at[ranking[jnp.where(places < fixed, places, passed)]].set(jnp.asarray(tallies, jnp.int32))

    tallies = jnp.where(number % 4 == 0, named(packed, number // 4), named(common, number - number // 4 - 1))
    mixed = jax.random.permutation(jax.random.fold_in(own, 3), number_of)
    giver, sink = mixed[0:number_of // 2 * 2:2], mixed[1:number_of // 2 * 2:2]
    slack = jnp.minimum(tallies[giver] - 1, most - tallies[sink]) // 2
    slack = jnp.where((giver == ranking[0]) | (sink == ranking[0]) | (tallies[sink] == 0), 0, jnp.maximum(slack, 0))
    passed = jax.random.randint(jax.random.fold_in(own, 4), (number_of // 2,), 0, 1 << 20) % (slack + 1)
    tallies = tallies.at[giver].add(-passed).at[sink].add(passed)
    labels = jnp.searchsorted(jnp.cumsum(tallies), jnp.arange(rows * top), side="right").astype(jnp.int32)
    listing = labels.reshape(top, rows).T
    listing = listing[jax.random.permutation(jax.random.fold_in(own, 1), rows)]
    offset_by = jax.random.randint(jax.random.fold_in(own, 2), (rows, 1), 0, top)
    return jnp.take_along_axis(listing, (jnp.arange(top)[None, :] + offset_by) % top, axis=1)


def shares(amount, total, bound, slope, full):
    loads = [(1 << 20) // math.isqrt(grade ** slope) + 1 for grade in range(1, amount + 1)]
    largest = bound if full else min(bound, max(-(-total // amount), total * loads[0] // sum(loads)))
    least = 1 if total - largest >= amount - 1 else 0
    given, spare = [largest] + [least] * (amount - 1), total - largest - least * (amount - 1)
    while spare > 0:
        free = [i for i in range(1, amount) if given[i] < largest] or [i for i in range(1, amount) if given[i] < bound]
        mass, left = sum([loads[i] for i in free]), spare
        for i in free:
            addition = min(bound - given[i], max(1, left * loads[i] // mass), spare)
            given[i] = given[i] + addition
            spare = spare - addition
    return np.array(given)


def centred(stream_key, shape, width, reach, cuts=(), kind=jnp.bfloat16):
    gain = block_scale(stream_key, shape, cuts, -0.22, 0.18) if cuts else 1.0
    drawn = jax.random.normal(stream_key, shape, jnp.float32) * width * gain
    return jnp.minimum(jnp.maximum(drawn, -reach), reach).astype(kind)


def setup_inputs(seed: int = 0) -> dict:
    streams_of = jax.random.split(jax.random.key(seed), 20)
    gate_pre = centred(streams_of[0], (TOKENS, DR), 1.0, 6.0, ((0, 64), (1, 2)))
    conv_in = centred(streams_of[1], (TOKENS, DR), 1.0, 6.0, ((0, 64), (1, 2)))
    conv_taps = centred(streams_of[2], (CONV, DR), CONV ** -0.5, 3.0, ((1, 2),))
    recur_map = centred(streams_of[3], (HEADS, BW, BW), BW ** -0.5, 0.375, ((0, 2),))
    input_map = centred(streams_of[4], (HEADS, BW, BW), BW ** -0.5, 0.375, ((0, 2),))
    rate_logit = draw_rate_logit(jax.random.fold_in(streams_of[19], 71), 0)
    decay_shift = draw_decay_shift(jax.random.fold_in(streams_of[19], 71), 0)
    out_weight = centred(streams_of[7], (DR, D), (DR // 4) ** -0.5, 0.25)
    residual = centred(streams_of[8], (TOKENS, D), 1.0, 6.0, ((0, 128),))
    gain_mix = jnp.clip(1.0 + 0.18 * jax.random.normal(streams_of[9], (D,), jnp.float32), 0.1, 1.9)
    routes_keys = jax.random.split(jax.random.fold_in(streams_of[10], 1), TOKENS // ROWS)
    routes_turns = jax.random.permutation(jax.random.fold_in(streams_of[10], 3), TOKENS // ROWS)
    routes = jax.vmap(lambda own, number: assign_block(jax.random.fold_in(streams_of[10], 2), own, number, ROWS, EXPERTS, TOPK, CAP, 1))(routes_keys, routes_turns).reshape((TOKENS, TOPK))
    route_weight = jnp.clip(0.2 + 0.8 * jax.random.uniform(streams_of[11], (TOKENS, TOPK), jnp.float32) ** block_scale(streams_of[11], (TOKENS, TOPK), ((0, 128),), -0.2, 0.2), 0.2, 1.0)
    shared_gate = centred(streams_of[12], (D, FS), D ** -0.5, 0.125)
    shared_up = centred(streams_of[13], (D, FS), D ** -0.5, 0.125)
    shared_down = centred(streams_of[14], (FS, D), (FS // 2) ** -0.5, 0.375)
    expert_gate = centred(streams_of[15], (EXPERTS, D, FE), D ** -0.5, 0.125, ((0, 128),))
    expert_up = centred(streams_of[16], (EXPERTS, D, FE), D ** -0.5, 0.125, ((0, 128),))
    expert_down = centred(streams_of[17], (EXPERTS, FE, D), (FE // 2) ** -0.5, 0.375, ((0, 128),))
    gain_out = jnp.clip(1.0 + 0.18 * jax.random.normal(streams_of[18], (D,), jnp.float32), 0.1, 1.9)
    return dict(gate_pre=gate_pre, conv_in=conv_in, conv_taps=conv_taps, recur_map=recur_map, input_map=input_map, rate_logit=rate_logit, decay_shift=decay_shift, out_weight=out_weight, residual=residual, gain_mix=gain_mix, routes=routes, route_weight=route_weight, shared_gate=shared_gate, shared_up=shared_up, shared_down=shared_down, expert_gate=expert_gate, expert_up=expert_up, expert_down=expert_down, gain_out=gain_out)


ALPHA = 8.0 ** 0.25
RATE_C = 8.0
NORM_EPS = 1e-05

def layer_norm(values, gains):
    center = values - lax.optimization_barrier(jnp.mean(values, axis=-1, keepdims=True))
    spread = lax.optimization_barrier(jnp.mean(center * center, axis=-1, keepdims=True))
    return center * lax.rsqrt(spread + NORM_EPS) * gains

def combine(former, latter):
    return (former[0] * latter[0], latter[0] * former[1] + latter[1])

def reference(gate_pre, conv_in, conv_taps, recur_map, input_map, rate_logit, decay_shift, out_weight, residual, gain_mix, routes, route_weight, shared_gate, shared_up, shared_down, expert_gate, expert_up, expert_down, gain_out):
    length = conv_in.shape[0]
    padded = jnp.concatenate([jnp.zeros((CONV - 1, DR), conv_in.dtype), conv_in], axis=0).astype(jnp.float32)
    filter_tap_weight = conv_taps.astype(jnp.float32)
    summed = jnp.zeros((length, DR), jnp.float32)
    for offset in range(CONV):
        summed = summed + filter_tap_weight[offset] * padded[offset:offset + length]
    conv_out = summed.astype(jnp.bfloat16)
    grouped = conv_out.astype(jnp.float32).reshape(length, HEADS, BW)
    recur_gate = jax.nn.sigmoid(jnp.einsum('thc,hcd->thd', grouped, recur_map.astype(jnp.float32)))
    input_gate = jax.nn.sigmoid(jnp.einsum('thc,hcd->thd', grouped, input_map.astype(jnp.float32)))
    log_decay = -RATE_C * jax.nn.softplus(-rate_logit).reshape(HEADS, BW) * recur_gate + decay_shift[:, :, None]
    update = jnp.sqrt(-jnp.expm1(2.0 * log_decay)) * input_gate * grouped
    states = lax.associative_scan(combine, (jnp.exp(log_decay), update), axis=0)[1]
    mixed_rows = (states.reshape(length, DR) * jax.nn.gelu(gate_pre.astype(jnp.float32), approximate=True)).astype(jnp.bfloat16)
    projected = jnp.dot(mixed_rows, out_weight, preferred_element_type=jnp.float32)
    normed = layer_norm(ALPHA * residual.astype(jnp.float32) + projected, gain_mix).astype(jnp.bfloat16)
    fanout = routes.shape[1]
    flat_ids = routes.reshape(-1).astype(jnp.int32)
    ordering = jnp.argsort(flat_ids, stable=True).astype(jnp.int32)
    sorted_ids = flat_ids[ordering]
    counts = jax.ops.segment_sum(jnp.ones_like(flat_ids), flat_ids, num_segments=EXPERTS).astype(jnp.int32)
    starts = (jnp.cumsum(counts) - counts).astype(jnp.int32)
    within = (jnp.arange(flat_ids.shape[0], dtype=jnp.int32) - starts[sorted_ids]).astype(jnp.int32)
    most_rows = length // ROWS * CAP
    sources = jnp.full((EXPERTS, most_rows), length, jnp.int32).at[sorted_ids, within].set(ordering // fanout)
    weights = jnp.zeros((EXPERTS, most_rows), jnp.float32).at[sorted_ids, within].set(route_weight.reshape(-1)[ordering].astype(jnp.float32))
    padded_rows = jnp.concatenate([normed, jnp.zeros((1, D), jnp.bfloat16)], axis=0)

    def specialist_pass(routed, member):
        chosen_ids, chosen_weights, gate_weight, up_weight, down_weight = member
        chosen = padded_rows[chosen_ids]
        hidden = (jax.nn.silu(jnp.dot(chosen, gate_weight, preferred_element_type=jnp.float32)) * jnp.dot(chosen, up_weight, preferred_element_type=jnp.float32)).astype(jnp.bfloat16)
        result = jnp.dot(hidden, down_weight, preferred_element_type=jnp.float32).astype(jnp.bfloat16)
        return (routed.at[chosen_ids].add(chosen_weights[:, None] * result.astype(jnp.float32)), None)
    routed = lax.scan(specialist_pass, jnp.zeros((length + 1, D), jnp.float32), (sources, weights, expert_gate, expert_up, expert_down))[0]
    shared_hidden = (jax.nn.silu(jnp.dot(normed, shared_gate, preferred_element_type=jnp.float32)) * jnp.dot(normed, shared_up, preferred_element_type=jnp.float32)).astype(jnp.bfloat16)
    moe_sum = jnp.dot(shared_hidden, shared_down, preferred_element_type=jnp.float32) + routed[:length]
    return layer_norm(ALPHA * normed.astype(jnp.float32) + moe_sum, gain_out).astype(jnp.bfloat16)
```

```python
import functools

import jax
import jax.numpy as jnp
from jax import lax
from jax.experimental import pallas as pl
from jax.experimental.pallas import tpu as pltpu
from jax.sharding import PartitionSpec as P

ALPHA = 8.0**0.25
RATE_C = 8.0
NORM_EPS = 1e-05
CAP = 8
PARTS = 2
LANES = 8
F32 = jnp.float32
BF16 = jnp.bfloat16
VMEM = pl.BlockSpec(memory_space=pltpu.VMEM)
SMEM = pl.BlockSpec(memory_space=pltpu.SMEM)


def call(kernel, out_shape, in_specs, flops, scratch=(), name=None):
    return pl.pallas_call(
        kernel,
        out_shape=out_shape,
        in_specs=in_specs,
        out_specs=jax.tree.map(lambda _: VMEM, out_shape),
        scratch_shapes=list(scratch),
        compiler_params=pltpu.CompilerParams(vmem_limit_bytes=48 * 2**20),
        cost_estimate=pl.CostEstimate(flops=flops, bytes_accessed=2**20, transcendentals=0),
        name=name,
    )


def shape(dims, dtype):
    return jax.ShapeDtypeStruct(dims, dtype)


def log1p_unit(u):
    s = u / (2.0 + u)
    q = s * s
    total = jnp.full_like(s, 1.0 / 17.0)
    for k in (15, 13, 11, 9, 7, 5, 3, 1):
        total = total * q + 1.0 / k
    return 2.0 * s * total


def minus_expm1(y):
    total = jnp.full_like(y, 1.0 / 362880.0)
    for k in (40320, 5040, 720, 120, 24, 6, 2, 1):
        total = total * y + 1.0 / k
    return jnp.where(y > -0.5, -y * total, 1.0 - jnp.exp(y))


def strided(ref, start, stride):
    parts = [ref[c, pl.ds(start, LANES, stride=stride), :] for c in range(ref.shape[0])]
    return jnp.concatenate(parts, axis=1)


def layer_norm(values, gains):
    center = values - jnp.mean(values, axis=-1, keepdims=True)
    spread = jnp.mean(center * center, axis=-1, keepdims=True)
    return center * lax.rsqrt(spread + NORM_EPS) * gains


def scan_kernel(
    halo_ref, x_ref, taps_ref, rmap_ref, imap_ref, rate_ref, shift_ref,
    h_ref, a_ref, hex_ref, aex_ref, tot_ref, ext, cv, rg, ig, sh,
):
    tokens, channels = x_ref.shape
    steps = tokens // LANES
    heads, width = rmap_ref.shape[:2]
    reach = halo_ref.shape[0]
    pad = 8 - reach
    for c in range(ext.shape[0]):
        cols = slice(c * 128, (c + 1) * 128)
        ext[c, pl.ds(pad, reach), :] = halo_ref[:, cols].astype(F32)
        ext[c, pl.ds(8, tokens), :] = x_ref[:, cols].astype(F32)
    taps = [taps_ref[pl.ds(j, 1), :].astype(F32) for j in range(reach + 1)]
    full = jnp.concatenate([shift_ref[...], jnp.zeros((128 - heads, tokens), F32)], axis=0)
    sh[...] = jnp.transpose(full)

    def conv(t, _):
        total = jnp.zeros((LANES, channels), F32)
        for j in range(reach + 1):
            total = total + taps[j] * strided(ext, t + pad + j, steps)
        cv[pl.ds(pl.multiple_of(t * LANES, LANES), LANES), :] = total.astype(BF16).astype(F32)
        return 0

    lax.fori_loop(0, steps, conv, 0, unroll=4)
    for k in range(heads):
        cols = slice(k * width, (k + 1) * width)
        block = cv[:, cols].astype(BF16)
        rg[:, cols] = jnp.dot(block, rmap_ref[k], preferred_element_type=F32)
        ig[:, cols] = jnp.dot(block, imap_ref[k], preferred_element_type=F32)
    logit = -rate_ref[...]
    slope = -RATE_C * (jnp.maximum(logit, 0.0) + log1p_unit(jnp.exp(-jnp.abs(logit))))

    def step(t, carry):
        rows = pl.ds(pl.multiple_of(t * LANES, LANES), LANES)
        moved = sh[pl.ds(t, LANES, stride=steps), :]
        out = []
        for k in range(heads):
            h, a = carry[k]
            cols = slice(k * width, (k + 1) * width)
            log_decay = slope[:, cols] * jax.nn.sigmoid(rg[rows, cols]) + moved[:, k : k + 1]
            update = (
                jnp.sqrt(minus_expm1(2.0 * log_decay))
                * jax.nn.sigmoid(ig[rows, cols])
                * cv[rows, cols]
            )
            decay = jnp.exp(log_decay)
            h = decay * h + update
            a = decay * a
            h_ref[rows, cols] = h
            a_ref[rows, cols] = a
            out.append((h, a))
        return tuple(out)

    start = tuple(
        (jnp.zeros((LANES, width), F32), jnp.ones((LANES, width), F32)) for _ in range(heads)
    )
    last = lax.fori_loop(0, steps, step, start, unroll=2)
    row = lax.broadcasted_iota(jnp.int32, (LANES, width), 0)
    for k in range(heads):
        cols = slice(k * width, (k + 1) * width)
        h, a = last[k]
        for d in (1, 2, 4):
            hp, ap = pltpu.roll(h, d, 0), pltpu.roll(a, d, 0)
            h = jnp.where(row >= d, a * hp + h, h)
            a = jnp.where(row >= d, a * ap, a)
        hex_ref[:, cols] = jnp.where(row >= 1, pltpu.roll(h, 1, 0), 0.0)
        aex_ref[:, cols] = jnp.where(row >= 1, pltpu.roll(a, 1, 0), 1.0)
        both = jnp.concatenate([a[LANES - 1 :], h[LANES - 1 :]], axis=0)
        tot_ref[:, :, cols] = jnp.broadcast_to(both[None], (tot_ref.shape[0], 2, width))


def mix_kernel(index_ref, seen_ref, h_ref, a_ref, hex_ref, aex_ref, gate_ref, mine_ref, theirs_ref, st):
    tokens, channels = h_ref.shape
    steps = tokens // LANES
    here, side = index_ref[0], index_ref[1]

    def fold(i, c):
        pair = seen_ref[i]
        return pair[0:1] * c + pair[1:2]

    carried = lax.fori_loop(0, here, fold, jnp.zeros((1, channels), F32))
    entry = hex_ref[...] + aex_ref[...] * carried

    def step(t, _):
        rows = pl.ds(pl.multiple_of(t * LANES, LANES), LANES)
        state = h_ref[rows, :] + a_ref[rows, :] * entry
        for c in range(st.shape[0]):
            st[c, pl.ds(t, LANES, stride=steps), :] = state[:, c * 128 : (c + 1) * 128]
        return 0

    lax.fori_loop(0, steps, step, 0, unroll=4)
    half = tokens // 2
    block = 16

    def mixed(rows):
        state = jnp.concatenate([st[c, rows, :] for c in range(st.shape[0])], axis=1)
        return (state * jax.nn.gelu(gate_ref[rows, :].astype(F32), approximate=True)).astype(BF16)

    def put(i, _):
        at = pl.multiple_of(i * block, block)
        rows = pl.ds(at, block)
        theirs_ref[rows, :] = mixed(pl.ds(pl.multiple_of((1 - side) * half + at, block), block))
        mine_ref[rows, :] = mixed(pl.ds(pl.multiple_of(side * half + at, block), block))
        return 0

    lax.fori_loop(0, half // block, put, 0)


def route_kernel(routes_ref, weight_ref, g_ref, c_ref):
    fanout, rows = routes_ref.shape
    experts = g_ref.shape[1] * PARTS // CAP
    per = CAP // PARTS
    slots = experts * per
    expert = lax.broadcasted_iota(jnp.int32, (experts, rows), 0)
    member = jnp.zeros((experts, rows), F32)
    weight = jnp.zeros((experts, rows), F32)
    for k in range(fanout):
        hit = expert == routes_ref[pl.ds(k, 1), :]
        member = member + jnp.where(hit, 1.0, 0.0)
        weight = weight + jnp.where(hit, weight_ref[pl.ds(k, 1), :], 0.0)
    earlier = (
        lax.broadcasted_iota(jnp.int32, (rows, rows), 0)
        < lax.broadcasted_iota(jnp.int32, (rows, rows), 1)
    )
    rank = jnp.dot(
        member.astype(BF16), jnp.where(earlier, 1.0, 0.0).astype(BF16), preferred_element_type=F32
    )
    rank = jnp.where(member > 0.0, rank, -1.0)
    slot = lax.broadcasted_iota(jnp.int32, (slots, experts), 0)
    spread = jnp.where(slot // per == lax.broadcasted_iota(jnp.int32, (slots, experts), 1), 1.0, 0.0)
    spread = spread.astype(BF16)
    high = weight.astype(BF16)
    low = (weight - high.astype(F32)).astype(BF16)

    def to_slots(values):
        return jnp.dot(spread, values, preferred_element_type=F32)

    rank, high, low = to_slots(rank.astype(BF16)), to_slots(high), to_slots(low)
    place = (lax.broadcasted_iota(jnp.int32, (slots, rows), 0) % per).astype(F32)
    for part in range(PARTS):
        chosen = rank == place + float(part * per)
        g_ref[part] = jnp.where(chosen, 1.0, 0.0).astype(BF16)
        c_ref[part, :rows] = jnp.transpose(jnp.where(chosen, high, 0.0)).astype(BF16)
        c_ref[part, rows:] = jnp.transpose(jnp.where(chosen, low, 0.0)).astype(BF16)


def project_kernel(index_ref, mine_ref, w_ref, res_ref, out_ref):
    depth = mine_ref.shape[1]
    rows = pl.ds(pl.multiple_of(index_ref[1] * depth, depth), depth)
    out_ref[...] = ALPHA * res_ref[...].astype(F32) + jnp.dot(
        mine_ref[...], w_ref[rows, :], preferred_element_type=F32
    )


def dispatch_kernel(index_ref, other_ref, w_ref, acc_ref, gain_ref, g_ref, normed_ref, *out_refs):
    depth = other_ref.shape[1]
    rows = pl.ds(pl.multiple_of((1 - index_ref[1]) * depth, depth), depth)
    values = acc_ref[...] + jnp.dot(other_ref[...], w_ref[rows, :], preferred_element_type=F32)
    normed = layer_norm(values, gain_ref[...]).astype(BF16)
    normed_ref[...] = normed
    for part in range(PARTS):
        out_refs[part][...] = jnp.dot(
            g_ref[part], normed, preferred_element_type=F32
        ).astype(BF16)


def hidden_of(x, gate, up):
    return (
        jax.nn.silu(jnp.dot(x, gate, preferred_element_type=F32))
        * jnp.dot(x, up, preferred_element_type=F32)
    ).astype(BF16)


def shared_kernel(x_ref, gate_ref, up_ref, down_ref, out_ref):
    x = x_ref[...]
    hidden = hidden_of(x, gate_ref[...], up_ref[...])
    out_ref[...] = ALPHA * x.astype(F32) + jnp.dot(
        hidden, down_ref[...], preferred_element_type=F32
    )


def expert_kernel(x_ref, gate_ref, up_ref, down_ref, out_ref):
    block = 256

    def step(i, _):
        rows = pl.ds(pl.multiple_of(i * block, block), block)
        hidden = hidden_of(x_ref[rows, :], gate_ref[0], up_ref[0])
        out_ref[rows, :] = jnp.dot(hidden, down_ref[0], preferred_element_type=F32).astype(BF16)
        return 0

    lax.fori_loop(0, x_ref.shape[0] // block, step, 0)


def weighted(c_ref, back_ref, part):
    both = jnp.dot(c_ref[part], back_ref[...], preferred_element_type=F32)
    rows = both.shape[0] // 2
    return both[:rows] + both[rows:]


def gather_kernel(base_ref, c_ref, back_ref, out_ref, *, part):
    out_ref[...] = base_ref[...] + weighted(c_ref, back_ref, part)


def finish_kernel(base_ref, c_ref, back_ref, gain_ref, out_ref, *, part):
    values = base_ref[...] + weighted(c_ref, back_ref, part)
    out_ref[...] = layer_norm(values, gain_ref[...]).astype(BF16)


def on_device(
    gate_pre, conv_in, conv_taps, recur_map, input_map, rate_logit, decay_shift, out_weight,
    residual, gain_mix, routes, route_weight, shared_gate, shared_up, shared_down, expert_gate,
    expert_up, expert_down, gain_out,
):
    tokens, channels = conv_in.shape
    reach = conv_taps.shape[0] - 1
    sp, tp = lax.axis_size("sp"), lax.axis_size("tp")
    experts = sp * tp
    rows = tokens // tp
    model = out_weight.shape[1]
    slots = experts * CAP // PARTS
    index = jnp.stack([lax.axis_index("sp"), lax.axis_index("tp")]).astype(jnp.int32)
    before = lax.ppermute(conv_in[tokens - reach :], "sp", [(i, i + 1) for i in range(sp - 1)])
    grid = shape((tokens, channels), F32)
    edge = shape((LANES, channels), F32)
    big = pltpu.VMEM((tokens, channels), F32)
    h, a, hex_, aex, totals = call(
        scan_kernel,
        (grid, grid, edge, edge, shape((sp, 2, channels), F32)),
        [VMEM] * 7,
        10**9,
        [pltpu.VMEM((channels // 128, tokens + 8, 128), F32), big, big, big, pltpu.VMEM((tokens, 128), F32)],
        name="scan",
    )(before, conv_in, conv_taps, recur_map, input_map, rate_logit[None], decay_shift.T)
    seen = lax.all_to_all(totals, "sp", 0, 0, tiled=True)
    g, c = call(
        route_kernel,
        (shape((PARTS, slots, rows), BF16), shape((PARTS, 2 * rows, slots), BF16)),
        [VMEM] * 2,
        10**8,
        name="route",
    )(routes.T, route_weight.T)
    piece = shape((rows, channels), BF16)
    mine, theirs = call(
        mix_kernel, (piece, piece), [SMEM] + [VMEM] * 6, 10**8, [pltpu.VMEM((channels // 128, tokens, 128), F32)], name="mix"
    )(index, seen, h, a, hex_, aex, gate_pre)
    other = lax.ppermute(theirs, "tp", [(0, 1), (1, 0)])
    wide = shape((rows, model), F32)
    acc = call(project_kernel, wide, [SMEM] + [VMEM] * 3, 10**9, name="project")(
        index, mine, out_weight, residual
    )
    normed, *outgoing = call(
        dispatch_kernel,
        (shape((rows, model), BF16),) + (shape((slots, model), BF16),) * PARTS,
        [SMEM] + [VMEM] * 5,
        2 * 10**9,
        name="dispatch",
    )(index, other, out_weight, acc, gain_mix[None], g)

    def exchanged(x):
        x = x.reshape(experts, CAP // PARTS, model)
        x = lax.all_to_all(x, ("sp", "tp"), split_axis=0, concat_axis=0, tiled=True)
        return x.reshape(slots, model)

    received = [exchanged(x) for x in outgoing]
    base = call(shared_kernel, wide, [VMEM] * 4, 10**9, name="shared")(
        normed, shared_gate, shared_up, shared_down
    )
    results = [
        call(expert_kernel, shape((slots, model), BF16), [VMEM] * 4, 3 * 10**9, name="expert")(
            x, expert_gate, expert_up, expert_down
        )
        for x in received
    ]
    back = [exchanged(x) for x in results]
    for part in range(PARTS - 1):
        base = call(
            functools.partial(gather_kernel, part=part), wide, [VMEM] * 3, 10**9, name="gather"
        )(base, c, back[part])
    return call(
        functools.partial(finish_kernel, part=PARTS - 1),
        shape((rows, model), BF16),
        [VMEM] * 4,
        10**9,
        name="finish",
    )(base, c, back[-1], gain_out[None])


def solution(mesh):
    return jax.shard_map(
        on_device,
        mesh=mesh,
        in_specs=(
            P("sp", "tp"),
            P("sp", "tp"),
            P(None, "tp"),
            P("tp", None, None),
            P("tp", None, None),
            P("tp"),
            P("sp", "tp"),
            P(),
            P(("sp", "tp"), None),
            P(),
            P(("sp", "tp"), None),
            P(("sp", "tp"), None),
            P(),
            P(),
            P(),
            P(("sp", "tp"), None, None),
            P(("sp", "tp"), None, None),
            P(("sp", "tp"), None, None),
            P(),
        ),
        out_specs=P(("sp", "tp"), None),
        check_vma=False,
    )
```

```python
import functools

import jax
import jax.numpy as jnp
from jax import lax
from jax.experimental import pallas as pl
from jax.experimental.pallas import tpu as pltpu
from jax.sharding import PartitionSpec as P

ALPHA = 8.0**0.25
RATE_C = 8.0
NORM_EPS = 1e-05
CAP = 8
BLOCK = 256
LANES = 8
F32 = jnp.float32
BF16 = jnp.bfloat16
VMEM = pl.BlockSpec(memory_space=pltpu.VMEM)
SMEM = pl.BlockSpec(memory_space=pltpu.SMEM)
HBM = pl.BlockSpec(memory_space=pltpu.HBM)


def call(
    kernel, out_shape, in_specs, flops, scratch=(), name=None, out_specs=None, grid=(), limit=16
):
    if out_specs is None:
        out_specs = jax.tree.map(lambda _: VMEM, out_shape)
    return pl.pallas_call(
        kernel,
        out_shape=out_shape,
        in_specs=in_specs,
        out_specs=out_specs,
        grid=grid,
        scratch_shapes=list(scratch),
        compiler_params=pltpu.CompilerParams(vmem_limit_bytes=limit * 2**20),
        cost_estimate=pl.CostEstimate(flops=flops, bytes_accessed=2**20, transcendentals=0),
        name=name,
    )


def shape(dims, dtype):
    return jax.ShapeDtypeStruct(dims, dtype)


def log1p_unit(u):
    s = u / (2.0 + u)
    q = s * s
    total = jnp.full_like(s, 1.0 / 17.0)
    for k in (15, 13, 11, 9, 7, 5, 3, 1):
        total = total * q + 1.0 / k
    return 2.0 * s * total


def minus_expm1(y):
    total = jnp.full_like(y, 1.0 / 362880.0)
    for k in (40320, 5040, 720, 120, 24, 6, 2, 1):
        total = total * y + 1.0 / k
    return jnp.where(y > -0.5, -y * total, 1.0 - jnp.exp(y))


def strided(ref, start, stride):
    parts = [ref[c, pl.ds(start, LANES, stride=stride), :] for c in range(ref.shape[0])]
    return jnp.concatenate(parts, axis=1)


def layer_norm(values, gains):
    center = values - jnp.mean(values, axis=-1, keepdims=True)
    spread = jnp.mean(center * center, axis=-1, keepdims=True)
    return center * lax.rsqrt(spread + NORM_EPS) * gains


def fetch(pairs, sems):
    copies = [pltpu.make_async_copy(a, b, sems.at[i]) for i, (a, b) in enumerate(pairs)]
    for copy in copies:
        copy.start()
    return copies


def elements(conv, recur, gain, slope, moved):
    log_decay = slope * jax.nn.sigmoid(recur) + moved
    update = jnp.sqrt(minus_expm1(2.0 * log_decay)) * jax.nn.sigmoid(gain) * conv
    return jnp.exp(log_decay), update


def scan_kernel(
    halo_ref, x_hbm, taps_hbm, rmap_hbm, imap_hbm, rate_hbm, shift_hbm, gate_hbm, routes_hbm,
    weight_hbm, tot_hbm, p_hbm, q_hbm, g_hbm, c_hbm,
    x_ref, taps_ref, rmap_ref, imap_ref, rate_ref, shift_ref, gate_ref, routes_ref, weight_ref,
    tot_ref, p_ref, q_ref, g_ref, c_ref, ext, cv, rg, ig, sh, hs, rs, sems, outs,
):
    copies = fetch(
        [
            (x_hbm, x_ref),
            (shift_hbm, shift_ref),
            (taps_hbm, taps_ref),
            (rate_hbm, rate_ref),
            (rmap_hbm, rmap_ref),
            (imap_hbm, imap_ref),
            (gate_hbm, gate_ref),
            (routes_hbm, routes_ref),
            (weight_hbm, weight_ref),
        ],
        sems,
    )
    tokens, channels = x_ref.shape
    steps = tokens // LANES
    heads, width = rmap_ref.shape[:2]
    reach = taps_ref.shape[0] - 1
    pad = 8 - reach
    for copy in copies[:4]:
        copy.wait()
    for c in range(ext.shape[0]):
        cols = slice(c * 128, (c + 1) * 128)
        ext[c, pl.ds(pad, reach), :] = halo_ref[:, cols].astype(F32)
        ext[c, pl.ds(8, tokens), :] = x_ref[:, cols].astype(F32)
    taps = [taps_ref[pl.ds(j, 1), :].astype(F32) for j in range(reach + 1)]
    full = jnp.concatenate([shift_ref[...], jnp.zeros((128 - heads, tokens), F32)], axis=0)
    sh[...] = jnp.transpose(full)
    logit = -rate_ref[...]
    slope = -RATE_C * (jnp.maximum(logit, 0.0) + log1p_unit(jnp.exp(-jnp.abs(logit))))

    def conv(t, _):
        total = jnp.zeros((LANES, channels), F32)
        for j in range(reach + 1):
            total = total + taps[j] * strided(ext, t + pad + j, steps)
        cv[pl.ds(pl.multiple_of(t * LANES, LANES), LANES), :] = total.astype(BF16).astype(F32)
        return 0

    lax.fori_loop(0, steps, conv, 0, unroll=4)
    for copy in copies[4:6]:
        copy.wait()
    for k in range(heads):
        cols = slice(k * width, (k + 1) * width)
        block = cv[:, cols].astype(BF16)
        rg[:, cols] = jnp.dot(block, rmap_ref[k], preferred_element_type=F32)
        ig[:, cols] = jnp.dot(block, imap_ref[k], preferred_element_type=F32)

    def step(t, carry):
        rows = pl.ds(pl.multiple_of(t * LANES, LANES), LANES)
        moved = sh[pl.ds(t, LANES, stride=steps), :]
        out = []
        for k in range(heads):
            h, run = carry[k]
            cols = slice(k * width, (k + 1) * width)
            decay, update = elements(
                cv[rows, cols], rg[rows, cols], ig[rows, cols], slope[:, cols], moved[:, k : k + 1]
            )
            h = decay * h + update
            run = decay * run
            for j in range(width // 128):
                at, part = k * (width // 128) + j, slice(j * 128, (j + 1) * 128)
                hs[at, pl.ds(t, LANES, stride=steps), :] = h[:, part]
                rs[at, pl.ds(t, LANES, stride=steps), :] = run[:, part]
            out.append((h, run))
        return tuple(out)

    start = tuple(
        (jnp.zeros((LANES, width), F32), jnp.ones((LANES, width), F32)) for _ in range(heads)
    )
    last = lax.fori_loop(0, steps, step, start, unroll=2)
    row = lax.broadcasted_iota(jnp.int32, (LANES, width), 0)
    enter, scale = [], []
    for k in range(heads):
        cols = slice(k * width, (k + 1) * width)
        h, a = last[k]
        for d in (1, 2, 4):
            hp, ap = pltpu.roll(h, d, 0), pltpu.roll(a, d, 0)
            h = jnp.where(row >= d, a * hp + h, h)
            a = jnp.where(row >= d, a * ap, a)
        enter.append(jnp.where(row >= 1, pltpu.roll(h, 1, 0), 0.0))
        scale.append(jnp.where(row >= 1, pltpu.roll(a, 1, 0), 1.0))
        both = jnp.concatenate([a[LANES - 1 :], h[LANES - 1 :]], axis=0)
        tot_ref[:, :, cols] = jnp.broadcast_to(both[None], (tot_ref.shape[0], 2, width))
    out_copies = [pltpu.make_async_copy(tot_ref, tot_hbm, outs.at[0])]
    out_copies[0].start()
    for copy in copies[6:]:
        copy.wait()
    enter, scale = jnp.concatenate(enter, axis=1), jnp.concatenate(scale, axis=1)
    block = 16
    for chunk in range(LANES):
        head, by = enter[chunk : chunk + 1], scale[chunk : chunk + 1]

        def put(i, _):
            rows = pl.ds(pl.multiple_of(chunk * steps + i * block, block), block)
            gate = jax.nn.gelu(gate_ref[rows, :].astype(F32), approximate=True)
            for c in range(hs.shape[0]):
                cols = slice(c * 128, (c + 1) * 128)
                run = rs[c, rows, :]
                p_ref[rows, cols] = (hs[c, rows, :] + run * head[:, cols]) * gate[:, cols]
                q_ref[rows, cols] = run * by[:, cols] * gate[:, cols]
            return 0

        lax.fori_loop(0, steps // block, put, 0)
    route(routes_ref, weight_ref, g_ref, c_ref)
    for i, (ref, hbm) in enumerate(
        ((p_ref, p_hbm), (q_ref, q_hbm), (g_ref, g_hbm), (c_ref, c_hbm))
    ):
        copy = pltpu.make_async_copy(ref, hbm, outs.at[i + 1])
        copy.start()
        out_copies.append(copy)
    for copy in out_copies:
        copy.wait()


def mix_kernel(index_ref, seen_ref, p_ref, q_ref, mine_ref, theirs_ref):
    tokens, channels = p_ref.shape
    here, side = index_ref[0], index_ref[1]

    def fold(i, c):
        pair = seen_ref[i]
        return pair[0:1] * c + pair[1:2]

    carried = lax.fori_loop(0, here, fold, jnp.zeros((1, channels), F32))
    half = tokens // 2
    block = 16

    def put(i, _):
        at = pl.multiple_of(i * block, block)
        for ref, part in ((theirs_ref, 1 - side), (mine_ref, side)):
            rows = pl.ds(pl.multiple_of(part * half + at, block), block)
            ref[pl.ds(at, block), :] = (p_ref[rows, :] + q_ref[rows, :] * carried).astype(BF16)
        return 0

    lax.fori_loop(0, half // block, put, 0, unroll=2)


def route(routes_ref, weight_ref, g_ref, c_ref):
    fanout, rows = routes_ref.shape
    slots = g_ref.shape[0]
    experts = slots // CAP
    expert = lax.broadcasted_iota(jnp.int32, (experts, rows), 0)
    member = jnp.zeros((experts, rows), F32)
    weight = jnp.zeros((experts, rows), F32)
    for k in range(fanout):
        hit = expert == routes_ref[pl.ds(k, 1), :]
        member = member + jnp.where(hit, 1.0, 0.0)
        weight = weight + jnp.where(hit, weight_ref[pl.ds(k, 1), :], 0.0)
    earlier = (
        lax.broadcasted_iota(jnp.int32, (rows, rows), 0)
        < lax.broadcasted_iota(jnp.int32, (rows, rows), 1)
    )
    rank = jnp.dot(
        member.astype(BF16), jnp.where(earlier, 1.0, 0.0).astype(BF16), preferred_element_type=F32
    )
    rank = jnp.where(member > 0.0, rank, -1.0).astype(BF16)
    high = weight.astype(BF16)
    low = (weight - high.astype(F32)).astype(BF16)
    slot = lax.broadcasted_iota(jnp.int32, (BLOCK, experts), 0)
    spread_at = lax.broadcasted_iota(jnp.int32, (BLOCK, experts), 1)
    place = (lax.broadcasted_iota(jnp.int32, (BLOCK, rows), 0) % CAP).astype(F32)
    for b in range(slots // BLOCK):
        spread = jnp.where((slot + b * BLOCK) // CAP == spread_at, 1.0, 0.0).astype(BF16)

        def to_slots(values):
            return jnp.dot(spread, values, preferred_element_type=F32)

        chosen = to_slots(rank) == place
        g_ref[pl.ds(b * BLOCK, BLOCK), :] = jnp.where(chosen, 1.0, 0.0).astype(BF16)
        c_ref[b, :rows] = jnp.transpose(jnp.where(chosen, to_slots(high), 0.0)).astype(BF16)
        c_ref[b, rows:] = jnp.transpose(jnp.where(chosen, to_slots(low), 0.0)).astype(BF16)


def project_kernel(index_ref, mine_ref, w_ref, res_ref, out_ref):
    depth = mine_ref.shape[1]
    rows = pl.ds(pl.multiple_of(index_ref[1] * depth, depth), depth)
    out_ref[...] = ALPHA * res_ref[...].astype(F32) + jnp.dot(
        mine_ref[...], w_ref[rows, :], preferred_element_type=F32
    )


def dispatch_kernel(index_ref, other_ref, w_ref, acc_ref, gain_ref, g_ref, normed_ref, out_ref):
    @pl.when(pl.program_id(0) == 0)
    def _():
        depth = other_ref.shape[1]
        rows = pl.ds(pl.multiple_of((1 - index_ref[1]) * depth, depth), depth)
        values = acc_ref[...] + jnp.dot(other_ref[...], w_ref[rows, :], preferred_element_type=F32)
        normed_ref[...] = layer_norm(values, gain_ref[...]).astype(BF16)

    out_ref[...] = jnp.dot(
        g_ref[...], normed_ref[...], preferred_element_type=F32
    ).astype(BF16)


def hidden_of(x, gate, up):
    return (
        jax.nn.silu(jnp.dot(x, gate, preferred_element_type=F32))
        * jnp.dot(x, up, preferred_element_type=F32)
    ).astype(BF16)


def shared_kernel(x_ref, gate_ref, up_ref, down_ref, out_ref):
    x = x_ref[...]
    hidden = hidden_of(x, gate_ref[...], up_ref[...])
    out_ref[...] = ALPHA * x.astype(F32) + jnp.dot(
        hidden, down_ref[...], preferred_element_type=F32
    )


def expert_kernel(x_ref, gate_ref, up_ref, down_ref, out_ref):
    hidden = hidden_of(x_ref[...], gate_ref[0], up_ref[0])
    out_ref[...] = jnp.dot(hidden, down_ref[0], preferred_element_type=F32).astype(BF16)


def finish_kernel(base_ref, c_ref, back_ref, gain_ref, out_ref, acc):
    i = pl.program_id(0)
    part = jnp.dot(c_ref[i], back_ref[...], preferred_element_type=F32)
    rows = part.shape[0] // 2
    part = part[:rows] + part[rows:]

    @pl.when(i == 0)
    def _():
        acc[...] = base_ref[...] + part

    @pl.when(i > 0)
    def _():
        acc[...] += part

    @pl.when(i == pl.num_programs(0) - 1)
    def _():
        out_ref[...] = layer_norm(acc[...], gain_ref[...]).astype(BF16)


def on_device(
    gate_pre, conv_in, conv_taps, recur_map, input_map, rate_logit, decay_shift, out_weight,
    residual, gain_mix, routes, route_weight, shared_gate, shared_up, shared_down, expert_gate,
    expert_up, expert_down, gain_out,
):
    tokens, channels = conv_in.shape
    reach = conv_taps.shape[0] - 1
    sp, tp = lax.axis_size("sp"), lax.axis_size("tp")
    experts = sp * tp
    rows = tokens // tp
    model = out_weight.shape[1]
    slots = experts * CAP
    blocks = slots // BLOCK
    sem = pltpu.SemaphoreType.DMA
    index = jnp.stack([lax.axis_index("sp"), lax.axis_index("tp")]).astype(jnp.int32)
    before = lax.ppermute(conv_in[tokens - reach :], "sp", [(i, i + 1) for i in range(sp - 1)])
    before, index = lax.optimization_barrier((before, index))
    grid = shape((tokens, channels), F32)
    big = pltpu.VMEM((tokens, channels), F32)
    lanes = pltpu.VMEM((channels // 128, tokens, 128), F32)
    operands = (
        conv_in, conv_taps, recur_map, input_map, rate_logit[None], decay_shift.T, gate_pre,
        routes.T, route_weight.T,
    )
    made = (
        shape((sp, 2, channels), F32), grid, grid, shape((slots, rows), BF16),
        shape((blocks, 2 * rows, BLOCK), BF16),
    )
    totals, p, q, g, c = call(
        scan_kernel,
        made,
        [VMEM] + [HBM] * len(operands),
        10**9,
        [pltpu.VMEM(x.shape, x.dtype) for x in operands + made]
        + [pltpu.VMEM((channels // 128, tokens + 8, 128), F32), big, big, big]
        + [pltpu.VMEM((tokens, 128), F32), lanes, lanes, sem((len(operands),)), sem((len(made),))],
        name="scan",
        out_specs=(HBM,) * len(made),
        limit=62,
    )(before, *operands)
    seen = lax.all_to_all(totals, "sp", 0, 0, tiled=True)
    piece = shape((rows, channels), BF16)
    mine, theirs = call(mix_kernel, (piece, piece), [SMEM] + [VMEM] * 3, 10**8, name="mix")(
        index, seen, p, q
    )
    other = lax.ppermute(theirs, "tp", [(0, 1), (1, 0)])
    wide = shape((rows, model), F32)
    acc = call(project_kernel, wide, [SMEM] + [VMEM] * 3, 10**9, name="project")(
        index, mine, out_weight, residual
    )
    strip = pl.BlockSpec((BLOCK, model), lambda i: (i, 0))
    normed, outgoing = call(
        dispatch_kernel,
        (shape((rows, model), BF16), shape((slots, model), BF16)),
        [SMEM] + [VMEM] * 4 + [pl.BlockSpec((BLOCK, rows), lambda i: (i, 0))],
        2 * 10**9,
        name="dispatch",
        out_specs=(VMEM, strip),
        grid=(blocks,),
    )(index, other, out_weight, acc, gain_mix[None], g)

    def exchanged(x):
        x = x.reshape(experts, CAP, model)
        x = lax.all_to_all(x, ("sp", "tp"), split_axis=0, concat_axis=0, tiled=True)
        return x.reshape(slots, model)

    received = exchanged(outgoing)
    results = call(
        expert_kernel,
        shape((slots, model), BF16),
        [strip] + [VMEM] * 3,
        6 * 10**9,
        name="expert",
        out_specs=strip,
        grid=(blocks,),
    )(received, expert_gate, expert_up, expert_down)
    normed, results = lax.optimization_barrier((normed, results))
    base = call(shared_kernel, wide, [VMEM] * 4, 10**10, name="shared")(
        normed, shared_gate, shared_up, shared_down
    )
    base, results = lax.optimization_barrier((base, results))
    back = exchanged(results)
    return call(
        finish_kernel,
        shape((rows, model), BF16),
        [VMEM, VMEM, strip, VMEM],
        10**9,
        [pltpu.VMEM((rows, model), F32)],
        name="finish",
        grid=(blocks,),
    )(base, c, back, gain_out[None])


def solution(mesh):
    return jax.shard_map(
        on_device,
        mesh=mesh,
        in_specs=(
            P("sp", "tp"),
            P("sp", "tp"),
            P(None, "tp"),
            P("tp", None, None),
            P("tp", None, None),
            P("tp"),
            P("sp", "tp"),
            P(),
            P(("sp", "tp"), None),
            P(),
            P(("sp", "tp"), None),
            P(("sp", "tp"), None),
            P(),
            P(),
            P(),
            P(("sp", "tp"), None, None),
            P(("sp", "tp"), None, None),
            P(("sp", "tp"), None, None),
            P(),
        ),
        out_specs=P(("sp", "tp"), None),
        check_vma=False,
    )
```

```python
import functools

import jax
import jax.numpy as jnp
from jax import lax
from jax.experimental import pallas as pl
from jax.experimental.pallas import tpu as pltpu
from jax.sharding import PartitionSpec as P

ALPHA = 8.0**0.25
RATE_C = 8.0
NORM_EPS = 1e-05
TINY = 1e-36
CAP = 8
BLOCK = 256
LANES = 8
F32 = jnp.float32
BF16 = jnp.bfloat16
VMEM = pl.BlockSpec(memory_space=pltpu.VMEM)
SMEM = pl.BlockSpec(memory_space=pltpu.SMEM)
HBM = pl.BlockSpec(memory_space=pltpu.HBM)


def call(
    kernel, out_shape, in_specs, flops, scratch=(), name=None, out_specs=None, grid=(), limit=16
):
    if out_specs is None:
        out_specs = jax.tree.map(lambda _: VMEM, out_shape)
    return pl.pallas_call(
        kernel,
        out_shape=out_shape,
        in_specs=in_specs,
        out_specs=out_specs,
        grid=grid,
        scratch_shapes=list(scratch),
        compiler_params=pltpu.CompilerParams(vmem_limit_bytes=limit * 2**20),
        cost_estimate=pl.CostEstimate(flops=flops, bytes_accessed=2**20, transcendentals=0),
        name=name,
    )


def shape(dims, dtype):
    return jax.ShapeDtypeStruct(dims, dtype)


def log1p_unit(u):
    s = u / (2.0 + u)
    q = s * s
    total = jnp.full_like(s, 1.0 / 17.0)
    for k in (15, 13, 11, 9, 7, 5, 3, 1):
        total = total * q + 1.0 / k
    return 2.0 * s * total


def minus_expm1_twice(x, decay):
    y = 2.0 * x
    total = jnp.full_like(y, 1.0 / 720.0)
    for k in (120, 24, 6, 2, 1):
        total = total * y + 1.0 / k
    return jnp.where(y > -0.125, -y * total, 1.0 - decay * decay)


def sigmoid(x):
    return 0.5 * jnp.tanh(0.5 * x) + 0.5


def layer_norm(values, gains):
    center = values - jnp.mean(values, axis=-1, keepdims=True)
    spread = jnp.mean(center * center, axis=-1, keepdims=True)
    return center * lax.rsqrt(spread + NORM_EPS) * gains


def fetch(pairs, sems):
    copies = [pltpu.make_async_copy(a, b, sems.at[i]) for i, (a, b) in enumerate(pairs)]
    for copy in copies:
        copy.start()
    return copies


def elements(conv, recur, gain, slope, moved):
    log_decay = slope * sigmoid(recur) + moved
    decay = jnp.exp(log_decay)
    power = minus_expm1_twice(log_decay, decay)
    return decay, power * lax.rsqrt(jnp.maximum(power, TINY)) * sigmoid(gain) * conv


def scan_kernel(
    halo_ref, x_hbm, taps_hbm, rmap_hbm, imap_hbm, rate_hbm, shift_hbm, tot_hbm, run_hbm, edge_hbm,
    x_ref, taps_ref, rmap_ref, imap_ref, rate_ref, shift_ref, tot_ref, run_ref, edge_ref,
    ext, cv, rg, ig, sh, sems, outs,
):
    copies = fetch(
        [
            (x_hbm, x_ref),
            (taps_hbm, taps_ref),
            (shift_hbm, shift_ref),
            (rate_hbm, rate_ref),
            (rmap_hbm, rmap_ref),
            (imap_hbm, imap_ref),
        ],
        sems,
    )
    tokens, channels = x_ref.shape
    steps = tokens // LANES
    stride = steps + 8
    heads, width = rmap_ref.shape[:2]
    reach = taps_ref.shape[0] - 1
    pad = 8 - reach
    for copy in copies[:2]:
        copy.wait()
    for c in range(channels // 128):
        cols = slice(c * 128, (c + 1) * 128)
        x = x_ref[:, cols].astype(F32)
        ext[c, pl.ds(pad, reach), :] = halo_ref[:, cols].astype(F32)
        for i in range(LANES):
            if i > 0:
                ext[c, pl.ds(stride * i, 8), :] = x[steps * i - 8 : steps * i]
            ext[c, pl.ds(stride * i + 8, steps), :] = x[steps * i : steps * (i + 1)]
        taps = [taps_ref[pl.ds(j, 1), cols].astype(F32) for j in range(reach + 1)]
        window = [ext[c, pl.ds(pad + j, LANES, stride=stride), :] for j in range(reach)]
        for t in range(steps):
            window.append(ext[c, pl.ds(8 + t, LANES, stride=stride), :])
            total = taps[0] * window[0]
            for j in range(1, reach + 1):
                total = total + taps[j] * window[j]
            window = window[1:]
            cv[pl.ds(t * LANES, LANES), cols] = total.astype(BF16).astype(F32)
    for copy in copies[2:]:
        copy.wait()
    for k in range(heads):
        cols = slice(k * width, (k + 1) * width)
        block = cv[:, cols].astype(BF16)
        rg[:, cols] = jnp.dot(block, rmap_ref[k], preferred_element_type=F32)
        ig[:, cols] = jnp.dot(block, imap_ref[k], preferred_element_type=F32)
    full = jnp.concatenate([shift_ref[...], jnp.zeros((128 - heads, tokens), F32)], axis=0)
    full = jnp.transpose(full)
    for i in range(LANES):
        sh[pl.ds(stride * i, steps), :] = full[steps * i : steps * (i + 1)]
    logit = -rate_ref[...]
    slope = -RATE_C * (jnp.maximum(logit, 0.0) + log1p_unit(jnp.exp(-jnp.abs(logit))))

    def step(t, carry):
        rows = pl.ds(pl.multiple_of(t * LANES, LANES), LANES)
        moved = sh[pl.ds(t, LANES, stride=stride), :]
        out = []
        for k in range(heads):
            h, run = carry[k]
            cols = slice(k * width, (k + 1) * width)
            decay, update = elements(
                cv[rows, cols], rg[rows, cols], ig[rows, cols], slope[:, cols], moved[:, k : k + 1]
            )
            h = decay * h + update
            run = decay * run
            run_ref[0, rows, cols] = h
            run_ref[1, rows, cols] = run
            out.append((h, run))
        return tuple(out)

    last = tuple(
        (jnp.zeros((LANES, width), F32), jnp.ones((LANES, width), F32)) for _ in range(heads)
    )
    sent = []
    for part in range(4):
        span = steps // 4
        last = lax.fori_loop(part * span, (part + 1) * span, step, last, unroll=2)
        rows = pl.ds(part * span * LANES, span * LANES)
        copy = pltpu.make_async_copy(run_ref.at[:, rows, :], run_hbm.at[:, rows, :], outs.at[part])
        copy.start()
        sent.append(copy)
    row = lax.broadcasted_iota(jnp.int32, (LANES, width), 0)
    for k in range(heads):
        cols = slice(k * width, (k + 1) * width)
        h, a = last[k]
        for d in (1, 2, 4):
            hp, ap = pltpu.roll(h, d, 0), pltpu.roll(a, d, 0)
            h = jnp.where(row >= d, a * hp + h, h)
            a = jnp.where(row >= d, a * ap, a)
        both = jnp.concatenate([a[LANES - 1 :], h[LANES - 1 :]], axis=0)
        tot_ref[:, :, cols] = jnp.broadcast_to(both[None], (tot_ref.shape[0], 2, width))
        edge_ref[0, :, cols] = jnp.where(row >= 1, pltpu.roll(h, 1, 0), 0.0)
        edge_ref[1, :, cols] = jnp.where(row >= 1, pltpu.roll(a, 1, 0), 1.0)
    sent += [
        pltpu.make_async_copy(tot_ref, tot_hbm, outs.at[4]),
        pltpu.make_async_copy(edge_ref, edge_hbm, outs.at[5]),
    ]
    for copy in sent[4:]:
        copy.start()
    for copy in sent:
        copy.wait()


def side_kernel(
    gate_hbm, routes_hbm, weight_hbm, run_hbm, edge_hbm, mixed_hbm, g_hbm, c_hbm,
    gate_ref, routes_ref, weight_ref, run_ref, edge_ref, mixed_ref, g_ref, c_ref, hs, rs, sems, outs,
):
    copies = fetch(
        [
            (routes_hbm, routes_ref),
            (weight_hbm, weight_ref),
            (gate_hbm, gate_ref),
            (run_hbm, run_ref),
            (edge_hbm, edge_ref),
        ],
        sems,
    )
    for copy in copies[:2]:
        copy.wait()
    route(routes_ref, weight_ref, g_ref, c_ref)
    for copy in copies[2:]:
        copy.wait()
    _, tokens, channels = run_ref.shape
    steps = tokens // LANES
    stride = steps + 8

    def step(t, _):
        rows = pl.ds(pl.multiple_of(t * LANES, LANES), LANES)
        run = run_ref[1, rows, :]
        own = run_ref[0, rows, :] + run * edge_ref[0]
        run = run * edge_ref[1]
        for c in range(hs.shape[0]):
            cols = slice(c * 128, (c + 1) * 128)
            hs[c, pl.ds(t, LANES, stride=stride), :] = own[:, cols]
            rs[c, pl.ds(t, LANES, stride=stride), :] = run[:, cols]
        return 0

    lax.fori_loop(0, steps, step, 0, unroll=2)
    block = 16

    def put(i, _):
        rows = pl.ds(pl.multiple_of(i * block, block), block)
        per = steps // block
        source = pl.ds(pl.multiple_of((i // per) * stride + (i % per) * block, 8), block)
        gate = jax.nn.gelu(gate_ref[rows, :].astype(F32), approximate=True)
        for c in range(hs.shape[0]):
            cols = slice(c * 128, (c + 1) * 128)
            mixed_ref[0, rows, cols] = hs[c, source, :] * gate[:, cols]
            mixed_ref[1, rows, cols] = rs[c, source, :] * gate[:, cols]
        return 0

    lax.fori_loop(0, tokens // block, put, 0)
    sent = [
        pltpu.make_async_copy(ref, hbm, outs.at[i])
        for i, (ref, hbm) in enumerate(((mixed_ref, mixed_hbm), (g_ref, g_hbm), (c_ref, c_hbm)))
    ]
    for copy in sent:
        copy.start()
    for copy in sent:
        copy.wait()


def mix_kernel(index_ref, seen_ref, mixed_ref, mine_ref, theirs_ref):
    _, tokens, channels = mixed_ref.shape
    here, side = index_ref[0], index_ref[1]

    def fold(i, c):
        pair = seen_ref[i]
        return pair[0:1] * c + pair[1:2]

    carried = lax.fori_loop(0, here, fold, jnp.zeros((1, channels), F32))
    half = tokens // 2
    block = 16

    def put(i, _):
        at = pl.multiple_of(i * block, block)
        for ref, part in ((theirs_ref, 1 - side), (mine_ref, side)):
            rows = pl.ds(pl.multiple_of(part * half + at, block), block)
            ref[pl.ds(at, block), :] = (mixed_ref[0, rows, :] + mixed_ref[1, rows, :] * carried).astype(
                BF16
            )
        return 0

    lax.fori_loop(0, half // block, put, 0, unroll=2)


def route(routes_ref, weight_ref, g_ref, c_ref):
    fanout, rows = routes_ref.shape
    slots = g_ref.shape[0]
    experts = slots // CAP
    expert = lax.broadcasted_iota(jnp.int32, (experts, rows), 0)
    member = jnp.zeros((experts, rows), F32)
    weight = jnp.zeros((experts, rows), F32)
    for k in range(fanout):
        hit = expert == routes_ref[pl.ds(k, 1), :]
        member = member + jnp.where(hit, 1.0, 0.0)
        weight = weight + jnp.where(hit, weight_ref[pl.ds(k, 1), :], 0.0)
    earlier = (
        lax.broadcasted_iota(jnp.int32, (rows, rows), 0)
        < lax.broadcasted_iota(jnp.int32, (rows, rows), 1)
    )
    rank = jnp.dot(
        member.astype(BF16), jnp.where(earlier, 1.0, 0.0).astype(BF16), preferred_element_type=F32
    )
    rank = jnp.where(member > 0.0, rank, -1.0).astype(BF16)
    high = weight.astype(BF16)
    low = (weight - high.astype(F32)).astype(BF16)
    slot = lax.broadcasted_iota(jnp.int32, (BLOCK, experts), 0)
    spread_at = lax.broadcasted_iota(jnp.int32, (BLOCK, experts), 1)
    place = (lax.broadcasted_iota(jnp.int32, (BLOCK, rows), 0) % CAP).astype(F32)
    for b in range(slots // BLOCK):
        spread = jnp.where((slot + b * BLOCK) // CAP == spread_at, 1.0, 0.0).astype(BF16)

        def to_slots(values):
            return jnp.dot(spread, values, preferred_element_type=F32)

        chosen = to_slots(rank) == place
        g_ref[pl.ds(b * BLOCK, BLOCK), :] = jnp.where(chosen, 1.0, 0.0).astype(BF16)
        cols = slice(b * BLOCK, (b + 1) * BLOCK)
        c_ref[:rows, cols] = jnp.transpose(jnp.where(chosen, to_slots(high), 0.0)).astype(BF16)
        c_ref[rows:, cols] = jnp.transpose(jnp.where(chosen, to_slots(low), 0.0)).astype(BF16)


def project_kernel(index_ref, mine_ref, res_ref, w_hbm, out_ref, rest_ref, own_ref, sems):
    depth = mine_ref.shape[1]
    side = index_ref[1]
    cut = depth // 4
    pairs = []
    for base, ref in ((side, own_ref), (1 - side, rest_ref)):
        for j in range(4):
            rows = pl.ds(pl.multiple_of(base * depth + j * cut, cut), cut)
            pairs.append((w_hbm.at[rows, :], ref.at[pl.ds(j * cut, cut), :]))
    copies = fetch(pairs, sems)
    out_ref[...] = ALPHA * res_ref[...].astype(F32)
    for j in range(4):
        copies[j].wait()
        rows = slice(j * cut, (j + 1) * cut)
        out_ref[...] += jnp.dot(mine_ref[:, rows], own_ref[rows, :], preferred_element_type=F32)
    for copy in copies[4:]:
        copy.wait()


def dispatch_kernel(other_ref, w_ref, acc_ref, gain_ref, g_ref, normed_ref, out_ref):
    values = acc_ref[...] + jnp.dot(other_ref[...], w_ref[...], preferred_element_type=F32)
    normed = layer_norm(values, gain_ref[...]).astype(BF16)
    normed_ref[...] = normed

    def put(i, _):
        at = pl.ds(pl.multiple_of(i * BLOCK, BLOCK), BLOCK)
        out_ref[at, :] = jnp.dot(
            g_ref[at, :], normed_ref[...], preferred_element_type=F32
        ).astype(BF16)
        return 0

    lax.fori_loop(0, out_ref.shape[0] // BLOCK, put, 0)


def hidden_of(x, gate, up):
    return (
        jax.nn.silu(jnp.dot(x, gate, preferred_element_type=F32))
        * jnp.dot(x, up, preferred_element_type=F32)
    ).astype(BF16)


def shared_kernel(x_ref, gate_ref, up_ref, down_ref, out_ref):
    x = x_ref[...]
    hidden = hidden_of(x, gate_ref[...], up_ref[...])
    out_ref[...] = ALPHA * x.astype(F32) + jnp.dot(
        hidden, down_ref[...], preferred_element_type=F32
    )


def expert_kernel(x_ref, gate_ref, up_ref, down_ref, out_ref):
    def step(i, _):
        rows = pl.ds(pl.multiple_of(i * BLOCK, BLOCK), BLOCK)
        hidden = hidden_of(x_ref[rows, :], gate_ref[0], up_ref[0])
        out_ref[rows, :] = jnp.dot(hidden, down_ref[0], preferred_element_type=F32).astype(BF16)
        return 0

    lax.fori_loop(0, x_ref.shape[0] // BLOCK, step, 0)


def finish_kernel(base_ref, c_ref, back_ref, gain_ref, out_ref, acc):
    rows = base_ref.shape[0]
    width = 512
    for j in range(base_ref.shape[1] // width):
        cols = slice(j * width, (j + 1) * width)
        part = jnp.dot(c_ref[...], back_ref[:, cols], preferred_element_type=F32)
        acc[:, cols] = base_ref[:, cols] + part[:rows] + part[rows:]
    out_ref[...] = layer_norm(acc[...], gain_ref[...]).astype(BF16)


def on_device(
    gate_pre, conv_in, conv_taps, recur_map, input_map, rate_logit, decay_shift, out_weight,
    residual, gain_mix, routes, route_weight, shared_gate, shared_up, shared_down, expert_gate,
    expert_up, expert_down, gain_out,
):
    tokens, channels = conv_in.shape
    reach = conv_taps.shape[0] - 1
    sp, tp = lax.axis_size("sp"), lax.axis_size("tp")
    experts = sp * tp
    rows = tokens // tp
    model = out_weight.shape[1]
    slots = experts * CAP
    sem = pltpu.SemaphoreType.DMA
    index = jnp.stack([lax.axis_index("sp"), lax.axis_index("tp")]).astype(jnp.int32)
    before = lax.ppermute(conv_in[tokens - reach :], "sp", [(i, i + 1) for i in range(sp - 1)])
    before, index = lax.optimization_barrier((before, index))
    pair = shape((2, tokens, channels), F32)
    big = pltpu.VMEM((tokens, channels), F32)
    apart = tokens + 8 * LANES
    lanes = pltpu.VMEM((channels // 128, apart, 128), F32)

    def staged(kernel, first, operands, made, flops, scratch, name):
        held = [pltpu.VMEM(x.shape, x.dtype) for x in tuple(operands) + made]
        return call(
            kernel,
            made,
            [VMEM] * len(first) + [HBM] * len(operands),
            flops,
            held + scratch,
            name=name,
            out_specs=(HBM,) * len(made),
            limit=62,
        )(*first, *operands)

    totals, local, edge = staged(
        scan_kernel,
        (before,),
        (conv_in, conv_taps, recur_map, input_map, rate_logit[None], decay_shift.T),
        (shape((sp, 2, channels), F32), pair, shape((2, LANES, channels), F32)),
        10**9,
        [lanes, big, big, big, pltpu.VMEM((apart, 128), F32), sem((6,)), sem((6,))],
        "scan",
    )
    seen = lax.all_to_all(totals, "sp", 0, 0, tiled=True)
    parts, g, c = staged(
        side_kernel,
        (),
        (gate_pre, routes.T, route_weight.T, local, edge),
        (pair, shape((slots, rows), BF16), shape((2 * rows, slots), BF16)),
        10**10,
        [lanes, lanes, sem((5,)), sem((3,))],
        "side",
    )
    piece = shape((rows, channels), BF16)
    mine, theirs = call(
        mix_kernel, (piece, piece), [SMEM, VMEM, VMEM], 10**8, name="mix", limit=8
    )(index, seen, parts)
    other = lax.ppermute(theirs, "tp", [(0, 1), (1, 0)])
    wide = shape((rows, model), F32)
    strip = (channels, model)
    acc, weight = call(
        project_kernel,
        (wide, shape(strip, BF16)),
        [SMEM, VMEM, VMEM, HBM],
        10**9,
        [pltpu.VMEM(strip, BF16), sem((8,))],
        name="project",
        limit=46,
    )(index, mine, residual, out_weight)
    normed, outgoing = call(
        dispatch_kernel,
        (shape((rows, model), BF16), shape((slots, model), BF16)),
        [VMEM] * 5,
        2 * 10**9,
        name="dispatch",
    )(other, weight, acc, gain_mix[None], g)

    def exchanged(x):
        x = x.reshape(experts, CAP, model)
        x = lax.all_to_all(x, ("sp", "tp"), split_axis=0, concat_axis=0, tiled=True)
        return x.reshape(slots, model)

    received = exchanged(outgoing)
    results = call(
        expert_kernel, shape((slots, model), BF16), [VMEM] * 4, 6 * 10**9, name="expert"
    )(received, expert_gate, expert_up, expert_down)
    normed, results = lax.optimization_barrier((normed, results))
    base = call(shared_kernel, wide, [VMEM] * 4, 10**10, name="shared")(
        normed, shared_gate, shared_up, shared_down
    )
    base, results = lax.optimization_barrier((base, results))
    back = exchanged(results)
    return call(
        finish_kernel,
        shape((rows, model), BF16),
        [VMEM] * 4,
        10**9,
        [pltpu.VMEM((rows, model), F32)],
        name="finish",
    )(base, c, back, gain_out[None])


def solution(mesh):
    return jax.shard_map(
        on_device,
        mesh=mesh,
        in_specs=(
            P("sp", "tp"),
            P("sp", "tp"),
            P(None, "tp"),
            P("tp", None, None),
            P("tp", None, None),
            P("tp"),
            P("sp", "tp"),
            P(),
            P(("sp", "tp"), None),
            P(),
            P(("sp", "tp"), None),
            P(("sp", "tp"), None),
            P(),
            P(),
            P(),
            P(("sp", "tp"), None, None),
            P(("sp", "tp"), None, None),
            P(("sp", "tp"), None, None),
            P(),
        ),
        out_specs=P(("sp", "tp"), None),
        check_vma=False,
    )
```

```python
import functools

import jax
import jax.numpy as jnp
from jax import lax
from jax.experimental import pallas as pl
from jax.experimental.pallas import tpu as pltpu
from jax.sharding import PartitionSpec as P

ALPHA = 8.0**0.25
RATE_C = 8.0
NORM_EPS = 1e-05
TINY = 1e-36
CAP = 8
BLOCK = 256
LANES = 8
F32 = jnp.float32
BF16 = jnp.bfloat16
VMEM = pl.BlockSpec(memory_space=pltpu.VMEM)
SMEM = pl.BlockSpec(memory_space=pltpu.SMEM)
HBM = pl.BlockSpec(memory_space=pltpu.HBM)


def call(
    kernel, out_shape, in_specs, flops, scratch=(), name=None, out_specs=None, grid=(), limit=16
):
    if out_specs is None:
        out_specs = jax.tree.map(lambda _: VMEM, out_shape)
    return pl.pallas_call(
        kernel,
        out_shape=out_shape,
        in_specs=in_specs,
        out_specs=out_specs,
        grid=grid,
        scratch_shapes=list(scratch),
        compiler_params=pltpu.CompilerParams(vmem_limit_bytes=limit * 2**20),
        cost_estimate=pl.CostEstimate(flops=flops, bytes_accessed=2**20, transcendentals=0),
        name=name,
    )


def shape(dims, dtype):
    return jax.ShapeDtypeStruct(dims, dtype)


def log1p_unit(u):
    s = u / (2.0 + u)
    q = s * s
    total = jnp.full_like(s, 1.0 / 17.0)
    for k in (15, 13, 11, 9, 7, 5, 3, 1):
        total = total * q + 1.0 / k
    return 2.0 * s * total


def minus_expm1_twice(x, decay):
    y = 2.0 * x
    total = jnp.full_like(y, 1.0 / 720.0)
    for k in (120, 24, 6, 2, 1):
        total = total * y + 1.0 / k
    return jnp.where(y > -0.125, -y * total, 1.0 - decay * decay)


def sigmoid(x):
    return 0.5 * jnp.tanh(0.5 * x) + 0.5


def layer_norm(values, gains):
    center = values - jnp.mean(values, axis=-1, keepdims=True)
    spread = jnp.mean(center * center, axis=-1, keepdims=True)
    return center * lax.rsqrt(spread + NORM_EPS) * gains


def fetch(pairs, sems):
    copies = [pltpu.make_async_copy(a, b, sems.at[i]) for i, (a, b) in enumerate(pairs)]
    for copy in copies:
        copy.start()
    return copies


def elements(conv, recur, gain, slope, moved):
    log_decay = slope * sigmoid(recur) + moved
    decay = jnp.exp(log_decay)
    power = minus_expm1_twice(log_decay, decay)
    return decay, power * lax.rsqrt(jnp.maximum(power, TINY)) * sigmoid(gain) * conv


def scan_kernel(
    halo_ref, x_hbm, taps_hbm, rmap_hbm, imap_hbm, rate_hbm, shift_hbm, tot_hbm, run_hbm, edge_hbm,
    x_ref, taps_ref, rmap_ref, imap_ref, rate_ref, shift_ref, tot_ref, run_ref, edge_ref,
    ext, cv, rg, ig, sh, sems, outs,
):
    copies = fetch(
        [
            (x_hbm, x_ref),
            (taps_hbm, taps_ref),
            (shift_hbm, shift_ref),
            (rate_hbm, rate_ref),
            (rmap_hbm, rmap_ref),
            (imap_hbm, imap_ref),
        ],
        sems,
    )
    tokens, channels = x_ref.shape
    steps = tokens // LANES
    stride = steps + 8
    heads, width = rmap_ref.shape[:2]
    reach = taps_ref.shape[0] - 1
    pad = 8 - reach
    for copy in copies[:2]:
        copy.wait()
    for c in range(channels // 128):
        cols = slice(c * 128, (c + 1) * 128)
        x = x_ref[:, cols].astype(F32)
        ext[c, pl.ds(pad, reach), :] = halo_ref[:, cols].astype(F32)
        for i in range(LANES):
            if i > 0:
                ext[c, pl.ds(stride * i, 8), :] = x[steps * i - 8 : steps * i]
            ext[c, pl.ds(stride * i + 8, steps), :] = x[steps * i : steps * (i + 1)]
        taps = [taps_ref[pl.ds(j, 1), cols].astype(F32) for j in range(reach + 1)]
        window = [ext[c, pl.ds(pad + j, LANES, stride=stride), :] for j in range(reach)]
        for t in range(steps):
            window.append(ext[c, pl.ds(8 + t, LANES, stride=stride), :])
            total = taps[0] * window[0]
            for j in range(1, reach + 1):
                total = total + taps[j] * window[j]
            window = window[1:]
            cv[pl.ds(t * LANES, LANES), cols] = total.astype(BF16).astype(F32)
    for copy in copies[2:]:
        copy.wait()
    for k in range(heads):
        cols = slice(k * width, (k + 1) * width)
        block = cv[:, cols].astype(BF16)
        rg[:, cols] = jnp.dot(block, rmap_ref[k], preferred_element_type=F32)
        ig[:, cols] = jnp.dot(block, imap_ref[k], preferred_element_type=F32)
    full = jnp.concatenate([shift_ref[...], jnp.zeros((128 - heads, tokens), F32)], axis=0)
    full = jnp.transpose(full)
    for i in range(LANES):
        sh[pl.ds(stride * i, steps), :] = full[steps * i : steps * (i + 1)]
    logit = -rate_ref[...]
    slope = -RATE_C * (jnp.maximum(logit, 0.0) + log1p_unit(jnp.exp(-jnp.abs(logit))))

    def step(t, carry):
        rows = pl.ds(pl.multiple_of(t * LANES, LANES), LANES)
        moved = sh[pl.ds(t, LANES, stride=stride), :]
        out = []
        for k in range(heads):
            h, run = carry[k]
            cols = slice(k * width, (k + 1) * width)
            decay, update = elements(
                cv[rows, cols], rg[rows, cols], ig[rows, cols], slope[:, cols], moved[:, k : k + 1]
            )
            h = decay * h + update
            run = decay * run
            for j in range(width // 128):
                lane = slice(j * 128, (j + 1) * 128)
                run_ref[0, k * (width // 128) + j, rows, :] = h[:, lane]
                run_ref[1, k * (width // 128) + j, rows, :] = run[:, lane]
            out.append((h, run))
        return tuple(out)

    last = tuple(
        (jnp.zeros((LANES, width), F32), jnp.ones((LANES, width), F32)) for _ in range(heads)
    )
    sent = []
    for part in range(4):
        span = steps // 4
        last = lax.fori_loop(part * span, (part + 1) * span, step, last, unroll=2)
        rows = pl.ds(part * span * LANES, span * LANES)
        copy = pltpu.make_async_copy(
            run_ref.at[:, :, rows, :], run_hbm.at[:, :, rows, :], outs.at[part]
        )
        copy.start()
        sent.append(copy)
    row = lax.broadcasted_iota(jnp.int32, (LANES, width), 0)
    ends = [[], []]
    for k in range(heads):
        cols = slice(k * width, (k + 1) * width)
        h, a = last[k]
        for d in (1, 2, 4):
            hp, ap = pltpu.roll(h, d, 0), pltpu.roll(a, d, 0)
            h = jnp.where(row >= d, a * hp + h, h)
            a = jnp.where(row >= d, a * ap, a)
        for j in range(width // 128):
            lane = slice(j * 128, (j + 1) * 128)
            ends[0].append(jnp.log(jnp.maximum(a[LANES - 1 :, lane], TINY)))
            ends[1].append(h[LANES - 1 :, lane])
        edge_ref[0, :, cols] = jnp.where(row >= 1, pltpu.roll(h, 1, 0), 0.0)
        edge_ref[1, :, cols] = jnp.where(row >= 1, pltpu.roll(a, 1, 0), 1.0)
    both = jnp.concatenate(ends[0] + ends[1], axis=0).astype(BF16)
    for i in range(tot_ref.shape[0]):
        tot_ref[i] = both
    sent += [
        pltpu.make_async_copy(tot_ref, tot_hbm, outs.at[4]),
        pltpu.make_async_copy(edge_ref, edge_hbm, outs.at[5]),
    ]
    for copy in sent[4:]:
        copy.start()
    for copy in sent:
        copy.wait()


def side_kernel(
    gate_hbm, routes_hbm, weight_hbm, run_hbm, edge_hbm, mixed_hbm, g_hbm, c_hbm,
    gate_ref, routes_ref, weight_ref, run_ref, edge_ref, mixed_ref, g_ref, c_ref, sems, outs,
):
    copies = fetch(
        [
            (routes_hbm, routes_ref),
            (weight_hbm, weight_ref),
            (gate_hbm, gate_ref),
            (run_hbm, run_ref),
            (edge_hbm, edge_ref),
        ],
        sems,
    )
    for copy in copies[:2]:
        copy.wait()
    route(routes_ref, weight_ref, g_ref, c_ref)
    for copy in copies[2:]:
        copy.wait()
    tokens, channels = gate_ref.shape
    steps = tokens // LANES
    block = 16
    per = steps // block

    def put(i, _):
        rows = pl.ds(pl.multiple_of(i * block, block), block)
        chunk = i // per
        source = pl.ds(chunk + (i % per) * (block * LANES), block, stride=LANES)
        gate = jax.nn.gelu(gate_ref[rows, :].astype(F32), approximate=True)
        enter, scale = edge_ref[0, pl.ds(chunk, 1), :], edge_ref[1, pl.ds(chunk, 1), :]
        for c in range(channels // 128):
            cols = slice(c * 128, (c + 1) * 128)
            run = run_ref[1, c, source, :]
            mixed_ref[0, rows, cols] = (run_ref[0, c, source, :] + run * enter[:, cols]) * gate[:, cols]
            mixed_ref[1, rows, cols] = run * scale[:, cols] * gate[:, cols]
        return 0

    pairs = [(g_ref, g_hbm), (c_ref, c_hbm)]
    sent = fetch(pairs, outs)
    quarter = tokens // 4
    for part in range(4):
        lax.fori_loop(part * quarter // block, (part + 1) * quarter // block, put, 0)
        rows = pl.ds(part * quarter, quarter)
        copy = pltpu.make_async_copy(
            mixed_ref.at[:, rows, :], mixed_hbm.at[pl.ds(0, 2), rows, :], outs.at[2 + part]
        )
        copy.start()
        sent.append(copy)
    for copy in sent:
        copy.wait()


def mix_kernel(
    index_ref, seen_ref, mixed_hbm, w_hbm, mine_ref, theirs_ref, w_ref, mixed_ref, sems
):
    _, tokens, channels = mixed_ref.shape
    here, side = index_ref[0], index_ref[1]
    depth = w_ref.shape[0]
    own = pl.ds(pl.multiple_of(side * depth, depth), depth)
    copies = fetch([(mixed_hbm.at[pl.ds(0, 2)], mixed_ref), (w_hbm.at[own, :], w_ref)], sems)
    carried = jnp.zeros((LANES, 128), F32)
    for i in range(seen_ref.shape[0]):
        pair = seen_ref[i].astype(F32)
        carried = jnp.where(i < here, jnp.exp(pair[:LANES]) * carried + pair[LANES:], carried)
    carried = jnp.concatenate([carried[i : i + 1] for i in range(LANES)], axis=1)
    half = tokens // 2
    block = 16
    copies[0].wait()

    def put(i, _):
        at = pl.multiple_of(i * block, block)
        for ref, part in ((theirs_ref, 1 - side), (mine_ref, side)):
            rows = pl.ds(pl.multiple_of(part * half + at, block), block)
            ref[pl.ds(at, block), :] = (mixed_ref[0, rows, :] + mixed_ref[1, rows, :] * carried).astype(
                BF16
            )
        return 0

    lax.fori_loop(0, half // block, put, 0, unroll=2)
    copies[1].wait()


def route(routes_ref, weight_ref, g_ref, c_ref):
    fanout, rows = routes_ref.shape
    slots = g_ref.shape[0]
    experts = slots // CAP
    expert = lax.broadcasted_iota(jnp.int32, (experts, rows), 0)
    member = jnp.zeros((experts, rows), F32)
    weight = jnp.zeros((experts, rows), F32)
    for k in range(fanout):
        hit = expert == routes_ref[pl.ds(k, 1), :]
        member = member + jnp.where(hit, 1.0, 0.0)
        weight = weight + jnp.where(hit, weight_ref[pl.ds(k, 1), :], 0.0)
    earlier = (
        lax.broadcasted_iota(jnp.int32, (rows, rows), 0)
        < lax.broadcasted_iota(jnp.int32, (rows, rows), 1)
    )
    rank = jnp.dot(
        member.astype(BF16), jnp.where(earlier, 1.0, 0.0).astype(BF16), preferred_element_type=F32
    )
    rank = jnp.where(member > 0.0, rank, -1.0).astype(BF16)
    high = weight.astype(BF16)
    low = (weight - high.astype(F32)).astype(BF16)
    slot = lax.broadcasted_iota(jnp.int32, (BLOCK, experts), 0)
    spread_at = lax.broadcasted_iota(jnp.int32, (BLOCK, experts), 1)
    place = (lax.broadcasted_iota(jnp.int32, (BLOCK, rows), 0) % CAP).astype(F32)
    for b in range(slots // BLOCK):
        spread = jnp.where((slot + b * BLOCK) // CAP == spread_at, 1.0, 0.0).astype(BF16)

        def to_slots(values):
            return jnp.dot(spread, values, preferred_element_type=F32)

        chosen = to_slots(rank) == place
        g_ref[pl.ds(b * BLOCK, BLOCK), :] = jnp.where(chosen, 1.0, 0.0).astype(BF16)
        cols = slice(b * BLOCK, (b + 1) * BLOCK)
        c_ref[:rows, cols] = jnp.transpose(jnp.where(chosen, to_slots(high), 0.0)).astype(BF16)
        c_ref[rows:, cols] = jnp.transpose(jnp.where(chosen, to_slots(low), 0.0)).astype(BF16)


def project_kernel(index_ref, mine_ref, res_ref, own_ref, w_hbm, out_ref, rest_ref, sems):
    depth = mine_ref.shape[1]
    rest = pl.ds(pl.multiple_of((1 - index_ref[1]) * depth, depth), depth)
    copies = fetch([(w_hbm.at[rest, :], rest_ref)], sems)
    out_ref[...] = ALPHA * res_ref[...].astype(F32) + jnp.dot(
        mine_ref[...], own_ref[...], preferred_element_type=F32
    )
    copies[0].wait()


def dispatch_kernel(other_ref, w_ref, acc_ref, gain_ref, g_ref, normed_ref, out_ref):
    values = acc_ref[...] + jnp.dot(other_ref[...], w_ref[...], preferred_element_type=F32)
    normed = layer_norm(values, gain_ref[...]).astype(BF16)
    normed_ref[...] = normed

    out_ref[...] = jnp.dot(g_ref[...], normed, preferred_element_type=F32).astype(BF16)


def hidden_of(x, gate, up):
    return (
        jax.nn.silu(jnp.dot(x, gate, preferred_element_type=F32))
        * jnp.dot(x, up, preferred_element_type=F32)
    ).astype(BF16)


def shared_kernel(x_ref, gate_ref, up_ref, down_ref, out_ref):
    x = x_ref[...]
    hidden = hidden_of(x, gate_ref[...], up_ref[...])
    out_ref[...] = ALPHA * x.astype(F32) + jnp.dot(
        hidden, down_ref[...], preferred_element_type=F32
    )


def expert_kernel(x_ref, gate_ref, up_ref, down_ref, out_ref):
    block = 2 * BLOCK

    def step(i, _):
        rows = pl.ds(pl.multiple_of(i * block, block), block)
        hidden = hidden_of(x_ref[rows, :], gate_ref[0], up_ref[0])
        out_ref[rows, :] = jnp.dot(hidden, down_ref[0], preferred_element_type=F32).astype(BF16)
        return 0

    lax.fori_loop(0, x_ref.shape[0] // block, step, 0)


def finish_kernel(base_ref, c_ref, back_ref, gain_ref, out_ref, acc):
    rows = base_ref.shape[0]
    width = 512
    for j in range(base_ref.shape[1] // width):
        cols = slice(j * width, (j + 1) * width)
        part = jnp.dot(c_ref[...], back_ref[:, cols], preferred_element_type=F32)
        acc[:, cols] = base_ref[:, cols] + part[:rows] + part[rows:]
    out_ref[...] = layer_norm(acc[...], gain_ref[...]).astype(BF16)


def on_device(
    gate_pre, conv_in, conv_taps, recur_map, input_map, rate_logit, decay_shift, out_weight,
    residual, gain_mix, routes, route_weight, shared_gate, shared_up, shared_down, expert_gate,
    expert_up, expert_down, gain_out,
):
    tokens, channels = conv_in.shape
    reach = conv_taps.shape[0] - 1
    sp, tp = lax.axis_size("sp"), lax.axis_size("tp")
    experts = sp * tp
    rows = tokens // tp
    model = out_weight.shape[1]
    slots = experts * CAP
    sem = pltpu.SemaphoreType.DMA
    index = jnp.stack([lax.axis_index("sp"), lax.axis_index("tp")]).astype(jnp.int32)
    before = lax.ppermute(conv_in[tokens - reach :], "sp", [(i, i + 1) for i in range(sp - 1)])
    before, index = lax.optimization_barrier((before, index))
    padded = shape((8, tokens, channels), F32)
    big = pltpu.VMEM((tokens, channels), F32)
    apart = tokens + 8 * LANES
    lanes = pltpu.VMEM((channels // 128, apart, 128), F32)

    def staged(kernel, first, operands, made, flops, scratch, name):
        held = [
            pltpu.VMEM((2,) + x.shape[1:] if x is padded else x.shape, x.dtype)
            for x in tuple(operands) + made
        ]
        return call(
            kernel,
            made,
            [VMEM] * len(first) + [HBM] * len(operands),
            flops,
            held + scratch,
            name=name,
            out_specs=(HBM,) * len(made),
            limit=62,
        )(*first, *operands)

    totals, local, edge = staged(
        scan_kernel,
        (before,),
        (conv_in, conv_taps, recur_map, input_map, rate_logit[None], decay_shift.T),
        (
            shape((sp, 2 * LANES, 128), BF16),
            shape((2, channels // 128, tokens, 128), F32),
            shape((2, LANES, channels), F32),
        ),
        10**9,
        [lanes, big, big, big, pltpu.VMEM((apart, 128), F32), sem((6,)), sem((6,))],
        "scan",
    )
    seen = lax.all_to_all(totals, "sp", 0, 0, tiled=True)
    parts, g, c = staged(
        side_kernel,
        (),
        (gate_pre, routes.T, route_weight.T, local, edge),
        (padded, shape((slots, rows), BF16), shape((2 * rows, slots), BF16)),
        10**10,
        [sem((5,)), sem((6,))],
        "side",
    )
    piece = shape((rows, channels), BF16)
    strip = shape((channels, model), BF16)
    mine, theirs, own = call(
        mix_kernel,
        (piece, piece, strip),
        [SMEM, VMEM, HBM, HBM],
        10**8,
        [pltpu.VMEM((2, tokens, channels), F32), sem((2,))],
        name="mix",
        limit=46,
    )(index, seen, parts, out_weight)
    other = lax.ppermute(theirs, "tp", [(0, 1), (1, 0)])
    wide = shape((rows, model), F32)
    acc, rest = call(
        project_kernel,
        (wide, strip),
        [SMEM, VMEM, VMEM, VMEM, HBM],
        10**9,
        [sem((1,))],
        name="project",
        limit=40,
    )(index, mine, residual, own, out_weight)
    normed, outgoing = call(
        dispatch_kernel,
        (shape((rows, model), BF16), shape((slots, model), BF16)),
        [VMEM] * 5,
        2 * 10**9,
        name="dispatch",
        limit=24,
    )(other, rest, acc, gain_mix[None], g)

    def exchanged(x):
        x = x.reshape(experts, CAP, model)
        x = lax.all_to_all(x, ("sp", "tp"), split_axis=0, concat_axis=0, tiled=True)
        return x.reshape(slots, model)

    received = exchanged(outgoing)
    results = call(
        expert_kernel, shape((slots, model), BF16), [VMEM] * 4, 6 * 10**9, name="expert", limit=24
    )(received, expert_gate, expert_up, expert_down)
    normed, results = lax.optimization_barrier((normed, results))
    base = call(shared_kernel, wide, [VMEM] * 4, 10**10, name="shared")(
        normed, shared_gate, shared_up, shared_down
    )
    base, results = lax.optimization_barrier((base, results))
    back = exchanged(results)
    return call(
        finish_kernel,
        shape((rows, model), BF16),
        [VMEM] * 4,
        10**9,
        [pltpu.VMEM((rows, model), F32)],
        name="finish",
    )(base, c, back, gain_out[None])


def solution(mesh):
    return jax.shard_map(
        on_device,
        mesh=mesh,
        in_specs=(
            P("sp", "tp"),
            P("sp", "tp"),
            P(None, "tp"),
            P("tp", None, None),
            P("tp", None, None),
            P("tp"),
            P("sp", "tp"),
            P(),
            P(("sp", "tp"), None),
            P(),
            P(("sp", "tp"), None),
            P(("sp", "tp"), None),
            P(),
            P(),
            P(),
            P(("sp", "tp"), None, None),
            P(("sp", "tp"), None, None),
            P(("sp", "tp"), None, None),
            P(),
        ),
        out_specs=P(("sp", "tp"), None),
        check_vma=False,
    )
```

```python
import functools

import jax
import jax.numpy as jnp
from jax import lax
from jax.experimental import pallas as pl
from jax.experimental.pallas import tpu as pltpu
from jax.sharding import PartitionSpec as P

ALPHA = 8.0**0.25
RATE_C = 8.0
NORM_EPS = 1e-05
TINY = 1e-36
CAP = 8
BLOCK = 256
PIECES = 8
LANES = 8
F32 = jnp.float32
BF16 = jnp.bfloat16
VMEM = pl.BlockSpec(memory_space=pltpu.VMEM)
SMEM = pl.BlockSpec(memory_space=pltpu.SMEM)
HBM = pl.BlockSpec(memory_space=pltpu.HBM)


def call(
    kernel, out_shape, in_specs, flops, scratch=(), name=None, out_specs=None, grid=(), limit=16
):
    if out_specs is None:
        out_specs = jax.tree.map(lambda _: VMEM, out_shape)
    return pl.pallas_call(
        kernel,
        out_shape=out_shape,
        in_specs=in_specs,
        out_specs=out_specs,
        grid=grid,
        scratch_shapes=list(scratch),
        compiler_params=pltpu.CompilerParams(vmem_limit_bytes=limit * 2**20),
        cost_estimate=pl.CostEstimate(flops=flops, bytes_accessed=2**20, transcendentals=0),
        name=name,
    )


def shape(dims, dtype):
    return jax.ShapeDtypeStruct(dims, dtype)


def log1p_unit(u):
    s = u / (2.0 + u)
    q = s * s
    total = jnp.full_like(s, 1.0 / 17.0)
    for k in (15, 13, 11, 9, 7, 5, 3, 1):
        total = total * q + 1.0 / k
    return 2.0 * s * total


def minus_expm1_twice(x, decay):
    y = 2.0 * x
    total = jnp.full_like(y, 1.0 / 720.0)
    for k in (120, 24, 6, 2, 1):
        total = total * y + 1.0 / k
    return jnp.where(y > -0.125, -y * total, 1.0 - decay * decay)


def sigmoid(x):
    return 0.5 * jnp.tanh(0.5 * x) + 0.5


def layer_norm(values, gains):
    center = values - jnp.mean(values, axis=-1, keepdims=True)
    spread = jnp.mean(center * center, axis=-1, keepdims=True)
    return center * lax.rsqrt(spread + NORM_EPS) * gains


def fetch(pairs, sems):
    copies = [pltpu.make_async_copy(a, b, sems.at[i]) for i, (a, b) in enumerate(pairs)]
    for copy in copies:
        copy.start()
    return copies


def elements(conv, recur, gain, slope, moved):
    log_decay = slope * sigmoid(recur) + moved
    decay = jnp.exp(log_decay)
    power = minus_expm1_twice(log_decay, decay)
    return decay, power * lax.rsqrt(jnp.maximum(power, TINY)) * sigmoid(gain) * conv


def scan_kernel(
    halo_ref, x_hbm, taps_hbm, rmap_hbm, imap_hbm, rate_hbm, shift_hbm, tot_hbm, run_hbm, edge_hbm,
    x_ref, taps_ref, rmap_ref, imap_ref, rate_ref, shift_ref, tot_ref, run_ref, edge_ref,
    ext, cv, rg, ig, sh, sems, outs,
):
    copies = fetch(
        [
            (x_hbm, x_ref),
            (taps_hbm, taps_ref),
            (shift_hbm, shift_ref),
            (rate_hbm, rate_ref),
            (rmap_hbm, rmap_ref),
            (imap_hbm, imap_ref),
        ],
        sems,
    )
    tokens, channels = x_ref.shape
    steps = tokens // LANES
    stride = steps + 8
    heads, width = rmap_ref.shape[:2]
    reach = taps_ref.shape[0] - 1
    pad = 8 - reach
    for copy in copies[:2]:
        copy.wait()
    for c in range(channels // 128):
        cols = slice(c * 128, (c + 1) * 128)
        x = x_ref[:, cols].astype(F32)
        ext[c, pl.ds(pad, reach), :] = halo_ref[:, cols].astype(F32)
        for i in range(LANES):
            if i > 0:
                ext[c, pl.ds(stride * i, 8), :] = x[steps * i - 8 : steps * i]
            ext[c, pl.ds(stride * i + 8, steps), :] = x[steps * i : steps * (i + 1)]
        taps = [taps_ref[pl.ds(j, 1), cols].astype(F32) for j in range(reach + 1)]
        window = [ext[c, pl.ds(pad + j, LANES, stride=stride), :] for j in range(reach)]
        for t in range(steps):
            window.append(ext[c, pl.ds(8 + t, LANES, stride=stride), :])
            total = taps[0] * window[0]
            for j in range(1, reach + 1):
                total = total + taps[j] * window[j]
            window = window[1:]
            cv[pl.ds(t * LANES, LANES), cols] = total.astype(BF16).astype(F32)
    for copy in copies[2:]:
        copy.wait()
    for k in range(heads):
        cols = slice(k * width, (k + 1) * width)
        block = cv[:, cols].astype(BF16)
        rg[:, cols] = jnp.dot(block, rmap_ref[k], preferred_element_type=F32)
        ig[:, cols] = jnp.dot(block, imap_ref[k], preferred_element_type=F32)
    full = jnp.concatenate([shift_ref[...], jnp.zeros((128 - heads, tokens), F32)], axis=0)
    full = jnp.transpose(full)
    for i in range(LANES):
        sh[pl.ds(stride * i, steps), :] = full[steps * i : steps * (i + 1)]
    logit = -rate_ref[...]
    slope = -RATE_C * (jnp.maximum(logit, 0.0) + log1p_unit(jnp.exp(-jnp.abs(logit))))

    def step(t, carry):
        rows = pl.ds(pl.multiple_of(t * LANES, LANES), LANES)
        moved = sh[pl.ds(t, LANES, stride=stride), :]
        out = []
        for k in range(heads):
            h, run = carry[k]
            cols = slice(k * width, (k + 1) * width)
            decay, update = elements(
                cv[rows, cols], rg[rows, cols], ig[rows, cols], slope[:, cols], moved[:, k : k + 1]
            )
            h = decay * h + update
            run = decay * run
            for j in range(width // 128):
                lane = slice(j * 128, (j + 1) * 128)
                run_ref[0, k * (width // 128) + j, rows, :] = h[:, lane]
                run_ref[1, k * (width // 128) + j, rows, :] = run[:, lane]
            out.append((h, run))
        return tuple(out)

    last = tuple(
        (jnp.zeros((LANES, width), F32), jnp.ones((LANES, width), F32)) for _ in range(heads)
    )
    sent = []
    for part in range(4):
        span = steps // 4
        last = lax.fori_loop(part * span, (part + 1) * span, step, last, unroll=2)
        rows = pl.ds(part * span * LANES, span * LANES)
        copy = pltpu.make_async_copy(
            run_ref.at[:, :, rows, :], run_hbm.at[:, :, rows, :], outs.at[part]
        )
        copy.start()
        sent.append(copy)
    row = lax.broadcasted_iota(jnp.int32, (LANES, width), 0)
    ends = [[], []]
    for k in range(heads):
        cols = slice(k * width, (k + 1) * width)
        h, a = last[k]
        for d in (1, 2, 4):
            hp, ap = pltpu.roll(h, d, 0), pltpu.roll(a, d, 0)
            h = jnp.where(row >= d, a * hp + h, h)
            a = jnp.where(row >= d, a * ap, a)
        for j in range(width // 128):
            lane = slice(j * 128, (j + 1) * 128)
            ends[0].append(jnp.log(jnp.maximum(a[LANES - 1 :, lane], TINY)))
            ends[1].append(h[LANES - 1 :, lane])
        edge_ref[0, :, cols] = jnp.where(row >= 1, pltpu.roll(h, 1, 0), 0.0)
        edge_ref[1, :, cols] = jnp.where(row >= 1, pltpu.roll(a, 1, 0), 1.0)
    both = jnp.concatenate(ends[0] + ends[1], axis=0).astype(BF16)
    for i in range(tot_ref.shape[0]):
        tot_ref[i] = both
    sent += [
        pltpu.make_async_copy(tot_ref, tot_hbm, outs.at[4]),
        pltpu.make_async_copy(edge_ref, edge_hbm, outs.at[5]),
    ]
    for copy in sent[4:]:
        copy.start()
    for copy in sent:
        copy.wait()


def side_kernel(
    gate_hbm, routes_hbm, weight_hbm, run_hbm, edge_hbm, mixed_hbm, g_hbm, c_hbm,
    gate_ref, routes_ref, weight_ref, run_ref, edge_ref, mixed_ref, g_ref, c_ref, sems, outs,
):
    copies = fetch(
        [
            (routes_hbm, routes_ref),
            (weight_hbm, weight_ref),
            (gate_hbm, gate_ref),
            (run_hbm, run_ref),
            (edge_hbm, edge_ref),
        ],
        sems,
    )
    for copy in copies[:2]:
        copy.wait()
    route(routes_ref, weight_ref, g_ref, c_ref)
    for copy in copies[2:]:
        copy.wait()
    tokens, channels = gate_ref.shape
    steps = tokens // LANES
    block = 16
    per = steps // block

    def put(i, _):
        rows = pl.ds(pl.multiple_of(i * block, block), block)
        chunk = i // per
        source = pl.ds(chunk + (i % per) * (block * LANES), block, stride=LANES)
        gate = jax.nn.gelu(gate_ref[rows, :].astype(F32), approximate=True)
        enter, scale = edge_ref[0, pl.ds(chunk, 1), :], edge_ref[1, pl.ds(chunk, 1), :]
        for c in range(channels // 128):
            cols = slice(c * 128, (c + 1) * 128)
            run = run_ref[1, c, source, :]
            mixed_ref[0, rows, cols] = (run_ref[0, c, source, :] + run * enter[:, cols]) * gate[:, cols]
            mixed_ref[1, rows, cols] = run * scale[:, cols] * gate[:, cols]
        return 0

    pairs = [(g_ref, g_hbm), (c_ref, c_hbm)]
    sent = fetch(pairs, outs)
    quarter = tokens // 4
    for part in range(4):
        lax.fori_loop(part * quarter // block, (part + 1) * quarter // block, put, 0)
        rows = pl.ds(part * quarter, quarter)
        copy = pltpu.make_async_copy(
            mixed_ref.at[:, rows, :], mixed_hbm.at[pl.ds(0, 2), rows, :], outs.at[2 + part]
        )
        copy.start()
        sent.append(copy)
    for copy in sent:
        copy.wait()


def mix_kernel(
    index_ref, seen_ref, mixed_hbm, w_hbm, mine_ref, theirs_ref, w_ref, mixed_ref, sems
):
    _, tokens, channels = mixed_ref.shape
    here, side = index_ref[0], index_ref[1]
    depth = w_ref.shape[0]
    cut = depth // PIECES
    pairs = []
    for j in range(4):
        rows = pl.ds(j * (tokens // 4), tokens // 4)
        pairs.append((mixed_hbm.at[pl.ds(0, 2), rows, :], mixed_ref.at[:, rows, :]))
    for j in range(PIECES):
        rows = pl.ds(pl.multiple_of(side * depth + j * cut, cut), cut)
        pairs.append((w_hbm.at[rows, :], w_ref.at[pl.ds(j * cut, cut), :]))
    copies = fetch(pairs, sems)
    carried = jnp.zeros((LANES, 128), F32)
    for i in range(seen_ref.shape[0]):
        pair = seen_ref[i].astype(F32)
        carried = jnp.where(i < here, jnp.exp(pair[:LANES]) * carried + pair[LANES:], carried)
    carried = jnp.concatenate([carried[i : i + 1] for i in range(LANES)], axis=1)
    half = tokens // 2
    block = 16
    for copy in copies[:4]:
        copy.wait()

    def put(i, _):
        at = pl.multiple_of(i * block, block)
        for ref, part in ((theirs_ref, 1 - side), (mine_ref, side)):
            rows = pl.ds(pl.multiple_of(part * half + at, block), block)
            ref[pl.ds(at, block), :] = (mixed_ref[0, rows, :] + mixed_ref[1, rows, :] * carried).astype(
                BF16
            )
        return 0

    lax.fori_loop(0, half // block, put, 0, unroll=2)
    for copy in copies[4:]:
        copy.wait()


def route(routes_ref, weight_ref, g_ref, c_ref):
    fanout, rows = routes_ref.shape
    slots = g_ref.shape[0]
    experts = slots // CAP
    expert = lax.broadcasted_iota(jnp.int32, (experts, rows), 0)
    member = jnp.zeros((experts, rows), F32)
    weight = jnp.zeros((experts, rows), F32)
    for k in range(fanout):
        hit = expert == routes_ref[pl.ds(k, 1), :]
        member = member + jnp.where(hit, 1.0, 0.0)
        weight = weight + jnp.where(hit, weight_ref[pl.ds(k, 1), :], 0.0)
    earlier = (
        lax.broadcasted_iota(jnp.int32, (rows, rows), 0)
        < lax.broadcasted_iota(jnp.int32, (rows, rows), 1)
    )
    rank = jnp.dot(
        member.astype(BF16), jnp.where(earlier, 1.0, 0.0).astype(BF16), preferred_element_type=F32
    )
    rank = jnp.where(member > 0.0, rank, -1.0).astype(BF16)
    high = weight.astype(BF16)
    low = (weight - high.astype(F32)).astype(BF16)
    slot = lax.broadcasted_iota(jnp.int32, (BLOCK, experts), 0)
    spread_at = lax.broadcasted_iota(jnp.int32, (BLOCK, experts), 1)
    place = (lax.broadcasted_iota(jnp.int32, (BLOCK, rows), 0) % CAP).astype(F32)
    for b in range(slots // BLOCK):
        spread = jnp.where((slot + b * BLOCK) // CAP == spread_at, 1.0, 0.0).astype(BF16)

        def to_slots(values):
            return jnp.dot(spread, values, preferred_element_type=F32)

        chosen = to_slots(rank) == place
        g_ref[pl.ds(b * BLOCK, BLOCK), :] = jnp.where(chosen, 1.0, 0.0).astype(BF16)
        cols = slice(b * BLOCK, (b + 1) * BLOCK)
        c_ref[:rows, cols] = jnp.transpose(jnp.where(chosen, to_slots(high), 0.0)).astype(BF16)
        c_ref[rows:, cols] = jnp.transpose(jnp.where(chosen, to_slots(low), 0.0)).astype(BF16)


def project_kernel(index_ref, mine_ref, res_ref, own_ref, w_hbm, out_ref, rest_ref, sems):
    depth = mine_ref.shape[1]
    cut = depth // PIECES
    pairs = []
    for j in range(PIECES):
        rows = pl.ds(pl.multiple_of((1 - index_ref[1]) * depth + j * cut, cut), cut)
        pairs.append((w_hbm.at[rows, :], rest_ref.at[pl.ds(j * cut, cut), :]))
    copies = fetch(pairs, sems)
    out_ref[...] = ALPHA * res_ref[...].astype(F32) + jnp.dot(
        mine_ref[...], own_ref[...], preferred_element_type=F32
    )
    for copy in copies:
        copy.wait()


def dispatch_kernel(other_ref, w_ref, acc_ref, gain_ref, g_ref, normed_ref, out_ref):
    values = acc_ref[...] + jnp.dot(other_ref[...], w_ref[...], preferred_element_type=F32)
    normed = layer_norm(values, gain_ref[...]).astype(BF16)
    normed_ref[...] = normed

    out_ref[...] = jnp.dot(g_ref[...], normed, preferred_element_type=F32).astype(BF16)


def hidden_of(x, gate, up):
    return (
        jax.nn.silu(jnp.dot(x, gate, preferred_element_type=F32))
        * jnp.dot(x, up, preferred_element_type=F32)
    ).astype(BF16)


def shared_kernel(x_ref, gate_ref, up_ref, down_ref, out_ref):
    x = x_ref[...]
    hidden = hidden_of(x, gate_ref[...], up_ref[...])
    out_ref[...] = ALPHA * x.astype(F32) + jnp.dot(
        hidden, down_ref[...], preferred_element_type=F32
    )


def expert_kernel(x_ref, gate_ref, up_ref, down_ref, out_ref):
    block = 2 * BLOCK

    def step(i, _):
        rows = pl.ds(pl.multiple_of(i * block, block), block)
        hidden = hidden_of(x_ref[rows, :], gate_ref[0], up_ref[0])
        out_ref[rows, :] = jnp.dot(hidden, down_ref[0], preferred_element_type=F32).astype(BF16)
        return 0

    lax.fori_loop(0, x_ref.shape[0] // block, step, 0)


def finish_kernel(base_ref, c_ref, back_ref, gain_ref, out_ref, acc):
    rows = base_ref.shape[0]
    width = 512
    for j in range(base_ref.shape[1] // width):
        cols = slice(j * width, (j + 1) * width)
        part = jnp.dot(c_ref[...], back_ref[:, cols], preferred_element_type=F32)
        acc[:, cols] = base_ref[:, cols] + part[:rows] + part[rows:]
    out_ref[...] = layer_norm(acc[...], gain_ref[...]).astype(BF16)


def on_device(
    gate_pre, conv_in, conv_taps, recur_map, input_map, rate_logit, decay_shift, out_weight,
    residual, gain_mix, routes, route_weight, shared_gate, shared_up, shared_down, expert_gate,
    expert_up, expert_down, gain_out,
):
    tokens, channels = conv_in.shape
    reach = conv_taps.shape[0] - 1
    sp, tp = lax.axis_size("sp"), lax.axis_size("tp")
    experts = sp * tp
    rows = tokens // tp
    model = out_weight.shape[1]
    slots = experts * CAP
    sem = pltpu.SemaphoreType.DMA
    index = jnp.stack([lax.axis_index("sp"), lax.axis_index("tp")]).astype(jnp.int32)
    before = lax.ppermute(conv_in[tokens - reach :], "sp", [(i, i + 1) for i in range(sp - 1)])
    before, index = lax.optimization_barrier((before, index))
    padded = shape((8, tokens, channels), F32)
    big = pltpu.VMEM((tokens, channels), F32)
    apart = tokens + 8 * LANES
    lanes = pltpu.VMEM((channels // 128, apart, 128), F32)

    def staged(kernel, first, operands, made, flops, scratch, name):
        held = [
            pltpu.VMEM((2,) + x.shape[1:] if x is padded else x.shape, x.dtype)
            for x in tuple(operands) + made
        ]
        return call(
            kernel,
            made,
            [VMEM] * len(first) + [HBM] * len(operands),
            flops,
            held + scratch,
            name=name,
            out_specs=(HBM,) * len(made),
            limit=62,
        )(*first, *operands)

    totals, local, edge = staged(
        scan_kernel,
        (before,),
        (conv_in, conv_taps, recur_map, input_map, rate_logit[None], decay_shift.T),
        (
            shape((sp, 2 * LANES, 128), BF16),
            shape((2, channels // 128, tokens, 128), F32),
            shape((2, LANES, channels), F32),
        ),
        10**9,
        [lanes, big, big, big, pltpu.VMEM((apart, 128), F32), sem((6,)), sem((6,))],
        "scan",
    )
    seen = lax.all_to_all(totals, "sp", 0, 0, tiled=True)
    parts, g, c = staged(
        side_kernel,
        (),
        (gate_pre, routes.T, route_weight.T, local, edge),
        (padded, shape((slots, rows), BF16), shape((2 * rows, slots), BF16)),
        10**10,
        [sem((5,)), sem((6,))],
        "side",
    )
    piece = shape((rows, channels), BF16)
    strip = shape((channels, model), BF16)
    mine, theirs, own = call(
        mix_kernel,
        (piece, piece, strip),
        [SMEM, VMEM, HBM, HBM],
        10**8,
        [pltpu.VMEM((2, tokens, channels), F32), sem((4 + PIECES,))],
        name="mix",
        limit=46,
    )(index, seen, parts, out_weight)
    other = lax.ppermute(theirs, "tp", [(0, 1), (1, 0)])
    wide = shape((rows, model), F32)
    acc, rest = call(
        project_kernel,
        (wide, strip),
        [SMEM, VMEM, VMEM, VMEM, HBM],
        10**9,
        [sem((PIECES,))],
        name="project",
        limit=40,
    )(index, mine, residual, own, out_weight)
    normed, outgoing = call(
        dispatch_kernel,
        (shape((rows, model), BF16), shape((slots, model), BF16)),
        [VMEM] * 5,
        2 * 10**9,
        name="dispatch",
        limit=24,
    )(other, rest, acc, gain_mix[None], g)

    def exchanged(x):
        x = x.reshape(experts, CAP, model)
        x = lax.all_to_all(x, ("sp", "tp"), split_axis=0, concat_axis=0, tiled=True)
        return x.reshape(slots, model)

    received = exchanged(outgoing)
    results = call(
        expert_kernel, shape((slots, model), BF16), [VMEM] * 4, 6 * 10**9, name="expert", limit=24
    )(received, expert_gate, expert_up, expert_down)
    normed, results = lax.optimization_barrier((normed, results))
    base = call(shared_kernel, wide, [VMEM] * 4, 10**10, name="shared")(
        normed, shared_gate, shared_up, shared_down
    )
    base, results = lax.optimization_barrier((base, results))
    back = exchanged(results)
    return call(
        finish_kernel,
        shape((rows, model), BF16),
        [VMEM] * 4,
        10**9,
        [pltpu.VMEM((rows, model), F32)],
        name="finish",
    )(base, c, back, gain_out[None])


def solution(mesh):
    return jax.shard_map(
        on_device,
        mesh=mesh,
        in_specs=(
            P("sp", "tp"),
            P("sp", "tp"),
            P(None, "tp"),
            P("tp", None, None),
            P("tp", None, None),
            P("tp"),
            P("sp", "tp"),
            P(),
            P(("sp", "tp"), None),
            P(),
            P(("sp", "tp"), None),
            P(("sp", "tp"), None),
            P(),
            P(),
            P(),
            P(("sp", "tp"), None, None),
            P(("sp", "tp"), None, None),
            P(("sp", "tp"), None, None),
            P(),
        ),
        out_specs=P(("sp", "tp"), None),
        check_vma=False,
    )
```

```python
import functools

import jax
import jax.numpy as jnp
from jax import lax
from jax.experimental import pallas as pl
from jax.experimental.pallas import tpu as pltpu
from jax.sharding import PartitionSpec as P

ALPHA = 8.0**0.25
RATE_C = 8.0
NORM_EPS = 1e-05
TINY = 1e-36
CAP = 8
BLOCK = 256
LANES = 8
F32 = jnp.float32
BF16 = jnp.bfloat16
VMEM = pl.BlockSpec(memory_space=pltpu.VMEM)
HBM = pl.BlockSpec(memory_space=pltpu.HBM)


def call(
    kernel, out_shape, in_specs, flops, scratch=(), name=None, out_specs=None, grid=(), limit=16
):
    if out_specs is None:
        out_specs = jax.tree.map(lambda _: VMEM, out_shape)
    return pl.pallas_call(
        kernel,
        out_shape=out_shape,
        in_specs=in_specs,
        out_specs=out_specs,
        grid=grid,
        scratch_shapes=list(scratch),
        compiler_params=pltpu.CompilerParams(vmem_limit_bytes=limit * 2**20),
        cost_estimate=pl.CostEstimate(flops=flops, bytes_accessed=2**20, transcendentals=0),
        name=name,
    )


def shape(dims, dtype):
    return jax.ShapeDtypeStruct(dims, dtype)


def log1p_unit(u):
    s = u / (2.0 + u)
    q = s * s
    total = jnp.full_like(s, 1.0 / 17.0)
    for k in (15, 13, 11, 9, 7, 5, 3, 1):
        total = total * q + 1.0 / k
    return 2.0 * s * total


def minus_expm1_twice(x, decay):
    y = 2.0 * x
    total = jnp.full_like(y, 1.0 / 720.0)
    for k in (120, 24, 6, 2, 1):
        total = total * y + 1.0 / k
    return jnp.where(y > -0.125, -y * total, 1.0 - decay * decay)


def sigmoid(x):
    return 0.5 * jnp.tanh(0.5 * x) + 0.5


def layer_norm(values, gains):
    center = values - jnp.mean(values, axis=-1, keepdims=True)
    spread = jnp.mean(center * center, axis=-1, keepdims=True)
    return center * lax.rsqrt(spread + NORM_EPS) * gains


def fetch(pairs, sems):
    copies = [pltpu.make_async_copy(a, b, sems.at[i]) for i, (a, b) in enumerate(pairs)]
    for copy in copies:
        copy.start()
    return copies


def elements(conv, recur, gain, slope, moved):
    log_decay = slope * sigmoid(recur) + moved
    decay = jnp.exp(log_decay)
    power = minus_expm1_twice(log_decay, decay)
    return decay, power * lax.rsqrt(jnp.maximum(power, TINY)) * sigmoid(gain) * conv


def scan_kernel(
    halo_hbm, x_hbm, taps_hbm, rmap_hbm, imap_hbm, rate_hbm, shift_hbm, tot_hbm, run_hbm, edge_hbm,
    halo_ref, x_ref, taps_ref, rmap_ref, imap_ref, rate_ref, shift_ref, tot_ref, run_ref, edge_ref,
    ext, cv, rg, ig, sh, sems, outs,
):
    copies = fetch(
        [
            (x_hbm, x_ref),
            (taps_hbm, taps_ref),
            (halo_hbm, halo_ref),
            (shift_hbm, shift_ref),
            (rate_hbm, rate_ref),
            (rmap_hbm, rmap_ref),
            (imap_hbm, imap_ref),
        ],
        sems,
    )
    tokens, channels = x_ref.shape
    steps = tokens // LANES
    stride = steps + 8
    heads, width = rmap_ref.shape[:2]
    reach = taps_ref.shape[0] - 1
    pad = 8 - reach
    for copy in copies[:3]:
        copy.wait()
    for c in range(channels // 128):
        cols = slice(c * 128, (c + 1) * 128)
        x = x_ref[:, cols].astype(F32)
        ext[c, pl.ds(pad, reach), :] = halo_ref[:, cols].astype(F32)
        for i in range(LANES):
            if i > 0:
                ext[c, pl.ds(stride * i, 8), :] = x[steps * i - 8 : steps * i]
            ext[c, pl.ds(stride * i + 8, steps), :] = x[steps * i : steps * (i + 1)]
        taps = [taps_ref[pl.ds(j, 1), cols].astype(F32) for j in range(reach + 1)]
        window = [ext[c, pl.ds(pad + j, LANES, stride=stride), :] for j in range(reach)]
        for t in range(steps):
            window.append(ext[c, pl.ds(8 + t, LANES, stride=stride), :])
            total = taps[0] * window[0]
            for j in range(1, reach + 1):
                total = total + taps[j] * window[j]
            window = window[1:]
            cv[pl.ds(t * LANES, LANES), cols] = total.astype(BF16).astype(F32)
    for copy in copies[3:]:
        copy.wait()
    for k in range(heads):
        cols = slice(k * width, (k + 1) * width)
        block = cv[:, cols].astype(BF16)
        rg[:, cols] = jnp.dot(block, rmap_ref[k], preferred_element_type=F32)
        ig[:, cols] = jnp.dot(block, imap_ref[k], preferred_element_type=F32)
    full = jnp.concatenate([shift_ref[...], jnp.zeros((128 - heads, tokens), F32)], axis=0)
    full = jnp.transpose(full)
    for i in range(LANES):
        sh[pl.ds(stride * i, steps), :] = full[steps * i : steps * (i + 1)]
    logit = -rate_ref[...]
    slope = -RATE_C * (jnp.maximum(logit, 0.0) + log1p_unit(jnp.exp(-jnp.abs(logit))))

    def step(t, carry):
        rows = pl.ds(pl.multiple_of(t * LANES, LANES), LANES)
        moved = sh[pl.ds(t, LANES, stride=stride), :]
        out = []
        for k in range(heads):
            h, run = carry[k]
            cols = slice(k * width, (k + 1) * width)
            decay, update = elements(
                cv[rows, cols], rg[rows, cols], ig[rows, cols], slope[:, cols], moved[:, k : k + 1]
            )
            h = decay * h + update
            run = decay * run
            for j in range(width // 128):
                lane = slice(j * 128, (j + 1) * 128)
                run_ref[0, k * (width // 128) + j, rows, :] = h[:, lane]
                run_ref[1, k * (width // 128) + j, rows, :] = run[:, lane]
            out.append((h, run))
        return tuple(out)

    last = tuple(
        (jnp.zeros((LANES, width), F32), jnp.ones((LANES, width), F32)) for _ in range(heads)
    )
    sent = []
    for part in range(4):
        span = steps // 4
        last = lax.fori_loop(part * span, (part + 1) * span, step, last, unroll=2)
        rows = pl.ds(part * span * LANES, span * LANES)
        copy = pltpu.make_async_copy(
            run_ref.at[:, :, rows, :], run_hbm.at[:, :, rows, :], outs.at[part]
        )
        copy.start()
        sent.append(copy)
    row = lax.broadcasted_iota(jnp.int32, (LANES, width), 0)
    ends = [[], []]
    for k in range(heads):
        cols = slice(k * width, (k + 1) * width)
        h, a = last[k]
        for d in (1, 2, 4):
            hp, ap = pltpu.roll(h, d, 0), pltpu.roll(a, d, 0)
            h = jnp.where(row >= d, a * hp + h, h)
            a = jnp.where(row >= d, a * ap, a)
        for j in range(width // 128):
            lane = slice(j * 128, (j + 1) * 128)
            ends[0].append(jnp.log(jnp.maximum(a[LANES - 1 :, lane], TINY)))
            ends[1].append(h[LANES - 1 :, lane])
        edge_ref[0, :, cols] = jnp.where(row >= 1, pltpu.roll(h, 1, 0), 0.0)
        edge_ref[1, :, cols] = jnp.where(row >= 1, pltpu.roll(a, 1, 0), 1.0)
    both = jnp.concatenate(ends[0] + ends[1], axis=0).astype(BF16)
    for i in range(tot_ref.shape[0]):
        tot_ref[i] = both
    sent += [
        pltpu.make_async_copy(tot_ref, tot_hbm, outs.at[4]),
        pltpu.make_async_copy(edge_ref, edge_hbm, outs.at[5]),
    ]
    for copy in sent[4:]:
        copy.start()
    for copy in sent:
        copy.wait()


def side_kernel(
    gate_hbm, routes_hbm, weight_hbm, run_hbm, edge_hbm, mixed_hbm, g_hbm, c_hbm,
    gate_ref, routes_ref, weight_ref, run_ref, edge_ref, mixed_ref, g_ref, c_ref, sems, outs,
):
    copies = fetch(
        [
            (routes_hbm, routes_ref),
            (weight_hbm, weight_ref),
            (gate_hbm, gate_ref),
            (run_hbm, run_ref),
            (edge_hbm, edge_ref),
        ],
        sems,
    )
    for copy in copies[:2]:
        copy.wait()
    route(routes_ref, weight_ref, g_ref, c_ref)
    for copy in copies[2:]:
        copy.wait()
    tokens, channels = gate_ref.shape
    steps = tokens // LANES
    block = 16
    per = steps // block

    def put(i, _):
        rows = pl.ds(pl.multiple_of(i * block, block), block)
        chunk = i // per
        source = pl.ds(chunk + (i % per) * (block * LANES), block, stride=LANES)
        gate = jax.nn.gelu(gate_ref[rows, :].astype(F32), approximate=True)
        enter, scale = edge_ref[0, pl.ds(chunk, 1), :], edge_ref[1, pl.ds(chunk, 1), :]
        for c in range(channels // 128):
            cols = slice(c * 128, (c + 1) * 128)
            run = run_ref[1, c, source, :]
            mixed_ref[0, rows, cols] = (run_ref[0, c, source, :] + run * enter[:, cols]) * gate[:, cols]
            mixed_ref[1, rows, cols] = run * scale[:, cols] * gate[:, cols]
        return 0

    pairs = [(g_ref, g_hbm), (c_ref, c_hbm)]
    sent = fetch(pairs, outs)
    quarter = tokens // 4
    for part in range(4):
        lax.fori_loop(part * quarter // block, (part + 1) * quarter // block, put, 0)
        rows = pl.ds(part * quarter, quarter)
        copy = pltpu.make_async_copy(
            mixed_ref.at[:, rows, :], mixed_hbm.at[pl.ds(0, 2), rows, :], outs.at[2 + part]
        )
        copy.start()
        sent.append(copy)
    for copy in sent:
        copy.wait()


def mix_kernel(
    seen_ref, mixed_hbm, w_hbm, mine_ref, theirs_ref, w_ref, mixed_ref, sems
):
    _, tokens, channels = mixed_ref.shape
    here, side = lax.axis_index("sp"), lax.axis_index("tp")
    half = tokens // 2
    strip = channels // 2
    pairs = []
    for j in range(4):
        rows = pl.ds(j * (tokens // 4), tokens // 4)
        pairs.append((mixed_hbm.at[pl.ds(0, 2), rows, :], mixed_ref.at[:, rows, :]))
    for j in range(3):
        at = (side if j < 2 else 1 - side) * channels + (j % 2) * strip
        at = pl.multiple_of(at, strip)
        pairs.append((w_hbm.at[pl.ds(at, strip), :], w_ref.at[pl.ds(j * strip, strip), :]))
    copies = fetch(pairs, sems)
    carried = jnp.zeros((LANES, 128), F32)
    for i in range(seen_ref.shape[0]):
        pair = seen_ref[i].astype(F32)
        carried = jnp.where(i < here, jnp.exp(pair[:LANES]) * carried + pair[LANES:], carried)
    carried = jnp.concatenate([carried[i : i + 1] for i in range(LANES)], axis=1)
    block = 16
    for copy in copies[:4]:
        copy.wait()

    def put(i, _):
        at = pl.multiple_of(i * block, block)
        for ref, part in ((theirs_ref, 1 - side), (mine_ref, side)):
            rows = pl.ds(pl.multiple_of(part * half + at, block), block)
            ref[pl.ds(at, block), :] = (mixed_ref[0, rows, :] + mixed_ref[1, rows, :] * carried).astype(
                BF16
            )
        return 0

    lax.fori_loop(0, half // block, put, 0, unroll=2)
    for copy in copies[4:]:
        copy.wait()


def route(routes_ref, weight_ref, g_ref, c_ref):
    fanout, rows = routes_ref.shape
    slots = g_ref.shape[0]
    experts = slots // CAP
    expert = lax.broadcasted_iota(jnp.int32, (experts, rows), 0)
    member = jnp.zeros((experts, rows), F32)
    weight = jnp.zeros((experts, rows), F32)
    for k in range(fanout):
        hit = expert == routes_ref[pl.ds(k, 1), :]
        member = member + jnp.where(hit, 1.0, 0.0)
        weight = weight + jnp.where(hit, weight_ref[pl.ds(k, 1), :], 0.0)
    earlier = (
        lax.broadcasted_iota(jnp.int32, (rows, rows), 0)
        < lax.broadcasted_iota(jnp.int32, (rows, rows), 1)
    )
    rank = jnp.dot(
        member.astype(BF16), jnp.where(earlier, 1.0, 0.0).astype(BF16), preferred_element_type=F32
    )
    rank = jnp.where(member > 0.0, rank, -1.0).astype(BF16)
    high = weight.astype(BF16)
    low = (weight - high.astype(F32)).astype(BF16)
    slot = lax.broadcasted_iota(jnp.int32, (BLOCK, experts), 0)
    spread_at = lax.broadcasted_iota(jnp.int32, (BLOCK, experts), 1)
    place = (lax.broadcasted_iota(jnp.int32, (BLOCK, rows), 0) % CAP).astype(F32)
    for b in range(slots // BLOCK):
        spread = jnp.where((slot + b * BLOCK) // CAP == spread_at, 1.0, 0.0).astype(BF16)

        def to_slots(values):
            return jnp.dot(spread, values, preferred_element_type=F32)

        chosen = to_slots(rank) == place
        g_ref[pl.ds(b * BLOCK, BLOCK), :] = jnp.where(chosen, 1.0, 0.0).astype(BF16)
        cols = slice(b * BLOCK, (b + 1) * BLOCK)
        c_ref[:rows, cols] = jnp.transpose(jnp.where(chosen, to_slots(high), 0.0)).astype(BF16)
        c_ref[rows:, cols] = jnp.transpose(jnp.where(chosen, to_slots(low), 0.0)).astype(BF16)


def project_kernel(mine_ref, res_ref, w_ref, w_hbm, out_ref, rest_ref, sems):
    depth = mine_ref.shape[1]
    half = depth // 2
    at = pl.multiple_of((1 - lax.axis_index("tp")) * depth + half, half)
    copies = fetch([(w_hbm.at[pl.ds(at, half), :], rest_ref)], sems)
    out_ref[...] = ALPHA * res_ref[...].astype(F32) + jnp.dot(
        mine_ref[...], w_ref[:depth], preferred_element_type=F32
    )
    copies[0].wait()


def dispatch_kernel(other_ref, w_ref, rest_ref, acc_ref, gain_ref, g_ref, normed_ref, out_ref):
    depth = other_ref.shape[1]
    values = (
        acc_ref[...]
        + jnp.dot(other_ref[:, : depth // 2], w_ref[depth:], preferred_element_type=F32)
        + jnp.dot(other_ref[:, depth // 2 :], rest_ref[...], preferred_element_type=F32)
    )
    normed = layer_norm(values, gain_ref[...]).astype(BF16)
    normed_ref[...] = normed

    out_ref[...] = jnp.dot(g_ref[...], normed, preferred_element_type=F32).astype(BF16)


def hidden_of(x, gate, up):
    return (
        jax.nn.silu(jnp.dot(x, gate, preferred_element_type=F32))
        * jnp.dot(x, up, preferred_element_type=F32)
    ).astype(BF16)


def shared_kernel(x_ref, gate_ref, up_ref, down_ref, out_ref):
    x = x_ref[...]
    hidden = hidden_of(x, gate_ref[...], up_ref[...])
    out_ref[...] = ALPHA * x.astype(F32) + jnp.dot(
        hidden, down_ref[...], preferred_element_type=F32
    )


def expert_kernel(x_ref, gate_ref, up_ref, down_ref, out_ref):
    block = 2 * BLOCK

    def step(i, _):
        rows = pl.ds(pl.multiple_of(i * block, block), block)
        hidden = hidden_of(x_ref[rows, :], gate_ref[0], up_ref[0])
        out_ref[rows, :] = jnp.dot(hidden, down_ref[0], preferred_element_type=F32).astype(BF16)
        return 0

    lax.fori_loop(0, x_ref.shape[0] // block, step, 0)


def finish_kernel(base_ref, c_ref, back_ref, gain_ref, out_ref, acc):
    rows = base_ref.shape[0]
    width = 512
    for j in range(base_ref.shape[1] // width):
        cols = slice(j * width, (j + 1) * width)
        part = jnp.dot(c_ref[...], back_ref[:, cols], preferred_element_type=F32)
        acc[:, cols] = base_ref[:, cols] + part[:rows] + part[rows:]
    out_ref[...] = layer_norm(acc[...], gain_ref[...]).astype(BF16)


def on_device(
    gate_pre, conv_in, conv_taps, recur_map, input_map, rate_logit, decay_shift, out_weight,
    residual, gain_mix, routes, route_weight, shared_gate, shared_up, shared_down, expert_gate,
    expert_up, expert_down, gain_out,
):
    tokens, channels = conv_in.shape
    reach = conv_taps.shape[0] - 1
    sp, tp = lax.axis_size("sp"), lax.axis_size("tp")
    experts = sp * tp
    rows = tokens // tp
    model = out_weight.shape[1]
    slots = experts * CAP
    sem = pltpu.SemaphoreType.DMA
    before = lax.ppermute(conv_in[tokens - reach :], "sp", [(i, i + 1) for i in range(sp - 1)])
    padded = shape((8, tokens, channels), F32)
    big = pltpu.VMEM((tokens, channels), F32)
    apart = tokens + 8 * LANES
    lanes = pltpu.VMEM((channels // 128, apart, 128), F32)

    def staged(kernel, operands, made, flops, scratch, name):
        held = [
            pltpu.VMEM((2,) + x.shape[1:] if x is padded else x.shape, x.dtype)
            for x in tuple(operands) + made
        ]
        return call(
            kernel,
            made,
            [HBM] * len(operands),
            flops,
            held + scratch,
            name=name,
            out_specs=(HBM,) * len(made),
            limit=62,
        )(*operands)

    totals, local, edge = staged(
        scan_kernel,
        (before, conv_in, conv_taps, recur_map, input_map, rate_logit[None], decay_shift.T),
        (
            shape((sp, 2 * LANES, 128), BF16),
            shape((2, channels // 128, tokens, 128), F32),
            shape((2, LANES, channels), F32),
        ),
        10**9,
        [lanes, big, big, big, pltpu.VMEM((apart, 128), F32), sem((7,)), sem((6,))],
        "scan",
    )
    seen = lax.all_to_all(totals, "sp", 0, 0, tiled=True)
    parts, g, c = staged(
        side_kernel,
        (gate_pre, routes.T, route_weight.T, local, edge),
        (padded, shape((slots, rows), BF16), shape((2 * rows, slots), BF16)),
        10**10,
        [sem((5,)), sem((6,))],
        "side",
    )
    piece = shape((rows, channels), BF16)
    mine, theirs, most = call(
        mix_kernel,
        (piece, piece, shape((3 * channels // 2, model), BF16)),
        [VMEM, HBM, HBM],
        10**8,
        [pltpu.VMEM((2, tokens, channels), F32), sem((7,))],
        name="mix",
        limit=44,
    )(seen, parts, out_weight)
    other = lax.ppermute(theirs, "tp", [(0, 1), (1, 0)])
    wide = shape((rows, model), F32)
    acc, rest = call(
        project_kernel,
        (wide, shape((channels // 2, model), BF16)),
        [VMEM, VMEM, VMEM, HBM],
        10**9,
        [sem((1,))],
        name="project",
        limit=40,
    )(mine, residual, most, out_weight)
    normed, outgoing = call(
        dispatch_kernel,
        (shape((rows, model), BF16), shape((slots, model), BF16)),
        [VMEM] * 6,
        2 * 10**9,
        name="dispatch",
        limit=24,
    )(other, most, rest, acc, gain_mix[None], g)

    def exchanged(x):
        x = x.reshape(experts, CAP, model)
        x = lax.all_to_all(x, ("sp", "tp"), split_axis=0, concat_axis=0, tiled=True)
        return x.reshape(slots, model)

    received = exchanged(outgoing)
    results = call(
        expert_kernel, shape((slots, model), BF16), [VMEM] * 4, 6 * 10**9, name="expert", limit=24
    )(received, expert_gate, expert_up, expert_down)
    normed, results = lax.optimization_barrier((normed, results))
    base = call(shared_kernel, wide, [VMEM] * 4, 10**10, name="shared")(
        normed, shared_gate, shared_up, shared_down
    )
    base, results = lax.optimization_barrier((base, results))
    back = exchanged(results)
    return call(
        finish_kernel,
        shape((rows, model), BF16),
        [VMEM] * 4,
        10**9,
        [pltpu.VMEM((rows, model), F32)],
        name="finish",
    )(base, c, back, gain_out[None])


def solution(mesh):
    return jax.shard_map(
        on_device,
        mesh=mesh,
        in_specs=(
            P("sp", "tp"),
            P("sp", "tp"),
            P(None, "tp"),
            P("tp", None, None),
            P("tp", None, None),
            P("tp"),
            P("sp", "tp"),
            P(),
            P(("sp", "tp"), None),
            P(),
            P(("sp", "tp"), None),
            P(("sp", "tp"), None),
            P(),
            P(),
            P(),
            P(("sp", "tp"), None, None),
            P(("sp", "tp"), None, None),
            P(("sp", "tp"), None, None),
            P(),
        ),
        out_specs=P(("sp", "tp"), None),
        check_vma=False,
    )
```

```python
import functools

import jax
import jax.numpy as jnp
from jax import lax
from jax.experimental import pallas as pl
from jax.experimental.pallas import tpu as pltpu
from jax.sharding import PartitionSpec as P

ALPHA = 8.0**0.25
RATE_C = 8.0
NORM_EPS = 1e-05
TINY = 1e-36
CAP = 8
BLOCK = 256
LANES = 8
F32 = jnp.float32
BF16 = jnp.bfloat16
VMEM = pl.BlockSpec(memory_space=pltpu.VMEM)
HBM = pl.BlockSpec(memory_space=pltpu.HBM)


def call(
    kernel, out_shape, in_specs, flops, scratch=(), name=None, out_specs=None, grid=(), limit=16
):
    if out_specs is None:
        out_specs = jax.tree.map(lambda _: VMEM, out_shape)
    return pl.pallas_call(
        kernel,
        out_shape=out_shape,
        in_specs=in_specs,
        out_specs=out_specs,
        grid=grid,
        scratch_shapes=list(scratch),
        compiler_params=pltpu.CompilerParams(vmem_limit_bytes=limit * 2**20),
        cost_estimate=pl.CostEstimate(flops=flops, bytes_accessed=2**20, transcendentals=0),
        name=name,
    )


def shape(dims, dtype):
    return jax.ShapeDtypeStruct(dims, dtype)


def log1p_unit(u):
    s = u / (2.0 + u)
    q = s * s
    total = jnp.full_like(s, 1.0 / 17.0)
    for k in (15, 13, 11, 9, 7, 5, 3, 1):
        total = total * q + 1.0 / k
    return 2.0 * s * total


def minus_expm1_twice(x, decay):
    y = 2.0 * x
    total = jnp.full_like(y, 1.0 / 720.0)
    for k in (120, 24, 6, 2, 1):
        total = total * y + 1.0 / k
    return jnp.where(y > -0.125, -y * total, 1.0 - decay * decay)


def sigmoid(x):
    return 0.5 * jnp.tanh(0.5 * x) + 0.5


def layer_norm(values, gains):
    center = values - jnp.mean(values, axis=-1, keepdims=True)
    spread = jnp.mean(center * center, axis=-1, keepdims=True)
    return center * lax.rsqrt(spread + NORM_EPS) * gains


def fetch(pairs, sems):
    copies = [pltpu.make_async_copy(a, b, sems.at[i]) for i, (a, b) in enumerate(pairs)]
    for copy in copies:
        copy.start()
    return copies


def elements(conv, recur, gain, slope, moved):
    log_decay = slope * sigmoid(recur) + moved
    decay = jnp.exp(log_decay)
    power = minus_expm1_twice(log_decay, decay)
    return decay, power * lax.rsqrt(jnp.maximum(power, TINY)) * sigmoid(gain) * conv


def scan_kernel(
    halo_hbm, x_hbm, taps_hbm, rmap_hbm, imap_hbm, rate_hbm, shift_hbm, tot_hbm, run_hbm, edge_hbm,
    halo_ref, x_ref, taps_ref, rmap_ref, imap_ref, rate_ref, shift_ref, tot_ref, run_ref, edge_ref,
    ext, cv, rg, ig, sh, sems, outs,
):
    copies = fetch(
        [
            (x_hbm, x_ref),
            (taps_hbm, taps_ref),
            (halo_hbm, halo_ref),
            (shift_hbm, shift_ref),
            (rate_hbm, rate_ref),
            (rmap_hbm, rmap_ref),
            (imap_hbm, imap_ref),
        ],
        sems,
    )
    tokens, channels = x_ref.shape
    steps = tokens // LANES
    stride = steps + 8
    heads, width = rmap_ref.shape[:2]
    reach = taps_ref.shape[0] - 1
    pad = 8 - reach
    for copy in copies[:3]:
        copy.wait()
    for c in range(channels // 128):
        cols = slice(c * 128, (c + 1) * 128)
        x = x_ref[:, cols].astype(F32)
        ext[c, pl.ds(pad, reach), :] = halo_ref[:, cols].astype(F32)
        for i in range(LANES):
            if i > 0:
                ext[c, pl.ds(stride * i, 8), :] = x[steps * i - 8 : steps * i]
            ext[c, pl.ds(stride * i + 8, steps), :] = x[steps * i : steps * (i + 1)]
        taps = [taps_ref[pl.ds(j, 1), cols].astype(F32) for j in range(reach + 1)]
        window = [ext[c, pl.ds(pad + j, LANES, stride=stride), :] for j in range(reach)]
        for t in range(steps):
            window.append(ext[c, pl.ds(8 + t, LANES, stride=stride), :])
            total = taps[0] * window[0]
            for j in range(1, reach + 1):
                total = total + taps[j] * window[j]
            window = window[1:]
            cv[pl.ds(t * LANES, LANES), cols] = total.astype(BF16).astype(F32)
    for copy in copies[3:]:
        copy.wait()
    for k in range(heads):
        cols = slice(k * width, (k + 1) * width)
        block = cv[:, cols].astype(BF16)
        rg[:, cols] = jnp.dot(block, rmap_ref[k], preferred_element_type=F32)
        ig[:, cols] = jnp.dot(block, imap_ref[k], preferred_element_type=F32)
    full = jnp.concatenate([shift_ref[...], jnp.zeros((128 - heads, tokens), F32)], axis=0)
    full = jnp.transpose(full)
    for i in range(LANES):
        sh[pl.ds(stride * i, steps), :] = full[steps * i : steps * (i + 1)]
    logit = -rate_ref[...]
    slope = -RATE_C * (jnp.maximum(logit, 0.0) + log1p_unit(jnp.exp(-jnp.abs(logit))))

    def step(t, carry):
        rows = pl.ds(pl.multiple_of(t * LANES, LANES), LANES)
        moved = sh[pl.ds(t, LANES, stride=stride), :]
        out = []
        for k in range(heads):
            h, run = carry[k]
            cols = slice(k * width, (k + 1) * width)
            decay, update = elements(
                cv[rows, cols], rg[rows, cols], ig[rows, cols], slope[:, cols], moved[:, k : k + 1]
            )
            h = decay * h + update
            run = decay * run
            for j in range(width // 128):
                lane = slice(j * 128, (j + 1) * 128)
                run_ref[0, k * (width // 128) + j, rows, :] = h[:, lane]
                run_ref[1, k * (width // 128) + j, rows, :] = run[:, lane]
            out.append((h, run))
        return tuple(out)

    last = tuple(
        (jnp.zeros((LANES, width), F32), jnp.ones((LANES, width), F32)) for _ in range(heads)
    )
    sent = []
    for part in range(4):
        span = steps // 4
        last = lax.fori_loop(part * span, (part + 1) * span, step, last, unroll=2)
        rows = pl.ds(part * span * LANES, span * LANES)
        copy = pltpu.make_async_copy(
            run_ref.at[:, :, rows, :], run_hbm.at[:, :, rows, :], outs.at[part]
        )
        copy.start()
        sent.append(copy)
    row = lax.broadcasted_iota(jnp.int32, (LANES, width), 0)
    ends = [[], []]
    for k in range(heads):
        cols = slice(k * width, (k + 1) * width)
        h, a = last[k]
        for d in (1, 2, 4):
            hp, ap = pltpu.roll(h, d, 0), pltpu.roll(a, d, 0)
            h = jnp.where(row >= d, a * hp + h, h)
            a = jnp.where(row >= d, a * ap, a)
        for j in range(width // 128):
            lane = slice(j * 128, (j + 1) * 128)
            ends[0].append(jnp.log(jnp.maximum(a[LANES - 1 :, lane], TINY)))
            ends[1].append(h[LANES - 1 :, lane])
        edge_ref[0, :, cols] = jnp.where(row >= 1, pltpu.roll(h, 1, 0), 0.0)
        edge_ref[1, :, cols] = jnp.where(row >= 1, pltpu.roll(a, 1, 0), 1.0)
    both = jnp.concatenate(ends[0] + ends[1], axis=0).astype(BF16)
    for i in range(tot_ref.shape[0]):
        tot_ref[i] = both
    sent += [
        pltpu.make_async_copy(tot_ref, tot_hbm, outs.at[4]),
        pltpu.make_async_copy(edge_ref, edge_hbm, outs.at[5]),
    ]
    for copy in sent[4:]:
        copy.start()
    for copy in sent:
        copy.wait()


def side_kernel(
    gate_hbm, routes_hbm, weight_hbm, run_hbm, edge_hbm, mixed_hbm, g_hbm, c_hbm,
    gate_ref, routes_ref, weight_ref, run_ref, edge_ref, mixed_ref, g_ref, c_ref, sems, outs,
):
    copies = fetch(
        [
            (routes_hbm, routes_ref),
            (weight_hbm, weight_ref),
            (gate_hbm, gate_ref),
            (run_hbm, run_ref),
            (edge_hbm, edge_ref),
        ],
        sems,
    )
    for copy in copies[:2]:
        copy.wait()
    route(routes_ref, weight_ref, g_ref, c_ref)
    for copy in copies[2:]:
        copy.wait()
    tokens, channels = gate_ref.shape
    steps = tokens // LANES
    block = 16
    per = steps // block

    def put(i, _):
        rows = pl.ds(pl.multiple_of(i * block, block), block)
        chunk = i // per
        source = pl.ds(chunk + (i % per) * (block * LANES), block, stride=LANES)
        gate = jax.nn.gelu(gate_ref[rows, :].astype(F32), approximate=True)
        enter, scale = edge_ref[0, pl.ds(chunk, 1), :], edge_ref[1, pl.ds(chunk, 1), :]
        for c in range(channels // 128):
            cols = slice(c * 128, (c + 1) * 128)
            run = run_ref[1, c, source, :]
            mixed_ref[0, rows, cols] = (run_ref[0, c, source, :] + run * enter[:, cols]) * gate[:, cols]
            mixed_ref[1, rows, cols] = run * scale[:, cols] * gate[:, cols]
        return 0

    pairs = [(g_ref, g_hbm), (c_ref, c_hbm)]
    sent = fetch(pairs, outs)
    quarter = tokens // 4
    for part in range(4):
        lax.fori_loop(part * quarter // block, (part + 1) * quarter // block, put, 0)
        rows = pl.ds(part * quarter, quarter)
        copy = pltpu.make_async_copy(
            mixed_ref.at[:, rows, :], mixed_hbm.at[pl.ds(0, 2), rows, :], outs.at[2 + part]
        )
        copy.start()
        sent.append(copy)
    for copy in sent:
        copy.wait()


def mix_kernel(
    seen_ref, mixed_hbm, w_hbm, mine_ref, theirs_ref, w_ref, mixed_ref, sems
):
    _, tokens, channels = mixed_ref.shape
    here, side = lax.axis_index("sp"), lax.axis_index("tp")
    half = tokens // 2
    strip = channels // 2
    pairs = []
    for j in range(4):
        rows = pl.ds(j * (tokens // 4), tokens // 4)
        pairs.append((mixed_hbm.at[pl.ds(0, 2), rows, :], mixed_ref.at[:, rows, :]))
    for j in range(3):
        at = (side if j < 2 else 1 - side) * channels + (j % 2) * strip
        at = pl.multiple_of(at, strip)
        pairs.append((w_hbm.at[pl.ds(at, strip), :], w_ref.at[pl.ds(j * strip, strip), :]))
    copies = fetch(pairs, sems)
    carried = jnp.zeros((LANES, 128), F32)
    for i in range(seen_ref.shape[0]):
        pair = seen_ref[i].astype(F32)
        carried = jnp.where(i < here, jnp.exp(pair[:LANES]) * carried + pair[LANES:], carried)
    carried = jnp.concatenate([carried[i : i + 1] for i in range(LANES)], axis=1)
    block = 16
    for copy in copies[:4]:
        copy.wait()

    def put(i, _):
        at = pl.multiple_of(i * block, block)
        for ref, part in ((theirs_ref, 1 - side), (mine_ref, side)):
            rows = pl.ds(pl.multiple_of(part * half + at, block), block)
            ref[pl.ds(at, block), :] = (mixed_ref[0, rows, :] + mixed_ref[1, rows, :] * carried).astype(
                BF16
            )
        return 0

    lax.fori_loop(0, half // block, put, 0, unroll=2)
    for copy in copies[4:]:
        copy.wait()


def route(routes_ref, weight_ref, g_ref, c_ref):
    fanout, rows = routes_ref.shape
    slots = g_ref.shape[0]
    experts = slots // CAP
    expert = lax.broadcasted_iota(jnp.int32, (experts, rows), 0)
    member = jnp.zeros((experts, rows), F32)
    weight = jnp.zeros((experts, rows), F32)
    for k in range(fanout):
        hit = expert == routes_ref[pl.ds(k, 1), :]
        member = member + jnp.where(hit, 1.0, 0.0)
        weight = weight + jnp.where(hit, weight_ref[pl.ds(k, 1), :], 0.0)
    earlier = (
        lax.broadcasted_iota(jnp.int32, (rows, rows), 0)
        < lax.broadcasted_iota(jnp.int32, (rows, rows), 1)
    )
    rank = jnp.dot(
        member.astype(BF16), jnp.where(earlier, 1.0, 0.0).astype(BF16), preferred_element_type=F32
    )
    rank = jnp.where(member > 0.0, rank, -1.0).astype(BF16)
    weight = weight.astype(BF16)
    slot = lax.broadcasted_iota(jnp.int32, (BLOCK, experts), 0)
    spread_at = lax.broadcasted_iota(jnp.int32, (BLOCK, experts), 1)
    place = (lax.broadcasted_iota(jnp.int32, (BLOCK, rows), 0) % CAP).astype(F32)
    for b in range(slots // BLOCK):
        spread = jnp.where((slot + b * BLOCK) // CAP == spread_at, 1.0, 0.0).astype(BF16)

        def to_slots(values):
            return jnp.dot(spread, values, preferred_element_type=F32)

        chosen = to_slots(rank) == place
        g_ref[pl.ds(b * BLOCK, BLOCK), :] = jnp.where(chosen, 1.0, 0.0).astype(BF16)
        cols = slice(b * BLOCK, (b + 1) * BLOCK)
        c_ref[:, cols] = jnp.transpose(jnp.where(chosen, to_slots(weight), 0.0)).astype(BF16)


def project_kernel(mine_ref, res_ref, w_ref, w_hbm, out_ref, rest_ref, sems):
    depth = mine_ref.shape[1]
    half = depth // 2
    at = pl.multiple_of((1 - lax.axis_index("tp")) * depth + half, half)
    copies = fetch([(w_hbm.at[pl.ds(at, half), :], rest_ref)], sems)
    out_ref[...] = ALPHA * res_ref[...].astype(F32) + jnp.dot(
        mine_ref[...], w_ref[:depth], preferred_element_type=F32
    )
    copies[0].wait()


def dispatch_kernel(other_ref, w_ref, rest_ref, acc_ref, gain_ref, g_ref, normed_ref, out_ref):
    depth = other_ref.shape[1]
    values = (
        acc_ref[...]
        + jnp.dot(other_ref[:, : depth // 2], w_ref[depth:], preferred_element_type=F32)
        + jnp.dot(other_ref[:, depth // 2 :], rest_ref[...], preferred_element_type=F32)
    )
    normed = layer_norm(values, gain_ref[...]).astype(BF16)
    normed_ref[...] = normed

    out_ref[...] = jnp.dot(g_ref[...], normed, preferred_element_type=F32).astype(BF16)


def hidden_of(x, gate, up):
    return (
        jax.nn.silu(jnp.dot(x, gate, preferred_element_type=F32))
        * jnp.dot(x, up, preferred_element_type=F32)
    ).astype(BF16)


def expert_kernel(
    x_ref, gate_ref, up_ref, down_ref, own_ref, sgate_ref, sup_ref, sdown_ref, out_ref, base_ref
):
    block = 2 * BLOCK

    def step(i, _):
        rows = pl.ds(pl.multiple_of(i * block, block), block)
        hidden = hidden_of(x_ref[rows, :], gate_ref[0], up_ref[0])
        out_ref[rows, :] = jnp.dot(hidden, down_ref[0], preferred_element_type=F32).astype(BF16)
        return 0

    lax.fori_loop(0, x_ref.shape[0] // block, step, 0)
    x = own_ref[...]
    hidden = hidden_of(x, sgate_ref[...], sup_ref[...])
    base_ref[...] = ALPHA * x.astype(F32) + jnp.dot(
        hidden, sdown_ref[...], preferred_element_type=F32
    )


def finish_kernel(base_ref, c_ref, back_ref, gain_ref, out_ref):
    values = base_ref[...] + jnp.dot(c_ref[...], back_ref[...], preferred_element_type=F32)
    out_ref[...] = layer_norm(values, gain_ref[...]).astype(BF16)


def on_device(
    gate_pre, conv_in, conv_taps, recur_map, input_map, rate_logit, decay_shift, out_weight,
    residual, gain_mix, routes, route_weight, shared_gate, shared_up, shared_down, expert_gate,
    expert_up, expert_down, gain_out,
):
    tokens, channels = conv_in.shape
    reach = conv_taps.shape[0] - 1
    sp, tp = lax.axis_size("sp"), lax.axis_size("tp")
    experts = sp * tp
    rows = tokens // tp
    model = out_weight.shape[1]
    slots = experts * CAP
    sem = pltpu.SemaphoreType.DMA
    before = lax.ppermute(conv_in[tokens - reach :], "sp", [(i, i + 1) for i in range(sp - 1)])
    padded = shape((8, tokens, channels), F32)
    big = pltpu.VMEM((tokens, channels), F32)
    apart = tokens + 8 * LANES
    lanes = pltpu.VMEM((channels // 128, apart, 128), F32)

    def staged(kernel, operands, made, flops, scratch, name):
        held = [
            pltpu.VMEM((2,) + x.shape[1:] if x is padded else x.shape, x.dtype)
            for x in tuple(operands) + made
        ]
        return call(
            kernel,
            made,
            [HBM] * len(operands),
            flops,
            held + scratch,
            name=name,
            out_specs=(HBM,) * len(made),
            limit=62,
        )(*operands)

    totals, local, edge = staged(
        scan_kernel,
        (before, conv_in, conv_taps, recur_map, input_map, rate_logit[None], decay_shift.T),
        (
            shape((sp, 2 * LANES, 128), BF16),
            shape((2, channels // 128, tokens, 128), F32),
            shape((2, LANES, channels), F32),
        ),
        10**9,
        [lanes, big, big, big, pltpu.VMEM((apart, 128), F32), sem((7,)), sem((6,))],
        "scan",
    )
    seen = lax.all_to_all(totals, "sp", 0, 0, tiled=True)
    parts, g, c = staged(
        side_kernel,
        (gate_pre, routes.T, route_weight.T, local, edge),
        (padded, shape((slots, rows), BF16), shape((rows, slots), BF16)),
        10**10,
        [sem((5,)), sem((6,))],
        "side",
    )
    piece = shape((rows, channels), BF16)
    mine, theirs, most = call(
        mix_kernel,
        (piece, piece, shape((3 * channels // 2, model), BF16)),
        [VMEM, HBM, HBM],
        10**8,
        [pltpu.VMEM((2, tokens, channels), F32), sem((7,))],
        name="mix",
        limit=44,
    )(seen, parts, out_weight)
    other = lax.ppermute(theirs, "tp", [(0, 1), (1, 0)])
    wide = shape((rows, model), F32)
    acc, rest = call(
        project_kernel,
        (wide, shape((channels // 2, model), BF16)),
        [VMEM, VMEM, VMEM, HBM],
        10**9,
        [sem((1,))],
        name="project",
        limit=40,
    )(mine, residual, most, out_weight)
    normed, outgoing = call(
        dispatch_kernel,
        (shape((rows, model), BF16), shape((slots, model), BF16)),
        [VMEM] * 6,
        2 * 10**9,
        name="dispatch",
        limit=24,
    )(other, most, rest, acc, gain_mix[None], g)

    def exchanged(x):
        x = x.reshape(experts, CAP, model)
        x = lax.all_to_all(x, ("sp", "tp"), split_axis=0, concat_axis=0, tiled=True)
        return x.reshape(slots, model)

    received = exchanged(outgoing)
    results, base = call(
        expert_kernel,
        (shape((slots, model), BF16), wide),
        [VMEM] * 8,
        7 * 10**9,
        name="expert",
        limit=24,
    )(
        received, expert_gate, expert_up, expert_down, normed, shared_gate, shared_up, shared_down
    )
    back = exchanged(results)
    return call(
        finish_kernel,
        shape((rows, model), BF16),
        [VMEM] * 4,
        10**9,
        name="finish",
    )(base, c, back, gain_out[None])


def solution(mesh):
    return jax.shard_map(
        on_device,
        mesh=mesh,
        in_specs=(
            P("sp", "tp"),
            P("sp", "tp"),
            P(None, "tp"),
            P("tp", None, None),
            P("tp", None, None),
            P("tp"),
            P("sp", "tp"),
            P(),
            P(("sp", "tp"), None),
            P(),
            P(("sp", "tp"), None),
            P(("sp", "tp"), None),
            P(),
            P(),
            P(),
            P(("sp", "tp"), None, None),
            P(("sp", "tp"), None, None),
            P(("sp", "tp"), None, None),
            P(),
        ),
        out_specs=P(("sp", "tp"), None),
        check_vma=False,
    )
```

```python
import functools

import jax
import jax.numpy as jnp
from jax import lax
from jax.experimental import pallas as pl
from jax.experimental.pallas import tpu as pltpu
from jax.sharding import PartitionSpec as P

ALPHA = 8.0**0.25
RATE_C = 8.0
NORM_EPS = 1e-05
TINY = 1e-36
CAP = 8
BLOCK = 256
LANES = 8
F32 = jnp.float32
BF16 = jnp.bfloat16
VMEM = pl.BlockSpec(memory_space=pltpu.VMEM)
HBM = pl.BlockSpec(memory_space=pltpu.HBM)


def call(
    kernel, out_shape, in_specs, flops, scratch=(), name=None, out_specs=None, grid=(), limit=16
):
    if out_specs is None:
        out_specs = jax.tree.map(lambda _: VMEM, out_shape)
    return pl.pallas_call(
        kernel,
        out_shape=out_shape,
        in_specs=in_specs,
        out_specs=out_specs,
        grid=grid,
        scratch_shapes=list(scratch),
        compiler_params=pltpu.CompilerParams(vmem_limit_bytes=int(limit * 2**20)),
        cost_estimate=pl.CostEstimate(flops=flops, bytes_accessed=2**20, transcendentals=0),
        name=name,
    )


def shape(dims, dtype):
    return jax.ShapeDtypeStruct(dims, dtype)


def log1p_unit(u):
    s = u / (2.0 + u)
    q = s * s
    total = jnp.full_like(s, 1.0 / 17.0)
    for k in (15, 13, 11, 9, 7, 5, 3, 1):
        total = total * q + 1.0 / k
    return 2.0 * s * total


def minus_expm1_twice(x, decay):
    y = 2.0 * x
    total = jnp.full_like(y, 1.0 / 720.0)
    for k in (120, 24, 6, 2, 1):
        total = total * y + 1.0 / k
    return jnp.where(y > -0.125, -y * total, 1.0 - decay * decay)


def sigmoid(x):
    return 0.5 * jnp.tanh(0.5 * x) + 0.5


def layer_norm(values, gains):
    center = values - jnp.mean(values, axis=-1, keepdims=True)
    spread = jnp.mean(center * center, axis=-1, keepdims=True)
    return center * lax.rsqrt(spread + NORM_EPS) * gains


def fetch(pairs, sems):
    copies = [pltpu.make_async_copy(a, b, sems.at[i]) for i, (a, b) in enumerate(pairs)]
    for copy in copies:
        copy.start()
    return copies


def elements(conv, recur, gain, slope, moved):
    log_decay = slope * sigmoid(recur) + moved
    decay = jnp.exp(log_decay)
    power = minus_expm1_twice(log_decay, decay)
    return decay, power * lax.rsqrt(jnp.maximum(power, TINY)) * sigmoid(gain) * conv


def scan_kernel(
    halo_ref, small_ref, x_hbm, rmap_hbm, imap_hbm, tot_hbm, run_hbm,
    x_ref, rmap_ref, imap_ref, tot_ref, run_ref,
    ext, cv, rg, ig, sh, sems, outs,
):
    copies = fetch(
        [
            (x_hbm, x_ref),
            (rmap_hbm, rmap_ref),
            (imap_hbm, imap_ref),
        ],
        sems,
    )
    tokens, channels = x_ref.shape
    steps = tokens // LANES
    stride = steps + 8
    heads, width = rmap_ref.shape[:2]
    reach = halo_ref.shape[0]
    pad = 8 - reach
    copies[0].wait()
    for c in range(channels // 128):
        cols = slice(c * 128, (c + 1) * 128)
        x = x_ref[:, cols].astype(F32)
        ext[c, pl.ds(pad, reach), :] = halo_ref[:, cols].astype(F32)
        for i in range(LANES):
            if i > 0:
                ext[c, pl.ds(stride * i, 8), :] = x[steps * i - 8 : steps * i]
            ext[c, pl.ds(stride * i + 8, steps), :] = x[steps * i : steps * (i + 1)]
        taps = [small_ref[pl.ds(j, 1), cols] for j in range(reach + 1)]
        window = [ext[c, pl.ds(pad + j, LANES, stride=stride), :] for j in range(reach)]
        for t in range(steps):
            window.append(ext[c, pl.ds(8 + t, LANES, stride=stride), :])
            total = taps[0] * window[0]
            for j in range(1, reach + 1):
                total = total + taps[j] * window[j]
            window = window[1:]
            cv[pl.ds(t * LANES, LANES), cols] = total.astype(BF16).astype(F32)
    for copy in copies[1:]:
        copy.wait()
    for k in range(heads):
        cols = slice(k * width, (k + 1) * width)
        block = cv[:, cols].astype(BF16)
        rg[:, cols] = jnp.dot(block, rmap_ref[k], preferred_element_type=F32)
        ig[:, cols] = jnp.dot(block, imap_ref[k], preferred_element_type=F32)
    lines = [small_ref[pl.ds(reach + 2, 1), k * tokens : (k + 1) * tokens] for k in range(heads)]
    full = jnp.concatenate(lines + [jnp.zeros((128 - heads, tokens), F32)], axis=0)
    full = jnp.transpose(full)
    for i in range(LANES):
        sh[pl.ds(stride * i, steps), :] = full[steps * i : steps * (i + 1)]
    logit = -small_ref[pl.ds(reach + 1, 1), :]
    slope = -RATE_C * (jnp.maximum(logit, 0.0) + log1p_unit(jnp.exp(-jnp.abs(logit))))

    def step(t, carry):
        rows = pl.ds(pl.multiple_of(t * LANES, LANES), LANES)
        moved = sh[pl.ds(t, LANES, stride=stride), :]
        out = []
        for k in range(heads):
            h, run = carry[k]
            cols = slice(k * width, (k + 1) * width)
            decay, update = elements(
                cv[rows, cols], rg[rows, cols], ig[rows, cols], slope[:, cols], moved[:, k : k + 1]
            )
            h = decay * h + update
            run = decay * run
            for j in range(width // 128):
                lane = slice(j * 128, (j + 1) * 128)
                run_ref[0, k * (width // 128) + j, rows, :] = h[:, lane]
                run_ref[1, k * (width // 128) + j, rows, :] = run[:, lane]
            out.append((h, run))
        return tuple(out)

    last = tuple(
        (jnp.zeros((LANES, width), F32), jnp.ones((LANES, width), F32)) for _ in range(heads)
    )
    sent = []
    for part in range(4):
        span = steps // 4
        last = lax.fori_loop(part * span, (part + 1) * span, step, last, unroll=2)
        rows = pl.ds(part * span * LANES, span * LANES)
        copy = pltpu.make_async_copy(
            run_ref.at[:, :, rows, :], run_hbm.at[:, :, rows, :], outs.at[part]
        )
        copy.start()
        sent.append(copy)
    row = lax.broadcasted_iota(jnp.int32, (LANES, width), 0)
    ends = [[], []]
    for k in range(heads):
        cols = slice(k * width, (k + 1) * width)
        h, a = last[k]
        for d in (1, 2, 4):
            hp, ap = pltpu.roll(h, d, 0), pltpu.roll(a, d, 0)
            h = jnp.where(row >= d, a * hp + h, h)
            a = jnp.where(row >= d, a * ap, a)
        for j in range(width // 128):
            lane = slice(j * 128, (j + 1) * 128)
            ends[0].append(jnp.log(jnp.maximum(a[LANES - 1 :, lane], TINY)))
            ends[1].append(h[LANES - 1 :, lane])
        enter = jnp.where(row >= 1, pltpu.roll(h, 1, 0), 0.0)
        scale = jnp.where(row >= 1, pltpu.roll(a, 1, 0), 1.0)
        for j in range(width // 128):
            lane = slice(j * 128, (j + 1) * 128)
            run_ref[0, k * (width // 128) + j, pl.ds(tokens, LANES), :] = enter[:, lane]
            run_ref[1, k * (width // 128) + j, pl.ds(tokens, LANES), :] = scale[:, lane]
    both = jnp.concatenate(ends[0] + ends[1], axis=0).astype(BF16)
    for i in range(tot_ref.shape[0]):
        tot_ref[i] = both
    rows = pl.ds(tokens, LANES)
    sent += [
        pltpu.make_async_copy(tot_ref, tot_hbm, outs.at[4]),
        pltpu.make_async_copy(run_ref.at[:, :, rows, :], run_hbm.at[:, :, rows, :], outs.at[5]),
    ]
    for copy in sent[4:]:
        copy.start()
    for copy in sent:
        copy.wait()


def side_kernel(
    gate_hbm, routes_hbm, weight_hbm, run_hbm, mixed_hbm, g_hbm, c_hbm,
    gate_ref, routes_ref, weight_ref, run_ref, mixed_ref, g_ref, c_ref, sems, outs,
):
    copies = fetch(
        [
            (routes_hbm, routes_ref),
            (weight_hbm, weight_ref),
            (gate_hbm, gate_ref),
            (run_hbm, run_ref),
        ],
        sems,
    )
    for copy in copies[:2]:
        copy.wait()
    route(routes_ref, weight_ref, g_ref, c_ref)
    for copy in copies[2:]:
        copy.wait()
    tokens, channels = gate_ref.shape
    steps = tokens // LANES
    block = 16
    per = steps // block

    def put(i, _):
        rows = pl.ds(pl.multiple_of(i * block, block), block)
        chunk = i // per
        source = pl.ds(chunk + (i % per) * (block * LANES), block, stride=LANES)
        gate = jax.nn.gelu(gate_ref[rows, :].astype(F32), approximate=True)
        edge = pl.ds(tokens + chunk, 1)
        for c in range(channels // 128):
            cols = slice(c * 128, (c + 1) * 128)
            run = run_ref[1, c, source, :]
            own = run_ref[0, c, source, :] + run * run_ref[0, c, edge, :]
            mixed_ref[0, rows, cols] = own * gate[:, cols]
            mixed_ref[1, rows, cols] = run * run_ref[1, c, edge, :] * gate[:, cols]
        return 0

    pairs = [(g_ref, g_hbm), (c_ref, c_hbm)]
    sent = fetch(pairs, outs)
    quarter = tokens // 4
    for part in range(4):
        lax.fori_loop(part * quarter // block, (part + 1) * quarter // block, put, 0)
        rows = pl.ds(part * quarter, quarter)
        copy = pltpu.make_async_copy(
            mixed_ref.at[:, rows, :], mixed_hbm.at[pl.ds(0, 2), rows, :], outs.at[2 + part]
        )
        copy.start()
        sent.append(copy)
    for copy in sent:
        copy.wait()


def mix_kernel(
    seen_ref, mixed_hbm, w_hbm, mine_ref, theirs_ref, w_ref, mixed_ref, sems
):
    _, tokens, channels = mixed_ref.shape
    here, side = lax.axis_index("sp"), lax.axis_index("tp")
    half = tokens // 2
    strip = channels // 2
    pairs = []
    for j in range(4):
        rows = pl.ds(j * (tokens // 4), tokens // 4)
        pairs.append((mixed_hbm.at[pl.ds(0, 2), rows, :], mixed_ref.at[:, rows, :]))
    for j in range(3):
        at = (side if j < 2 else 1 - side) * channels + (j % 2) * strip
        at = pl.multiple_of(at, strip)
        pairs.append((w_hbm.at[pl.ds(at, strip), :], w_ref.at[pl.ds(j * strip, strip), :]))
    copies = fetch(pairs, sems)
    carried = jnp.zeros((LANES, 128), F32)
    for i in range(seen_ref.shape[0]):
        pair = seen_ref[i].astype(F32)
        carried = jnp.where(i < here, jnp.exp(pair[:LANES]) * carried + pair[LANES:], carried)
    carried = jnp.concatenate([carried[i : i + 1] for i in range(LANES)], axis=1)
    block = 16
    for copy in copies[:4]:
        copy.wait()

    def put(i, _):
        at = pl.multiple_of(i * block, block)
        for ref, part in ((theirs_ref, 1 - side), (mine_ref, side)):
            rows = pl.ds(pl.multiple_of(part * half + at, block), block)
            ref[pl.ds(at, block), :] = (mixed_ref[0, rows, :] + mixed_ref[1, rows, :] * carried).astype(
                BF16
            )
        return 0

    lax.fori_loop(0, half // block, put, 0, unroll=2)
    for copy in copies[4:]:
        copy.wait()


def route(routes_ref, weight_ref, g_ref, c_ref):
    fanout, rows = routes_ref.shape
    slots = g_ref.shape[0]
    experts = slots // CAP
    expert = lax.broadcasted_iota(jnp.int32, (experts, rows), 0)
    member = jnp.zeros((experts, rows), F32)
    weight = jnp.zeros((experts, rows), F32)
    for k in range(fanout):
        hit = expert == routes_ref[pl.ds(k, 1), :]
        member = member + jnp.where(hit, 1.0, 0.0)
        weight = weight + jnp.where(hit, weight_ref[pl.ds(k, 1), :], 0.0)
    earlier = (
        lax.broadcasted_iota(jnp.int32, (rows, rows), 0)
        < lax.broadcasted_iota(jnp.int32, (rows, rows), 1)
    )
    rank = jnp.dot(
        member.astype(BF16), jnp.where(earlier, 1.0, 0.0).astype(BF16), preferred_element_type=F32
    )
    rank = jnp.where(member > 0.0, rank, -1.0).astype(BF16)
    weight = weight.astype(BF16)
    slot = lax.broadcasted_iota(jnp.int32, (BLOCK, experts), 0)
    spread_at = lax.broadcasted_iota(jnp.int32, (BLOCK, experts), 1)
    place = (lax.broadcasted_iota(jnp.int32, (BLOCK, rows), 0) % CAP).astype(F32)
    for b in range(slots // BLOCK):
        spread = jnp.where((slot + b * BLOCK) // CAP == spread_at, 1.0, 0.0).astype(BF16)

        def to_slots(values):
            return jnp.dot(spread, values, preferred_element_type=F32)

        chosen = to_slots(rank) == place
        g_ref[pl.ds(b * BLOCK, BLOCK), :] = jnp.where(chosen, 1.0, 0.0).astype(BF16)
        cols = slice(b * BLOCK, (b + 1) * BLOCK)
        c_ref[:, cols] = jnp.transpose(jnp.where(chosen, to_slots(weight), 0.0)).astype(BF16)


def project_kernel(mine_ref, res_ref, w_ref, w_hbm, out_ref, rest_ref, sems):
    depth = mine_ref.shape[1]
    half = depth // 2
    at = pl.multiple_of((1 - lax.axis_index("tp")) * depth + half, half)
    copies = fetch([(w_hbm.at[pl.ds(at, half), :], rest_ref)], sems)
    out_ref[...] = ALPHA * res_ref[...].astype(F32) + jnp.dot(
        mine_ref[...], w_ref[:depth], preferred_element_type=F32
    )
    copies[0].wait()


def dispatch_kernel(other_ref, w_ref, rest_ref, acc_ref, gain_ref, g_ref, normed_ref, out_ref):
    depth = other_ref.shape[1]
    values = (
        acc_ref[...]
        + jnp.dot(other_ref[:, : depth // 2], w_ref[depth:], preferred_element_type=F32)
        + jnp.dot(other_ref[:, depth // 2 :], rest_ref[...], preferred_element_type=F32)
    )
    normed = layer_norm(values, gain_ref[...]).astype(BF16)
    normed_ref[...] = normed

    out_ref[...] = jnp.dot(g_ref[...], normed, preferred_element_type=F32).astype(BF16)


def hidden_of(x, gate, up):
    return (
        jax.nn.silu(jnp.dot(x, gate, preferred_element_type=F32))
        * jnp.dot(x, up, preferred_element_type=F32)
    ).astype(BF16)


def expert_kernel(
    x_ref, gate_ref, up_ref, down_ref, own_ref, sgate_ref, sup_ref, sdown_ref, out_ref, base_ref
):
    block = 2 * BLOCK

    def step(i, _):
        rows = pl.ds(pl.multiple_of(i * block, block), block)
        hidden = hidden_of(x_ref[rows, :], gate_ref[0], up_ref[0])
        out_ref[rows, :] = jnp.dot(hidden, down_ref[0], preferred_element_type=F32).astype(BF16)
        return 0

    lax.fori_loop(0, x_ref.shape[0] // block, step, 0)
    x = own_ref[...]
    hidden = hidden_of(x, sgate_ref[...], sup_ref[...])
    base_ref[...] = ALPHA * x.astype(F32) + jnp.dot(
        hidden, sdown_ref[...], preferred_element_type=F32
    )


def finish_kernel(base_ref, c_ref, back_ref, gain_ref, out_ref):
    values = base_ref[...] + jnp.dot(c_ref[...], back_ref[...], preferred_element_type=F32)
    out_ref[...] = layer_norm(values, gain_ref[...]).astype(BF16)


def on_device(
    gate_pre, conv_in, conv_taps, recur_map, input_map, rate_logit, decay_shift, out_weight,
    residual, gain_mix, routes, route_weight, shared_gate, shared_up, shared_down, expert_gate,
    expert_up, expert_down, gain_out,
):
    tokens, channels = conv_in.shape
    reach = conv_taps.shape[0] - 1
    sp, tp = lax.axis_size("sp"), lax.axis_size("tp")
    experts = sp * tp
    rows = tokens // tp
    model = out_weight.shape[1]
    slots = experts * CAP
    sem = pltpu.SemaphoreType.DMA
    before = lax.ppermute(conv_in[tokens - reach :], "sp", [(i, i + 1) for i in range(sp - 1)])
    padded = shape((8, tokens, channels), F32)
    big = pltpu.VMEM((tokens, channels), F32)
    apart = tokens + 8 * LANES
    lanes = pltpu.VMEM((channels // 128, apart, 128), F32)

    def staged(kernel, operands, made, flops, scratch, name):
        held = [
            pltpu.VMEM((2,) + x.shape[1:] if x is padded else x.shape, x.dtype)
            for x in tuple(operands) + made
        ]
        return call(
            kernel,
            made,
            [HBM] * len(operands),
            flops,
            held + scratch,
            name=name,
            out_specs=(HBM,) * len(made),
            limit=62,
        )(*operands)

    small = jnp.concatenate(
        [conv_taps.astype(F32), rate_logit[None], decay_shift.T.reshape(1, -1)], axis=0
    )
    made = (
        shape((sp, 2 * LANES, 128), BF16),
        shape((2, channels // 128, tokens + LANES, 128), F32),
    )
    held = (conv_in, recur_map, input_map) + made
    totals, local = call(
        scan_kernel,
        made,
        [VMEM] * 2 + [HBM] * 3,
        10**9,
        [pltpu.VMEM(x.shape, x.dtype) for x in held]
        + [lanes, big, big, big, pltpu.VMEM((apart, 128), F32), sem((3,)), sem((6,))],
        name="scan",
        out_specs=(HBM,) * 2,
        limit=53.5,
    )(before, small, conv_in, recur_map, input_map)
    seen = lax.all_to_all(totals, "sp", 0, 0, tiled=True)
    parts, g, c = staged(
        side_kernel,
        (gate_pre, routes.T, route_weight.T, local),
        (padded, shape((slots, rows), BF16), shape((rows, slots), BF16)),
        10**10,
        [sem((4,)), sem((6,))],
        "side",
    )
    piece = shape((rows, channels), BF16)
    mine, theirs, most = call(
        mix_kernel,
        (piece, piece, shape((3 * channels // 2, model), BF16)),
        [VMEM, HBM, HBM],
        10**8,
        [pltpu.VMEM((2, tokens, channels), F32), sem((7,))],
        name="mix",
        limit=44,
    )(seen, parts, out_weight)
    other = lax.ppermute(theirs, "tp", [(0, 1), (1, 0)])
    wide = shape((rows, model), F32)
    acc, rest = call(
        project_kernel,
        (wide, shape((channels // 2, model), BF16)),
        [VMEM, VMEM, VMEM, HBM],
        10**9,
        [sem((1,))],
        name="project",
        limit=40,
    )(mine, residual, most, out_weight)
    normed, outgoing = call(
        dispatch_kernel,
        (shape((rows, model), BF16), shape((slots, model), BF16)),
        [VMEM] * 6,
        2 * 10**9,
        name="dispatch",
        limit=24,
    )(other, most, rest, acc, gain_mix[None], g)

    def exchanged(x):
        x = x.reshape(experts, CAP, model)
        x = lax.all_to_all(x, ("sp", "tp"), split_axis=0, concat_axis=0, tiled=True)
        return x.reshape(slots, model)

    received = exchanged(outgoing)
    results, base = call(
        expert_kernel,
        (shape((slots, model), BF16), wide),
        [VMEM] * 8,
        7 * 10**9,
        name="expert",
        limit=24,
    )(
        received, expert_gate, expert_up, expert_down, normed, shared_gate, shared_up, shared_down
    )
    back = exchanged(results)
    return call(
        finish_kernel,
        shape((rows, model), BF16),
        [VMEM] * 4,
        10**9,
        name="finish",
    )(base, c, back, gain_out[None])


def solution(mesh):
    return jax.shard_map(
        on_device,
        mesh=mesh,
        in_specs=(
            P("sp", "tp"),
            P("sp", "tp"),
            P(None, "tp"),
            P("tp", None, None),
            P("tp", None, None),
            P("tp"),
            P("sp", "tp"),
            P(),
            P(("sp", "tp"), None),
            P(),
            P(("sp", "tp"), None),
            P(("sp", "tp"), None),
            P(),
            P(),
            P(),
            P(("sp", "tp"), None, None),
            P(("sp", "tp"), None, None),
            P(("sp", "tp"), None, None),
            P(),
        ),
        out_specs=P(("sp", "tp"), None),
        check_vma=False,
    )
```

```python
import functools

import jax
import jax.numpy as jnp
from jax import lax
from jax.experimental import pallas as pl
from jax.experimental.pallas import tpu as pltpu
from jax.sharding import PartitionSpec as P

ALPHA = 8.0**0.25
RATE_C = 8.0
NORM_EPS = 1e-05
TINY = 1e-36
CAP = 8
BLOCK = 256
LANES = 8
F32 = jnp.float32
BF16 = jnp.bfloat16
VMEM = pl.BlockSpec(memory_space=pltpu.VMEM)
HBM = pl.BlockSpec(memory_space=pltpu.HBM)


def call(
    kernel, out_shape, in_specs, flops, scratch=(), name=None, out_specs=None, grid=(), limit=16
):
    if out_specs is None:
        out_specs = jax.tree.map(lambda _: VMEM, out_shape)
    return pl.pallas_call(
        kernel,
        out_shape=out_shape,
        in_specs=in_specs,
        out_specs=out_specs,
        grid=grid,
        scratch_shapes=list(scratch),
        compiler_params=pltpu.CompilerParams(vmem_limit_bytes=int(limit * 2**20)),
        cost_estimate=pl.CostEstimate(flops=flops, bytes_accessed=2**20, transcendentals=0),
        name=name,
    )


def shape(dims, dtype):
    return jax.ShapeDtypeStruct(dims, dtype)


def log1p_unit(u):
    s = u / (2.0 + u)
    q = s * s
    total = jnp.full_like(s, 1.0 / 17.0)
    for k in (15, 13, 11, 9, 7, 5, 3, 1):
        total = total * q + 1.0 / k
    return 2.0 * s * total


def minus_expm1_twice(x, decay):
    y = 2.0 * x
    total = jnp.full_like(y, 1.0 / 720.0)
    for k in (120, 24, 6, 2, 1):
        total = total * y + 1.0 / k
    return jnp.where(y > -0.125, -y * total, 1.0 - decay * decay)


def sigmoid(x):
    return 0.5 * jnp.tanh(0.5 * x) + 0.5


def layer_norm(values, gains):
    center = values - jnp.mean(values, axis=-1, keepdims=True)
    spread = jnp.mean(center * center, axis=-1, keepdims=True)
    return center * lax.rsqrt(spread + NORM_EPS) * gains


def fetch(pairs, sems):
    copies = [pltpu.make_async_copy(a, b, sems.at[i]) for i, (a, b) in enumerate(pairs)]
    for copy in copies:
        copy.start()
    return copies


def elements(conv, recur, gain, slope, moved):
    log_decay = slope * sigmoid(recur) + moved
    decay = jnp.exp(log_decay)
    power = minus_expm1_twice(log_decay, decay)
    return decay, power * lax.rsqrt(jnp.maximum(power, TINY)) * sigmoid(gain) * conv


def scan_kernel(
    halo_ref, small_ref, x_hbm, rmap_hbm, imap_hbm, tot_hbm, run_hbm,
    x_ref, rmap_ref, imap_ref, tot_ref, run_ref,
    ext, cv, rg, ig, sh, sems, outs,
):
    copies = fetch(
        [
            (x_hbm, x_ref),
            (rmap_hbm, rmap_ref),
            (imap_hbm, imap_ref),
        ],
        sems,
    )
    tokens, channels = x_ref.shape
    steps = tokens // LANES
    stride = steps + 8
    heads, width = rmap_ref.shape[:2]
    reach = halo_ref.shape[0]
    pad = 8 - reach
    copies[0].wait()
    for c in range(channels // 128):
        cols = slice(c * 128, (c + 1) * 128)
        x = x_ref[:, cols].astype(F32)
        ext[c, pl.ds(pad, reach), :] = halo_ref[:, cols].astype(F32)
        for i in range(LANES):
            if i > 0:
                ext[c, pl.ds(stride * i, 8), :] = x[steps * i - 8 : steps * i]
            ext[c, pl.ds(stride * i + 8, steps), :] = x[steps * i : steps * (i + 1)]
        taps = [small_ref[pl.ds(j, 1), cols] for j in range(reach + 1)]
        window = [ext[c, pl.ds(pad + j, LANES, stride=stride), :] for j in range(reach)]
        for t in range(steps):
            window.append(ext[c, pl.ds(8 + t, LANES, stride=stride), :])
            total = taps[0] * window[0]
            for j in range(1, reach + 1):
                total = total + taps[j] * window[j]
            window = window[1:]
            cv[pl.ds(t * LANES, LANES), cols] = total.astype(BF16).astype(F32)
    for copy in copies[1:]:
        copy.wait()
    for k in range(heads):
        cols = slice(k * width, (k + 1) * width)
        block = cv[:, cols].astype(BF16)
        rg[:, cols] = jnp.dot(block, rmap_ref[k], preferred_element_type=F32)
        ig[:, cols] = jnp.dot(block, imap_ref[k], preferred_element_type=F32)
    lines = [small_ref[pl.ds(reach + 2 + k, 1), :tokens] for k in range(heads)]
    full = jnp.concatenate(lines + [jnp.zeros((128 - heads, tokens), F32)], axis=0)
    full = jnp.transpose(full)
    for i in range(LANES):
        sh[pl.ds(stride * i, steps), :] = full[steps * i : steps * (i + 1)]
    logit = -small_ref[pl.ds(reach + 1, 1), :]
    slope = -RATE_C * (jnp.maximum(logit, 0.0) + log1p_unit(jnp.exp(-jnp.abs(logit))))

    def step(t, carry):
        rows = pl.ds(pl.multiple_of(t * LANES, LANES), LANES)
        moved = sh[pl.ds(t, LANES, stride=stride), :]
        out = []
        for k in range(heads):
            h, run = carry[k]
            cols = slice(k * width, (k + 1) * width)
            decay, update = elements(
                cv[rows, cols], rg[rows, cols], ig[rows, cols], slope[:, cols], moved[:, k : k + 1]
            )
            h = decay * h + update
            run = decay * run
            for j in range(width // 128):
                lane = slice(j * 128, (j + 1) * 128)
                run_ref[0, k * (width // 128) + j, rows, :] = h[:, lane]
                run_ref[1, k * (width // 128) + j, rows, :] = run[:, lane]
            out.append((h, run))
        return tuple(out)

    last = tuple(
        (jnp.zeros((LANES, width), F32), jnp.ones((LANES, width), F32)) for _ in range(heads)
    )
    sent = []
    for part in range(4):
        span = steps // 4
        last = lax.fori_loop(part * span, (part + 1) * span, step, last, unroll=2)
        rows = pl.ds(part * span * LANES, span * LANES)
        copy = pltpu.make_async_copy(
            run_ref.at[:, :, rows, :], run_hbm.at[:, :, rows, :], outs.at[part]
        )
        copy.start()
        sent.append(copy)
    row = lax.broadcasted_iota(jnp.int32, (LANES, width), 0)
    ends = [[], []]
    for k in range(heads):
        cols = slice(k * width, (k + 1) * width)
        h, a = last[k]
        for d in (1, 2, 4):
            hp, ap = pltpu.roll(h, d, 0), pltpu.roll(a, d, 0)
            h = jnp.where(row >= d, a * hp + h, h)
            a = jnp.where(row >= d, a * ap, a)
        for j in range(width // 128):
            lane = slice(j * 128, (j + 1) * 128)
            ends[0].append(jnp.log(jnp.maximum(a[LANES - 1 :, lane], TINY)))
            ends[1].append(h[LANES - 1 :, lane])
        enter = jnp.where(row >= 1, pltpu.roll(h, 1, 0), 0.0)
        scale = jnp.where(row >= 1, pltpu.roll(a, 1, 0), 1.0)
        for j in range(width // 128):
            lane = slice(j * 128, (j + 1) * 128)
            run_ref[0, k * (width // 128) + j, pl.ds(tokens, LANES), :] = enter[:, lane]
            run_ref[1, k * (width // 128) + j, pl.ds(tokens, LANES), :] = scale[:, lane]
    both = jnp.concatenate(ends[0] + ends[1], axis=0).astype(BF16)
    for i in range(tot_ref.shape[0]):
        tot_ref[i] = both
    rows = pl.ds(tokens, LANES)
    sent += [
        pltpu.make_async_copy(tot_ref, tot_hbm, outs.at[4]),
        pltpu.make_async_copy(run_ref.at[:, :, rows, :], run_hbm.at[:, :, rows, :], outs.at[5]),
    ]
    for copy in sent[4:]:
        copy.start()
    for copy in sent:
        copy.wait()


def side_kernel(
    gate_hbm, routes_hbm, weight_hbm, run_hbm, mixed_hbm, g_hbm, c_hbm,
    gate_ref, routes_ref, weight_ref, run_ref, mixed_ref, g_ref, c_ref, sems, outs,
):
    copies = fetch(
        [
            (routes_hbm, routes_ref),
            (weight_hbm, weight_ref),
            (gate_hbm, gate_ref),
            (run_hbm, run_ref),
        ],
        sems,
    )
    for copy in copies[:2]:
        copy.wait()
    route(routes_ref, weight_ref, g_ref, c_ref)
    for copy in copies[2:]:
        copy.wait()
    tokens, channels = gate_ref.shape
    steps = tokens // LANES
    block = 16
    per = steps // block

    def put(i, _):
        rows = pl.ds(pl.multiple_of(i * block, block), block)
        chunk = i // per
        source = pl.ds(chunk + (i % per) * (block * LANES), block, stride=LANES)
        gate = jax.nn.gelu(gate_ref[rows, :].astype(F32), approximate=True)
        edge = pl.ds(tokens + chunk, 1)
        for c in range(channels // 128):
            cols = slice(c * 128, (c + 1) * 128)
            run = run_ref[1, c, source, :]
            own = run_ref[0, c, source, :] + run * run_ref[0, c, edge, :]
            mixed_ref[0, rows, cols] = own * gate[:, cols]
            mixed_ref[1, rows, cols] = run * run_ref[1, c, edge, :] * gate[:, cols]
        return 0

    pairs = [(g_ref, g_hbm), (c_ref, c_hbm)]
    sent = fetch(pairs, outs)
    quarter = tokens // 4
    for part in range(4):
        lax.fori_loop(part * quarter // block, (part + 1) * quarter // block, put, 0)
        rows = pl.ds(part * quarter, quarter)
        copy = pltpu.make_async_copy(
            mixed_ref.at[:, rows, :], mixed_hbm.at[pl.ds(0, 2), rows, :], outs.at[2 + part]
        )
        copy.start()
        sent.append(copy)
    for copy in sent:
        copy.wait()


def mix_kernel(
    seen_ref, mixed_hbm, w_hbm, mine_ref, theirs_ref, w_ref, mixed_ref, sems
):
    _, tokens, channels = mixed_ref.shape
    here, side = lax.axis_index("sp"), lax.axis_index("tp")
    half = tokens // 2
    strip = channels // 2
    pairs = []
    for j in range(4):
        rows = pl.ds(j * (tokens // 4), tokens // 4)
        pairs.append((mixed_hbm.at[pl.ds(0, 2), rows, :], mixed_ref.at[:, rows, :]))
    pairs.append((w_hbm.at[pl.ds(pl.multiple_of(side * channels, strip), strip), :], w_ref))
    copies = fetch(pairs, sems)
    carried = jnp.zeros((LANES, 128), F32)
    for i in range(seen_ref.shape[0]):
        pair = seen_ref[i].astype(F32)
        carried = jnp.where(i < here, jnp.exp(pair[:LANES]) * carried + pair[LANES:], carried)
    carried = jnp.concatenate([carried[i : i + 1] for i in range(LANES)], axis=1)
    block = 16
    for copy in copies[:4]:
        copy.wait()

    def put(i, _):
        at = pl.multiple_of(i * block, block)
        for ref, part in ((theirs_ref, 1 - side), (mine_ref, side)):
            rows = pl.ds(pl.multiple_of(part * half + at, block), block)
            ref[pl.ds(at, block), :] = (mixed_ref[0, rows, :] + mixed_ref[1, rows, :] * carried).astype(
                BF16
            )
        return 0

    lax.fori_loop(0, half // block, put, 0, unroll=2)
    for copy in copies[4:]:
        copy.wait()


def route(routes_ref, weight_ref, g_ref, c_ref):
    fanout, rows = routes_ref.shape
    slots = g_ref.shape[0]
    experts = slots // CAP
    expert = lax.broadcasted_iota(jnp.int32, (experts, rows), 0)
    member = jnp.zeros((experts, rows), F32)
    weight = jnp.zeros((experts, rows), F32)
    for k in range(fanout):
        hit = expert == routes_ref[pl.ds(k, 1), :]
        member = member + jnp.where(hit, 1.0, 0.0)
        weight = weight + jnp.where(hit, weight_ref[pl.ds(k, 1), :], 0.0)
    earlier = (
        lax.broadcasted_iota(jnp.int32, (rows, rows), 0)
        < lax.broadcasted_iota(jnp.int32, (rows, rows), 1)
    )
    rank = jnp.dot(
        member.astype(BF16), jnp.where(earlier, 1.0, 0.0).astype(BF16), preferred_element_type=F32
    )
    rank = jnp.where(member > 0.0, rank, -1.0).astype(BF16)
    weight = weight.astype(BF16)
    slot = lax.broadcasted_iota(jnp.int32, (BLOCK, experts), 0)
    spread_at = lax.broadcasted_iota(jnp.int32, (BLOCK, experts), 1)
    place = (lax.broadcasted_iota(jnp.int32, (BLOCK, rows), 0) % CAP).astype(F32)
    for b in range(slots // BLOCK):
        spread = jnp.where((slot + b * BLOCK) // CAP == spread_at, 1.0, 0.0).astype(BF16)

        def to_slots(values):
            return jnp.dot(spread, values, preferred_element_type=F32)

        chosen = to_slots(rank) == place
        g_ref[pl.ds(b * BLOCK, BLOCK), :] = jnp.where(chosen, 1.0, 0.0).astype(BF16)
        cols = slice(b * BLOCK, (b + 1) * BLOCK)
        c_ref[:, cols] = jnp.transpose(jnp.where(chosen, to_slots(weight), 0.0)).astype(BF16)


def project_kernel(mine_ref, res_ref, w_ref, w_hbm, out_ref, rest_ref, own_ref, sems):
    depth = mine_ref.shape[1]
    half = depth // 2
    side = lax.axis_index("tp")
    pairs = [(w_hbm.at[pl.ds(pl.multiple_of(side * depth + half, half), half), :], own_ref)]
    for j in range(2):
        at = pl.multiple_of((1 - side) * depth + j * half, half)
        pairs.append((w_hbm.at[pl.ds(at, half), :], rest_ref.at[pl.ds(j * half, half), :]))
    copies = fetch(pairs, sems)
    out_ref[...] = ALPHA * res_ref[...].astype(F32) + jnp.dot(
        mine_ref[:, :half], w_ref[...], preferred_element_type=F32
    )
    copies[0].wait()
    out_ref[...] += jnp.dot(mine_ref[:, half:], own_ref[...], preferred_element_type=F32)
    for copy in copies[1:]:
        copy.wait()


def dispatch_kernel(other_ref, rest_ref, acc_ref, gain_ref, g_ref, normed_ref, out_ref):
    values = acc_ref[...] + jnp.dot(other_ref[...], rest_ref[...], preferred_element_type=F32)
    normed = layer_norm(values, gain_ref[...]).astype(BF16)
    normed_ref[...] = normed

    out_ref[...] = jnp.dot(g_ref[...], normed, preferred_element_type=F32).astype(BF16)


def hidden_of(x, gate, up):
    return (
        jax.nn.silu(jnp.dot(x, gate, preferred_element_type=F32))
        * jnp.dot(x, up, preferred_element_type=F32)
    ).astype(BF16)


def expert_kernel(
    x_ref, gate_ref, up_ref, down_ref, own_ref, sgate_ref, sup_ref, sdown_ref, out_ref, base_ref
):
    block = 2 * BLOCK

    def step(i, _):
        rows = pl.ds(pl.multiple_of(i * block, block), block)
        hidden = hidden_of(x_ref[rows, :], gate_ref[0], up_ref[0])
        out_ref[rows, :] = jnp.dot(hidden, down_ref[0], preferred_element_type=F32).astype(BF16)
        return 0

    lax.fori_loop(0, x_ref.shape[0] // block, step, 0)
    x = own_ref[...]
    hidden = hidden_of(x, sgate_ref[...], sup_ref[...])
    base_ref[...] = ALPHA * x.astype(F32) + jnp.dot(
        hidden, sdown_ref[...], preferred_element_type=F32
    )


def finish_kernel(base_ref, c_ref, back_ref, gain_ref, out_ref):
    values = base_ref[...] + jnp.dot(c_ref[...], back_ref[...], preferred_element_type=F32)
    out_ref[...] = layer_norm(values, gain_ref[...]).astype(BF16)


def on_device(
    gate_pre, conv_in, conv_taps, recur_map, input_map, rate_logit, decay_shift, out_weight,
    residual, gain_mix, routes, route_weight, shared_gate, shared_up, shared_down, expert_gate,
    expert_up, expert_down, gain_out,
):
    tokens, channels = conv_in.shape
    reach = conv_taps.shape[0] - 1
    sp, tp = lax.axis_size("sp"), lax.axis_size("tp")
    experts = sp * tp
    rows = tokens // tp
    model = out_weight.shape[1]
    slots = experts * CAP
    sem = pltpu.SemaphoreType.DMA
    before = lax.ppermute(conv_in[tokens - reach :], "sp", [(i, i + 1) for i in range(sp - 1)])
    padded = shape((8, tokens, channels), F32)
    big = pltpu.VMEM((tokens, channels), F32)
    apart = tokens + 8 * LANES
    lanes = pltpu.VMEM((channels // 128, apart, 128), F32)

    def staged(kernel, operands, made, flops, scratch, name):
        held = [
            pltpu.VMEM((2,) + x.shape[1:] if x is padded else x.shape, x.dtype)
            for x in tuple(operands) + made
        ]
        return call(
            kernel,
            made,
            [HBM] * len(operands),
            flops,
            held + scratch,
            name=name,
            out_specs=(HBM,) * len(made),
            limit=62,
        )(*operands)

    small = jnp.concatenate(
        [
            conv_taps.astype(F32),
            rate_logit[None],
            jnp.pad(decay_shift.T, ((0, 0), (0, channels - tokens))),
        ],
        axis=0,
    )
    made = (
        shape((sp, 2 * LANES, 128), BF16),
        shape((2, channels // 128, tokens + LANES, 128), F32),
    )
    held = (conv_in, recur_map, input_map) + made
    totals, local = call(
        scan_kernel,
        made,
        [VMEM] * 2 + [HBM] * 3,
        10**9,
        [pltpu.VMEM(x.shape, x.dtype) for x in held]
        + [lanes, big, big, big, pltpu.VMEM((apart, 128), F32), sem((3,)), sem((6,))],
        name="scan",
        out_specs=(HBM,) * 2,
        limit=53.5,
    )(before, small, conv_in, recur_map, input_map)
    seen = lax.all_to_all(totals, "sp", 0, 0, tiled=True)
    parts, g, c = staged(
        side_kernel,
        (gate_pre, routes.T, route_weight.T, local),
        (padded, shape((slots, rows), BF16), shape((rows, slots), BF16)),
        10**10,
        [sem((4,)), sem((6,))],
        "side",
    )
    piece = shape((rows, channels), BF16)
    mine, theirs, most = call(
        mix_kernel,
        (piece, piece, shape((channels // 2, model), BF16)),
        [VMEM, HBM, HBM],
        10**8,
        [pltpu.VMEM((2, tokens, channels), F32), sem((5,))],
        name="mix",
        limit=48,
    )(seen, parts, out_weight)
    other = lax.ppermute(theirs, "tp", [(0, 1), (1, 0)])
    wide = shape((rows, model), F32)
    acc, rest = call(
        project_kernel,
        (wide, shape((channels, model), BF16)),
        [VMEM, VMEM, VMEM, HBM],
        10**9,
        [pltpu.VMEM((channels // 2, model), BF16), sem((3,))],
        name="project",
        limit=41,
    )(mine, residual, most, out_weight)
    normed, outgoing = call(
        dispatch_kernel,
        (shape((rows, model), BF16), shape((slots, model), BF16)),
        [VMEM] * 5,
        2 * 10**9,
        name="dispatch",
        limit=24,
    )(other, rest, acc, gain_mix[None], g)

    def exchanged(x):
        x = x.reshape(experts, CAP, model)
        x = lax.all_to_all(x, ("sp", "tp"), split_axis=0, concat_axis=0, tiled=True)
        return x.reshape(slots, model)

    received = exchanged(outgoing)
    results, base = call(
        expert_kernel,
        (shape((slots, model), BF16), wide),
        [VMEM] * 8,
        7 * 10**9,
        name="expert",
        limit=24,
    )(
        received, expert_gate, expert_up, expert_down, normed, shared_gate, shared_up, shared_down
    )
    back = exchanged(results)
    return call(
        finish_kernel,
        shape((rows, model), BF16),
        [VMEM] * 4,
        10**9,
        name="finish",
    )(base, c, back, gain_out[None])


def solution(mesh):
    return jax.shard_map(
        on_device,
        mesh=mesh,
        in_specs=(
            P("sp", "tp"),
            P("sp", "tp"),
            P(None, "tp"),
            P("tp", None, None),
            P("tp", None, None),
            P("tp"),
            P("sp", "tp"),
            P(),
            P(("sp", "tp"), None),
            P(),
            P(("sp", "tp"), None),
            P(("sp", "tp"), None),
            P(),
            P(),
            P(),
            P(("sp", "tp"), None, None),
            P(("sp", "tp"), None, None),
            P(("sp", "tp"), None, None),
            P(),
        ),
        out_specs=P(("sp", "tp"), None),
        check_vma=False,
    )
```

```python
import functools

import jax
import jax.numpy as jnp
from jax import lax
from jax.experimental import pallas as pl
from jax.experimental.pallas import tpu as pltpu
from jax.sharding import PartitionSpec as P

ALPHA = 8.0**0.25
RATE_C = 8.0
NORM_EPS = 1e-05
TINY = 1e-36
CAP = 8
BLOCK = 256
LANES = 8
F32 = jnp.float32
BF16 = jnp.bfloat16
VMEM = pl.BlockSpec(memory_space=pltpu.VMEM)
HBM = pl.BlockSpec(memory_space=pltpu.HBM)


def call(
    kernel, out_shape, in_specs, flops, scratch=(), name=None, out_specs=None, grid=(), limit=16
):
    if out_specs is None:
        out_specs = jax.tree.map(lambda _: VMEM, out_shape)
    return pl.pallas_call(
        kernel,
        out_shape=out_shape,
        in_specs=in_specs,
        out_specs=out_specs,
        grid=grid,
        scratch_shapes=list(scratch),
        compiler_params=pltpu.CompilerParams(vmem_limit_bytes=int(limit * 2**20)),
        cost_estimate=pl.CostEstimate(flops=flops, bytes_accessed=2**20, transcendentals=0),
        name=name,
    )


def shape(dims, dtype):
    return jax.ShapeDtypeStruct(dims, dtype)


def log1p_unit(u):
    s = u / (2.0 + u)
    q = s * s
    total = jnp.full_like(s, 1.0 / 17.0)
    for k in (15, 13, 11, 9, 7, 5, 3, 1):
        total = total * q + 1.0 / k
    return 2.0 * s * total


def minus_expm1_twice(x, decay):
    y = 2.0 * x
    total = jnp.full_like(y, 1.0 / 720.0)
    for k in (120, 24, 6, 2, 1):
        total = total * y + 1.0 / k
    return jnp.where(y > -0.125, -y * total, 1.0 - decay * decay)


def sigmoid(x):
    return 0.5 * jnp.tanh(0.5 * x) + 0.5


def layer_norm(values, gains):
    center = values - jnp.mean(values, axis=-1, keepdims=True)
    spread = jnp.mean(center * center, axis=-1, keepdims=True)
    return center * lax.rsqrt(spread + NORM_EPS) * gains


def fetch(pairs, sems):
    copies = [pltpu.make_async_copy(a, b, sems.at[i]) for i, (a, b) in enumerate(pairs)]
    for copy in copies:
        copy.start()
    return copies


def elements(conv, recur, gain, slope, moved):
    log_decay = slope * sigmoid(recur) + moved
    decay = jnp.exp(log_decay)
    power = minus_expm1_twice(log_decay, decay)
    return decay, power * lax.rsqrt(jnp.maximum(power, TINY)) * sigmoid(gain) * conv


def scan_kernel(
    halo_ref, small_ref, x_hbm, rmap_hbm, imap_hbm, tot_hbm, run_hbm,
    x_ref, rmap_ref, imap_ref, tot_ref, run_ref,
    ext, cv, rg, ig, sh, sems, outs,
):
    copies = fetch(
        [
            (x_hbm, x_ref),
            (rmap_hbm, rmap_ref),
            (imap_hbm, imap_ref),
        ],
        sems,
    )
    tokens, channels = x_ref.shape
    steps = tokens // LANES
    stride = steps + 8
    heads, width = rmap_ref.shape[:2]
    reach = halo_ref.shape[0]
    pad = 8 - reach
    copies[0].wait()
    for c in range(channels // 128):
        cols = slice(c * 128, (c + 1) * 128)
        x = x_ref[:, cols].astype(F32)
        ext[c, pl.ds(pad, reach), :] = halo_ref[:, cols].astype(F32)
        for i in range(LANES):
            if i > 0:
                ext[c, pl.ds(stride * i, 8), :] = x[steps * i - 8 : steps * i]
            ext[c, pl.ds(stride * i + 8, steps), :] = x[steps * i : steps * (i + 1)]
        taps = [small_ref[pl.ds(j, 1), cols] for j in range(reach + 1)]
        window = [ext[c, pl.ds(pad + j, LANES, stride=stride), :] for j in range(reach)]
        for t in range(steps):
            window.append(ext[c, pl.ds(8 + t, LANES, stride=stride), :])
            total = taps[0] * window[0]
            for j in range(1, reach + 1):
                total = total + taps[j] * window[j]
            window = window[1:]
            cv[pl.ds(t * LANES, LANES), cols] = total.astype(BF16).astype(F32)
    for copy in copies[1:]:
        copy.wait()
    for k in range(heads):
        cols = slice(k * width, (k + 1) * width)
        block = cv[:, cols].astype(BF16)
        rg[:, cols] = jnp.dot(block, rmap_ref[k], preferred_element_type=F32)
        ig[:, cols] = jnp.dot(block, imap_ref[k], preferred_element_type=F32)
    lines = [small_ref[pl.ds(reach + 2 + k, 1), :tokens] for k in range(heads)]
    full = jnp.concatenate(lines + [jnp.zeros((128 - heads, tokens), F32)], axis=0)
    full = jnp.transpose(full)
    for i in range(LANES):
        sh[pl.ds(stride * i, steps), :] = full[steps * i : steps * (i + 1)]
    logit = -small_ref[pl.ds(reach + 1, 1), :]
    slope = -RATE_C * (jnp.maximum(logit, 0.0) + log1p_unit(jnp.exp(-jnp.abs(logit))))

    def step(t, carry):
        rows = pl.ds(pl.multiple_of(t * LANES, LANES), LANES)
        moved = sh[pl.ds(t, LANES, stride=stride), :]
        out = []
        for k in range(heads):
            h, run = carry[k]
            cols = slice(k * width, (k + 1) * width)
            decay, update = elements(
                cv[rows, cols], rg[rows, cols], ig[rows, cols], slope[:, cols], moved[:, k : k + 1]
            )
            h = decay * h + update
            run = decay * run
            for j in range(width // 128):
                lane = slice(j * 128, (j + 1) * 128)
                run_ref[0, k * (width // 128) + j, rows, :] = h[:, lane]
                run_ref[1, k * (width // 128) + j, rows, :] = run[:, lane]
            out.append((h, run))
        return tuple(out)

    last = tuple(
        (jnp.zeros((LANES, width), F32), jnp.ones((LANES, width), F32)) for _ in range(heads)
    )
    sent = []
    for part in range(4):
        span = steps // 4
        last = lax.fori_loop(part * span, (part + 1) * span, step, last, unroll=2)
        rows = pl.ds(part * span * LANES, span * LANES)
        copy = pltpu.make_async_copy(
            run_ref.at[:, :, rows, :], run_hbm.at[:, :, rows, :], outs.at[part]
        )
        copy.start()
        sent.append(copy)
    row = lax.broadcasted_iota(jnp.int32, (LANES, width), 0)
    ends = [[], []]
    for k in range(heads):
        cols = slice(k * width, (k + 1) * width)
        h, a = last[k]
        for d in (1, 2, 4):
            hp, ap = pltpu.roll(h, d, 0), pltpu.roll(a, d, 0)
            h = jnp.where(row >= d, a * hp + h, h)
            a = jnp.where(row >= d, a * ap, a)
        for j in range(width // 128):
            lane = slice(j * 128, (j + 1) * 128)
            ends[0].append(jnp.log(jnp.maximum(a[LANES - 1 :, lane], TINY)))
            ends[1].append(h[LANES - 1 :, lane])
        enter = jnp.where(row >= 1, pltpu.roll(h, 1, 0), 0.0)
        scale = jnp.where(row >= 1, pltpu.roll(a, 1, 0), 1.0)
        for j in range(width // 128):
            lane = slice(j * 128, (j + 1) * 128)
            run_ref[0, k * (width // 128) + j, pl.ds(tokens, LANES), :] = enter[:, lane]
            run_ref[1, k * (width // 128) + j, pl.ds(tokens, LANES), :] = scale[:, lane]
    both = jnp.concatenate(ends[0] + ends[1], axis=0).astype(BF16)
    for i in range(tot_ref.shape[0]):
        tot_ref[i] = both
    rows = pl.ds(tokens, LANES)
    sent += [
        pltpu.make_async_copy(tot_ref, tot_hbm, outs.at[4]),
        pltpu.make_async_copy(run_ref.at[:, :, rows, :], run_hbm.at[:, :, rows, :], outs.at[5]),
    ]
    for copy in sent[4:]:
        copy.start()
    for copy in sent:
        copy.wait()


def side_kernel(
    gate_hbm, routes_hbm, weight_hbm, run_hbm, mixed_hbm, g_hbm, c_hbm,
    gate_ref, routes_ref, weight_ref, run_ref, mixed_ref, g_ref, c_ref, sems, outs,
):
    copies = fetch(
        [
            (routes_hbm, routes_ref),
            (weight_hbm, weight_ref),
            (gate_hbm, gate_ref),
            (run_hbm, run_ref),
        ],
        sems,
    )
    for copy in copies[:2]:
        copy.wait()
    route(routes_ref, weight_ref, g_ref, c_ref)
    for copy in copies[2:]:
        copy.wait()
    tokens, channels = gate_ref.shape
    steps = tokens // LANES
    block = 16
    per = steps // block

    def put(i, _):
        rows = pl.ds(pl.multiple_of(i * block, block), block)
        chunk = i // per
        source = pl.ds(chunk + (i % per) * (block * LANES), block, stride=LANES)
        gate = jax.nn.gelu(gate_ref[rows, :].astype(F32), approximate=True)
        edge = pl.ds(tokens + chunk, 1)
        for c in range(channels // 128):
            cols = slice(c * 128, (c + 1) * 128)
            run = run_ref[1, c, source, :]
            own = run_ref[0, c, source, :] + run * run_ref[0, c, edge, :]
            mixed_ref[0, rows, cols] = own * gate[:, cols]
            mixed_ref[1, rows, cols] = run * run_ref[1, c, edge, :] * gate[:, cols]
        return 0

    pairs = [(g_ref, g_hbm), (c_ref, c_hbm)]
    sent = fetch(pairs, outs)
    quarter = tokens // 4
    for part in range(4):
        lax.fori_loop(part * quarter // block, (part + 1) * quarter // block, put, 0)
        rows = pl.ds(part * quarter, quarter)
        copy = pltpu.make_async_copy(
            mixed_ref.at[:, rows, :], mixed_hbm.at[pl.ds(0, 2), rows, :], outs.at[2 + part]
        )
        copy.start()
        sent.append(copy)
    for copy in sent:
        copy.wait()


def mix_kernel(
    seen_ref, mixed_hbm, w_hbm, mine_ref, theirs_ref, w_ref, mixed_ref, sems
):
    _, tokens, channels = mixed_ref.shape
    here, side = lax.axis_index("sp"), lax.axis_index("tp")
    half = tokens // 2
    strip = channels // 2
    pairs = []
    for j in range(2):
        at = pl.multiple_of((1 - side if j == 0 else side) * half, half)
        for k in range(2):
            pairs.append((mixed_hbm.at[k, pl.ds(at, half), :], mixed_ref.at[k, pl.ds(j * half, half), :]))
    pairs.append((w_hbm.at[pl.ds(pl.multiple_of(side * channels, strip), strip), :], w_ref))
    copies = fetch(pairs, sems)
    carried = jnp.zeros((LANES, 128), F32)
    for i in range(seen_ref.shape[0]):
        pair = seen_ref[i].astype(F32)
        carried = jnp.where(i < here, jnp.exp(pair[:LANES]) * carried + pair[LANES:], carried)
    carried = jnp.concatenate([carried[i : i + 1] for i in range(LANES)], axis=1)
    block = 16
    for j, ref in enumerate((theirs_ref, mine_ref)):
        for copy in copies[2 * j : 2 * j + 2]:
            copy.wait()

        def put(i, _):
            rows = pl.ds(pl.multiple_of(j * half + i * block, block), block)
            ref[pl.ds(pl.multiple_of(i * block, block), block), :] = (
                mixed_ref[0, rows, :] + mixed_ref[1, rows, :] * carried
            ).astype(BF16)
            return 0

        lax.fori_loop(0, half // block, put, 0, unroll=2)
    for copy in copies[4:]:
        copy.wait()


def route(routes_ref, weight_ref, g_ref, c_ref):
    fanout, rows = routes_ref.shape
    slots = g_ref.shape[0]
    experts = slots // CAP
    expert = lax.broadcasted_iota(jnp.int32, (experts, rows), 0)
    member = jnp.zeros((experts, rows), F32)
    weight = jnp.zeros((experts, rows), F32)
    for k in range(fanout):
        hit = expert == routes_ref[pl.ds(k, 1), :]
        member = member + jnp.where(hit, 1.0, 0.0)
        weight = weight + jnp.where(hit, weight_ref[pl.ds(k, 1), :], 0.0)
    earlier = (
        lax.broadcasted_iota(jnp.int32, (rows, rows), 0)
        < lax.broadcasted_iota(jnp.int32, (rows, rows), 1)
    )
    rank = jnp.dot(
        member.astype(BF16), jnp.where(earlier, 1.0, 0.0).astype(BF16), preferred_element_type=F32
    )
    rank = jnp.where(member > 0.0, rank, -1.0).astype(BF16)
    weight = weight.astype(BF16)
    slot = lax.broadcasted_iota(jnp.int32, (BLOCK, experts), 0)
    spread_at = lax.broadcasted_iota(jnp.int32, (BLOCK, experts), 1)
    place = (lax.broadcasted_iota(jnp.int32, (BLOCK, rows), 0) % CAP).astype(F32)
    for b in range(slots // BLOCK):
        spread = jnp.where((slot + b * BLOCK) // CAP == spread_at, 1.0, 0.0).astype(BF16)

        def to_slots(values):
            return jnp.dot(spread, values, preferred_element_type=F32)

        chosen = to_slots(rank) == place
        g_ref[pl.ds(b * BLOCK, BLOCK), :] = jnp.where(chosen, 1.0, 0.0).astype(BF16)
        cols = slice(b * BLOCK, (b + 1) * BLOCK)
        c_ref[:, cols] = jnp.transpose(jnp.where(chosen, to_slots(weight), 0.0)).astype(BF16)


def project_kernel(mine_ref, res_ref, w_ref, w_hbm, out_ref, rest_ref, own_ref, sems):
    depth = mine_ref.shape[1]
    half = depth // 2
    side = lax.axis_index("tp")
    pairs = [(w_hbm.at[pl.ds(pl.multiple_of(side * depth + half, half), half), :], own_ref)]
    for j in range(2):
        at = pl.multiple_of((1 - side) * depth + j * half, half)
        pairs.append((w_hbm.at[pl.ds(at, half), :], rest_ref.at[pl.ds(j * half, half), :]))
    copies = fetch(pairs, sems)
    out_ref[...] = ALPHA * res_ref[...].astype(F32) + jnp.dot(
        mine_ref[:, :half], w_ref[...], preferred_element_type=F32
    )
    copies[0].wait()
    out_ref[...] += jnp.dot(mine_ref[:, half:], own_ref[...], preferred_element_type=F32)
    for copy in copies[1:]:
        copy.wait()


def dispatch_kernel(other_ref, rest_ref, acc_ref, gain_ref, g_ref, normed_ref, out_ref):
    values = acc_ref[...] + jnp.dot(other_ref[...], rest_ref[...], preferred_element_type=F32)
    normed = layer_norm(values, gain_ref[...]).astype(BF16)
    normed_ref[...] = normed

    out_ref[...] = jnp.dot(g_ref[...], normed, preferred_element_type=F32).astype(BF16)


def hidden_of(x, gate, up):
    return (
        jax.nn.silu(jnp.dot(x, gate, preferred_element_type=F32))
        * jnp.dot(x, up, preferred_element_type=F32)
    ).astype(BF16)


def expert_kernel(
    x_ref, gate_ref, up_ref, down_ref, own_ref, sgate_ref, sup_ref, sdown_ref, out_ref, base_ref
):
    block = 2 * BLOCK

    def step(i, _):
        rows = pl.ds(pl.multiple_of(i * block, block), block)
        hidden = hidden_of(x_ref[rows, :], gate_ref[0], up_ref[0])
        out_ref[rows, :] = jnp.dot(hidden, down_ref[0], preferred_element_type=F32).astype(BF16)
        return 0

    lax.fori_loop(0, x_ref.shape[0] // block, step, 0)
    x = own_ref[...]
    hidden = hidden_of(x, sgate_ref[...], sup_ref[...])
    base_ref[...] = ALPHA * x.astype(F32) + jnp.dot(
        hidden, sdown_ref[...], preferred_element_type=F32
    )


def finish_kernel(base_ref, c_ref, back_ref, gain_ref, out_ref):
    values = base_ref[...] + jnp.dot(c_ref[...], back_ref[...], preferred_element_type=F32)
    out_ref[...] = layer_norm(values, gain_ref[...]).astype(BF16)


def on_device(
    gate_pre, conv_in, conv_taps, recur_map, input_map, rate_logit, decay_shift, out_weight,
    residual, gain_mix, routes, route_weight, shared_gate, shared_up, shared_down, expert_gate,
    expert_up, expert_down, gain_out,
):
    tokens, channels = conv_in.shape
    reach = conv_taps.shape[0] - 1
    sp, tp = lax.axis_size("sp"), lax.axis_size("tp")
    experts = sp * tp
    rows = tokens // tp
    model = out_weight.shape[1]
    slots = experts * CAP
    sem = pltpu.SemaphoreType.DMA
    before = lax.ppermute(conv_in[tokens - reach :], "sp", [(i, i + 1) for i in range(sp - 1)])
    padded = shape((8, tokens, channels), F32)
    big = pltpu.VMEM((tokens, channels), F32)
    apart = tokens + 8 * LANES
    lanes = pltpu.VMEM((channels // 128, apart, 128), F32)

    def staged(kernel, operands, made, flops, scratch, name):
        held = [
            pltpu.VMEM((2,) + x.shape[1:] if x is padded else x.shape, x.dtype)
            for x in tuple(operands) + made
        ]
        return call(
            kernel,
            made,
            [HBM] * len(operands),
            flops,
            held + scratch,
            name=name,
            out_specs=(HBM,) * len(made),
            limit=62,
        )(*operands)

    small = jnp.concatenate(
        [
            conv_taps.astype(F32),
            rate_logit[None],
            jnp.pad(decay_shift.T, ((0, 0), (0, channels - tokens))),
        ],
        axis=0,
    )
    made = (
        shape((sp, 2 * LANES, 128), BF16),
        shape((2, channels // 128, tokens + LANES, 128), F32),
    )
    held = (conv_in, recur_map, input_map) + made
    totals, local = call(
        scan_kernel,
        made,
        [VMEM] * 2 + [HBM] * 3,
        10**9,
        [pltpu.VMEM(x.shape, x.dtype) for x in held]
        + [lanes, big, big, big, pltpu.VMEM((apart, 128), F32), sem((3,)), sem((6,))],
        name="scan",
        out_specs=(HBM,) * 2,
        limit=53.5,
    )(before, small, conv_in, recur_map, input_map)
    seen = lax.all_to_all(totals, "sp", 0, 0, tiled=True)
    parts, g, c = staged(
        side_kernel,
        (gate_pre, routes.T, route_weight.T, local),
        (padded, shape((slots, rows), BF16), shape((rows, slots), BF16)),
        10**10,
        [sem((4,)), sem((6,))],
        "side",
    )
    piece = shape((rows, channels), BF16)
    mine, theirs, most = call(
        mix_kernel,
        (piece, piece, shape((channels // 2, model), BF16)),
        [VMEM, HBM, HBM],
        10**8,
        [pltpu.VMEM((2, tokens, channels), F32), sem((5,))],
        name="mix",
        limit=48,
    )(seen, parts, out_weight)
    other = lax.ppermute(theirs, "tp", [(0, 1), (1, 0)])
    wide = shape((rows, model), F32)
    acc, rest = call(
        project_kernel,
        (wide, shape((channels, model), BF16)),
        [VMEM, VMEM, VMEM, HBM],
        10**9,
        [pltpu.VMEM((channels // 2, model), BF16), sem((3,))],
        name="project",
        limit=41,
    )(mine, residual, most, out_weight)
    normed, outgoing = call(
        dispatch_kernel,
        (shape((rows, model), BF16), shape((slots, model), BF16)),
        [VMEM] * 5,
        2 * 10**9,
        name="dispatch",
        limit=24,
    )(other, rest, acc, gain_mix[None], g)

    def exchanged(x):
        x = x.reshape(experts, CAP, model)
        x = lax.all_to_all(x, ("sp", "tp"), split_axis=0, concat_axis=0, tiled=True)
        return x.reshape(slots, model)

    received = exchanged(outgoing)
    results, base = call(
        expert_kernel,
        (shape((slots, model), BF16), wide),
        [VMEM] * 8,
        7 * 10**9,
        name="expert",
        limit=24,
    )(
        received, expert_gate, expert_up, expert_down, normed, shared_gate, shared_up, shared_down
    )
    back = exchanged(results)
    return call(
        finish_kernel,
        shape((rows, model), BF16),
        [VMEM] * 4,
        10**9,
        name="finish",
    )(base, c, back, gain_out[None])


def solution(mesh):
    return jax.shard_map(
        on_device,
        mesh=mesh,
        in_specs=(
            P("sp", "tp"),
            P("sp", "tp"),
            P(None, "tp"),
            P("tp", None, None),
            P("tp", None, None),
            P("tp"),
            P("sp", "tp"),
            P(),
            P(("sp", "tp"), None),
            P(),
            P(("sp", "tp"), None),
            P(("sp", "tp"), None),
            P(),
            P(),
            P(),
            P(("sp", "tp"), None, None),
            P(("sp", "tp"), None, None),
            P(("sp", "tp"), None, None),
            P(),
        ),
        out_specs=P(("sp", "tp"), None),
        check_vma=False,
    )
```
